256 devices in a mesh: sp: 64 (over z, x, core), tp: 4 (over y).
Axes of the slice: x: 4, y: 4, z: 8, core: 2. Of those that a mesh axis runs over, the one named last changes fastest.
Arguments:
- residual: bfloat16 [16384, 2048], P(('sp', 'tp')), may hold values from -6 to 6
- query_wide: bfloat16 [16384, 512], P('sp', 'tp'), may hold values from -8 to 8
- key_wide: bfloat16 [16384, 512], P('sp', 'tp'), may hold values from -8 to 8
- value_wide: bfloat16 [16384, 512], P('sp', 'tp'), may hold values from -6 to 6
- query_narrow: bfloat16 [16384, 512], P('sp', 'tp'), may hold values from -8 to 8
- key_narrow: bfloat16 [16384, 512], P('sp', 'tp'), may hold values from -8 to 8
- value_narrow: bfloat16 [16384, 512], P('sp', 'tp'), may hold values from -6 to 6
- gate_wide: float32 [16384, 4], P('sp', 'tp'), may hold values from -2 to 20
- gate_narrow: float32 [16384, 8], P('sp', 'tp'), may hold values from -2 to 20
- out_wide: bfloat16 [512, 2048], replicated, may hold values from -0.1875 to 0.1875
- out_narrow: bfloat16 [512, 2048], replicated, may hold values from -0.1875 to 0.1875
- norm_gain: float32 [2048], replicated, may hold values from 0.1 to 1.9
- routing: int32 [16384, 2], P(('sp', 'tp')), may hold values from 0 to 63, as said below
- route_weight: float32 [16384, 2], P(('sp', 'tp')), may hold values from 0.3 to 1.5
- gate_weight: bfloat16 [64, 2048, 1024], P('sp', None, 'tp'), may hold values from -0.125 to 0.125
- up_weight: bfloat16 [64, 2048, 1024], P('sp', None, 'tp'), may hold values from -0.125 to 0.125
- down_weight: bfloat16 [64, 1024, 2048], P('sp', 'tp'), may hold values from -0.1875 to 0.1875
Outputs:
- result: bfloat16 [16384, 2048], P(('sp', 'tp'))
The draws below stay inside these ranges and needn't reach their ends.
Inputs may be any that keep to these rules, and one draw needn't show every extreme that they name: `routing`: each row names 2 different experts of one group (experts g * 16 to g * 16 + 15). In each aligned block of 64 rows (the rows of one device) no expert is named by more than 4 rows; one group, the same for all blocks, has each of its experts named by exactly 4 rows of every block.
All inputs are finite; a program needn't handle non-finite values.
Results may differ from the reference program's by a relative error of at most 0.017.
Values may be sent and summed in bfloat16 or wider, within the bound.
No kernel may reach another device: no remote copies, remote signals or barrier semaphores. Data moves between devices by JAX's collectives and lax.ppermute only.
A program may use at most 128 MiB of HBM per device.

```python
import math
import jax
import jax.numpy as jnp
from jax import lax

D = 2048
WIDE = 4
HW = 128
NARROW = 8
HN = 64
FFE = 1024
GROUPS = 4
TOP = 2
TOK_DEV = 256
TOKENS = 16384
EXPERTS = 64
EPG = 16
ROWS_DEV = 64
CAP = 4
N_TP = 4


def projected(key, breadth, salt_value):
    values = 1.7 * jax.random.normal(jax.random.fold_in(key, salt_value), (TOKENS, breadth), jnp.float32)
    values = jnp.clip(values, -8.0, 8.0)
    return values.astype(jnp.bfloat16)


def forget(key, head_count, salt_value):
    seeded = jax.random.fold_in(key, salt_value)
    order_key, drift_key, jitter_key = jax.random.split(seeded, 3)
    ranking = jax.random.permutation(order_key, head_count)
    keeping = head_count // 2
    baseline = jnp.where(ranking < keeping, jnp.log(1.0 * TOKENS), jnp.log(40.0))
    shards = TOKENS // TOK_DEV
    drift_part = jax.random.uniform(drift_key, (shards, 1, head_count), jnp.float32, -0.8, 0.8)
    drift_part = jnp.broadcast_to(drift_part, (shards, TOK_DEV, head_count)).reshape(TOKENS, head_count)
    jitter = jnp.clip(jax.random.normal(jitter_key, (TOKENS, head_count), jnp.float32), -4.0, 4.0)
    return (baseline[None, :] + drift_part + jitter).astype(jnp.float32)


def draw_query_wide(key, part):
    return projected(key, WIDE * HW, 11)


def draw_key_wide(key, part):
    return projected(key, WIDE * HW, 12)


def draw_query_narrow(key, part):
    return projected(key, NARROW * HN, 21)


def draw_key_narrow(key, part):
    return projected(key, NARROW * HN, 22)


def draw_gate_wide(key, part):
    return forget(key, WIDE, 31)


def draw_gate_narrow(key, part):
    return forget(key, NARROW, 32)


def route_block(key, full_group):
    cut_key, label_key, row_key = jax.random.split(key, 3)
    half_rows = ROWS_DEV // 2
    ordinal = jnp.arange(ROWS_DEV, dtype=jnp.int32)
    cut_points = jnp.sort(jax.random.randint(cut_key, (GROUPS - 2,), 0, half_rows + 1))
    remainder = ordinal - half_rows
    other_group = jnp.sum((remainder[:, None] >= cut_points[None, :]).astype(jnp.int32), axis=1)
    group_starts = jnp.concatenate([jnp.zeros((1,), jnp.int32), cut_points.astype(jnp.int32)])
    in_full = ordinal < half_rows
    ranking = jnp.where(in_full, ordinal, remainder - group_starts[other_group])
    chosen_group = jnp.where(in_full, full_group, (full_group + 1 + other_group) % GROUPS)

    def labels_of(group_number):
        return jax.random.permutation(jax.random.fold_in(label_key, group_number), EPG)
    labels = jax.vmap(labels_of)(jnp.arange(GROUPS, dtype=jnp.int32))
    slot_number = TOP * ranking[:, None] + jnp.arange(TOP, dtype=jnp.int32)[None, :]
    local_expert = labels[chosen_group[:, None], slot_number % EPG]
    expert_ids = (chosen_group[:, None] * EPG + local_expert).astype(jnp.int32)
    shuffled = jax.random.permutation(row_key, ROWS_DEV)
    return jnp.zeros((ROWS_DEV, TOP), jnp.int32).at[shuffled].set(expert_ids)


def draw_routing(key, part):
    seeded = jax.random.fold_in(key, 4242)
    full_group = jax.random.randint(jax.random.fold_in(seeded, 1), (), 0, GROUPS)

    def one_block(block_number):
        return route_block(jax.random.fold_in(seeded, block_number + 2), full_group)
    blocks = jax.vmap(one_block)(jnp.arange(TOKENS // ROWS_DEV, dtype=jnp.int32))
    return blocks.reshape(TOKENS, TOP)


def block_scale(own_key, dims, cuts, low, largest):
    loudness, own = 1.0, jax.random.fold_in(own_key, 6)
    for axis_at, shards_of in cuts:
        heights = jnp.exp(jax.random.uniform(jax.random.fold_in(own, axis_at), (shards_of,), jnp.float32, low / len(cuts), largest / len(cuts)))
        loudness = loudness * jnp.repeat(heights, dims[axis_at] // shards_of).reshape([-1 if axis == axis_at else 1 for axis in range(len(dims))])
    return loudness


def bell_draw(stream_key, shape, scale, most, cuts=(), kind=jnp.bfloat16):
    array = jax.random.normal(stream_key, shape, jnp.float32) * scale
    if len(cuts) > 0:
        array = block_scale(stream_key, shape, cuts, -0.22, 0.18) * array
    return jnp.clip(array, min=-most, max=most).astype(kind)


def setup_inputs(seed: int = 0) -> dict:
    key_list = jax.random.split(jax.random.key(seed), 18)
    return {
        "residual": bell_draw(key_list[0], (TOKENS, D), 1.0, 6.0, ((0, 256),)),
        "query_wide": draw_query_wide(jax.random.fold_in(key_list[17], 71), 0),
        "key_wide": draw_key_wide(jax.random.fold_in(key_list[17], 71), 0),
        "value_wide": bell_draw(key_list[3], (TOKENS, WIDE * HW), 1.0, 6.0, ((0, 64), (1, 4))),
        "query_narrow": draw_query_narrow(jax.random.fold_in(key_list[17], 71), 0),
        "key_narrow": draw_key_narrow(jax.random.fold_in(key_list[17], 71), 0),
        "value_narrow": bell_draw(key_list[6], (TOKENS, NARROW * HN), 1.0, 6.0, ((0, 64), (1, 4))),
        "gate_wide": draw_gate_wide(jax.random.fold_in(key_list[17], 71), 0),
        "gate_narrow": draw_gate_narrow(jax.random.fold_in(key_list[17], 71), 0),
        "out_wide": bell_draw(key_list[9], (WIDE * HW, D), (WIDE * HW + NARROW * HN) ** -0.5, 0.1875),
        "out_narrow": bell_draw(key_list[10], (NARROW * HN, D), (WIDE * HW + NARROW * HN) ** -0.5, 0.1875),
        "norm_gain": jnp.clip(1.0 + 0.18 * jax.random.normal(key_list[11], (D,), jnp.float32), 0.1, 1.9),
        "routing": draw_routing(jax.random.fold_in(key_list[17], 71), 0),
        "route_weight": jnp.clip(jnp.exp(math.log(1.5) - 1.60943787 * jax.random.uniform(key_list[13], (TOKENS, TOP), jnp.float32) ** block_scale(key_list[13], (TOKENS, TOP), ((0, 256),), -0.2, 0.2)), 0.3, 1.5),
        "gate_weight": bell_draw(key_list[14], (EXPERTS, D, FFE), D ** -0.5, 0.125, ((0, 64), (2, 4))),
        "up_weight": bell_draw(key_list[15], (EXPERTS, D, FFE), D ** -0.5, 0.125, ((0, 64), (2, 4))),
        "down_weight": bell_draw(key_list[16], (EXPERTS, FFE, D), FFE ** -0.5, 0.1875, ((0, 64), (1, 4))),
    }


epsilon = 1e-06

def attend(queries, keys, values, gates, head_width):
    length = queries.shape[0]
    head_count = gates.shape[1]
    decay = jnp.cumsum(jax.nn.log_sigmoid(gates.astype(jnp.float32)), axis=0)
    grid_query = queries.reshape(length, head_count, head_width).astype(jnp.float32)
    grid_key = keys.reshape(length, head_count, head_width).astype(jnp.float32)
    grid_value = values.reshape(length, head_count, head_width).astype(jnp.float32)
    block_size = math.gcd(length, 512)
    key_place = jnp.arange(length, dtype=jnp.int32)

    def one_block(position):
        begin = (position * block_size).astype(jnp.int32)
        part_query = lax.dynamic_slice_in_dim(grid_query, begin, block_size, 0)
        part_decay = lax.dynamic_slice_in_dim(decay, begin, block_size, 0)
        scores = jnp.einsum('thd,phd->htp', part_query, grid_key) * head_width ** (-0.5)
        scores = scores + part_decay.T[:, :, None] - decay.T[:, None, :]
        query_place = begin + jnp.arange(block_size, dtype=jnp.int32)
        scores = jnp.where(key_place[None, None, :] <= query_place[None, :, None], scores, -jnp.inf)
        weights = jnp.exp(scores - lax.optimization_barrier(jnp.max(scores, axis=2, keepdims=True)))
        weight_sum = lax.optimization_barrier(jnp.sum(weights, axis=2))
        rounded = lax.optimization_barrier(weights.astype(jnp.bfloat16)).astype(jnp.float32)
        mixed_heads = jnp.einsum('htp,phd->htd', rounded, grid_value) / weight_sum[:, :, None]
        return jnp.transpose(mixed_heads, (1, 0, 2)).reshape(block_size, head_count * head_width).astype(jnp.bfloat16)
    blocks = lax.map(one_block, jnp.arange(length // block_size, dtype=jnp.int32))
    return blocks.reshape(length, head_count * head_width)

def experts_apply(normed, routing, route_weight, gate_weight, up_weight, down_weight):
    length = normed.shape[0]
    chosen_count = routing.shape[1]
    expert_count = gate_weight.shape[0]
    flat_routes = routing.reshape(-1).astype(jnp.int32)
    matches = (flat_routes[:, None] == jnp.arange(expert_count, dtype=jnp.int32)[None, :]).astype(jnp.int32)
    ranking = lax.optimization_barrier(jnp.sum((jnp.cumsum(matches, axis=0) - matches) * matches, axis=1)).astype(jnp.int32)
    capacity_all = length // ROWS_DEV * CAP
    lookup = jnp.full((expert_count, capacity_all), length * chosen_count, jnp.int32)
    lookup = lookup.at[flat_routes, ranking].set(jnp.arange(length * chosen_count, dtype=jnp.int32))
    flat_weights = route_weight.reshape(-1)

    def one_expert(carried, pieces):
        copies, gate_part, up_part, down_part = pieces
        positions = (copies // chosen_count).astype(jnp.int32)
        chosen_rows = jnp.take(normed, positions, axis=0, mode='clip')
        gate_value = jnp.dot(chosen_rows, gate_part, preferred_element_type=jnp.float32)
        up_value = jnp.dot(chosen_rows, up_part, preferred_element_type=jnp.float32)
        hidden = (jax.nn.silu(gate_value) * up_value).astype(jnp.bfloat16)
        hidden_blocks = hidden.reshape(capacity_all, N_TP, -1).astype(jnp.float32)
        down_blocks = down_part.reshape(N_TP, -1, down_part.shape[1]).astype(jnp.float32)
        partial_out = jnp.einsum('lnf,nfd->nld', hidden_blocks, down_blocks)
        partial_out = lax.optimization_barrier(partial_out.astype(jnp.bfloat16)).astype(jnp.float32)
        expert_out = lax.optimization_barrier(jnp.sum(partial_out, axis=0)).astype(jnp.bfloat16)
        scale = jnp.take(flat_weights, copies, mode='fill', fill_value=0.0)
        carried = carried.at[positions].add(scale[:, None] * expert_out.astype(jnp.float32), mode='drop')
        return (carried, None)
    start = jnp.zeros((length, normed.shape[1]), jnp.float32)
    total, _ = lax.scan(one_expert, start, (lookup, gate_weight, up_weight, down_weight))
    return total

def reference(residual, query_wide, key_wide, value_wide, query_narrow, key_narrow, value_narrow, gate_wide, gate_narrow, out_wide, out_narrow, norm_gain, routing, route_weight, gate_weight, up_weight, down_weight):
    att_wide = attend(query_wide, key_wide, value_wide, gate_wide, HW)
    att_narrow = attend(query_narrow, key_narrow, value_narrow, gate_narrow, HN)
    mixed = jnp.dot(att_wide, out_wide, preferred_element_type=jnp.float32)
    mixed = mixed + jnp.dot(att_narrow, out_narrow, preferred_element_type=jnp.float32)
    middle = (residual.astype(jnp.float32) + mixed).astype(jnp.bfloat16)
    middle_wide = middle.astype(jnp.float32)
    spread = lax.optimization_barrier(jnp.mean(middle_wide * middle_wide, axis=1, keepdims=True))
    normed = (middle_wide * lax.rsqrt(spread + epsilon) * norm_gain).astype(jnp.bfloat16)
    routed = experts_apply(normed, routing, route_weight, gate_weight, up_weight, down_weight)
    return (middle_wide + routed).astype(jnp.bfloat16)
```

```python
import functools

import jax
import jax.numpy as jnp
from jax import lax
from jax.experimental import pallas as pl
from jax.experimental.pallas import tpu as pltpu
from jax.sharding import Mesh
from jax.sharding import PartitionSpec as P

HW = 128
HN = 64
GROUPS = 4
EPS = 1e-06
LOG2E = 1.4426950408889634
LOW = -1e30
TQ = 256


def dot_f32(a, b, dims=(((1,), (0,)), ((), ()))):
    return lax.dot_general(a, b, dims, preferred_element_type=jnp.float32)


def attention_kernel(
    place_ref, q_ref, dk_ref, kv_ref, *rest, flip, row0, rows, dev_rows, tiles, first, last
):
    if first:
        ins, rest = (), rest
    else:
        ins, rest = rest[:3], rest[3:]
    if last:
        out_ref, m_ref, l_ref, acc_ref, qh_ref = rest
    else:
        m_ref, l_ref, acc_ref, qh_ref = rest
    t = pl.program_id(0)
    place = place_ref[0]
    chip, core = place // 2, place % 2
    sub = core if flip == 0 else 1 - core
    tile_keys = kv_ref.shape[0]
    chips_tile = tile_keys // rows
    last_tile = chip // chips_tile
    queries = q_ref.shape[0]
    scale = jnp.where(core == 0, jnp.float32(HW**-0.5 * LOG2E), jnp.float32(HN**-0.5 * LOG2E))

    @pl.when(t == 0)
    def _():
        if first:
            m_ref[...] = jnp.full_like(m_ref, LOW)
            l_ref[...] = jnp.zeros_like(l_ref)
            acc_ref[...] = jnp.zeros_like(acc_ref)
        else:
            m_ref[...] = ins[0][...]
            l_ref[...] = ins[1][...]
            acc_ref[...] = ins[2][...]
        lane = lax.broadcasted_iota(jnp.int32, (queries, HW), 1)
        q = q_ref[...]
        zero = jnp.zeros_like(q)
        qh_ref[0] = jnp.where((core == 0) | (lane < HN), q, zero)
        qh_ref[1] = jnp.where(lane >= HN, q, zero)

    def one(h, masked):
        k = kv_ref[:, :HW]
        v = kv_ref[:, HW:]
        lines = dev_rows // 128
        dk = jnp.concatenate(
            [
                dk_ref[2 * c + sub, pl.ds(lines * (h + core) + (row0 + r) // 128, 1), :]
                for c in range(chips_tile)
                for r in range(0, rows, 128)
            ],
            axis=1,
        )
        for r0 in range(0, queries, TQ):
            span = pl.ds(r0, TQ)
            s = dot_f32(qh_ref[h, span, :], k, (((1,), (1,)), ((), ()))) * scale - dk
            if masked:
                col = lax.broadcasted_iota(jnp.int32, (TQ, tile_keys), 1)
                row = lax.broadcasted_iota(jnp.int32, (TQ, tile_keys), 0)
                key_chip = t * chips_tile + col // rows
                key_place = key_chip * (2 * dev_rows) + sub * dev_rows + row0 + col % rows
                s = jnp.where(key_place <= chip * (2 * dev_rows) + r0 + row, s, LOW)
            m_old = m_ref[h, span, :]
            m_new = jnp.maximum(m_old, jnp.max(s, axis=1, keepdims=True))
            alpha = jnp.exp2(m_old - m_new)
            p = jnp.exp2(s - m_new[:, :1])
            m_ref[h, span, :] = m_new
            l_ref[h, span, :] = l_ref[h, span, :] * alpha + jnp.sum(p, axis=1, keepdims=True)
            acc_ref[h, span, :] = acc_ref[h, span, :] * alpha + dot_f32(p.astype(jnp.bfloat16), v)

    for masked in (False, True):
        at = (t == last_tile) if masked else (t < last_tile)

        @pl.when(at)
        def _():
            one(0, masked)

        @pl.when(at & (core == 1))
        def _():
            one(1, masked)

    if last:

        @pl.when(t == tiles - 1)
        def _():
            one_head = acc_ref[0] / l_ref[0]
            lane = lax.broadcasted_iota(jnp.int32, (queries, HW), 1)
            other = acc_ref[1] / jnp.where(core == 0, 1.0, l_ref[1])
            out_ref[...] = jnp.where((core == 0) | (lane < HN), one_head, other).astype(jnp.bfloat16)


def attend_chunk(place, q, dk, kv, state, flip, row0, rows, dev_rows, last):
    queries = q.shape[0]
    keys = kv.shape[0]
    tile_keys = min(1024, keys)
    chips_tile = tile_keys // rows
    tiles = keys // tile_keys
    first = state is None

    def clamp(t, place):
        return jnp.minimum(t, place[0] // 2 // chips_tile)

    whole = pl.BlockSpec((2, queries, HW), lambda t, place: (0, 0, 0))
    in_specs = [
        pl.BlockSpec((queries, HW), lambda t, place: (0, 0)),
        pl.BlockSpec((2 * chips_tile, *dk.shape[1:]), lambda t, place: (clamp(t, place), 0, 0)),
        pl.BlockSpec((tile_keys, 2 * HW), lambda t, place: (clamp(t, place), 0)),
    ]
    args = [q, dk, kv]
    if not first:
        in_specs += [whole] * 3
        args += list(state)
    held = jax.ShapeDtypeStruct((2, queries, HW), jnp.float32)
    scratch = [pltpu.VMEM((2, queries, HW), jnp.bfloat16)]
    if last:
        out_shape = jax.ShapeDtypeStruct((queries, HW), jnp.bfloat16)
        out_specs = pl.BlockSpec((queries, HW), lambda t, place: (0, 0))
        scratch = [pltpu.VMEM((2, queries, HW), jnp.float32)] * 3 + scratch
    else:
        out_shape = [held] * 3
        out_specs = [whole] * 3
    return pl.pallas_call(
        functools.partial(
            attention_kernel,
            flip=flip,
            row0=row0,
            rows=rows,
            dev_rows=dev_rows,
            tiles=tiles,
            first=first,
            last=last,
        ),
        out_shape=out_shape,
        grid_spec=pltpu.PrefetchScalarGridSpec(
            num_scalar_prefetch=1,
            grid=(tiles,),
            in_specs=in_specs,
            out_specs=out_specs,
            scratch_shapes=scratch,
        ),
        compiler_params=pltpu.CompilerParams(
            dimension_semantics=("arbitrary",), vmem_limit_bytes=60 * 1024 * 1024
        ),
        cost_estimate=pl.CostEstimate(
            flops=8 * queries * keys * HW, transcendentals=2 * queries * keys, bytes_accessed=4 * keys * HW
        ),
        name="attend",
    )(place, *args)


def running_kernel(wide_ref, narrow_ref, out_ref):
    gates = jnp.concatenate([wide_ref[...], narrow_ref[...]], axis=0)
    kept = jnp.minimum(gates, 0.0) - jnp.log1p(jnp.exp(-jnp.abs(gates)))
    heads, rows = kept.shape
    row = lax.broadcasted_iota(jnp.int32, (rows, rows), 0)
    col = lax.broadcasted_iota(jnp.int32, (rows, rows), 1)
    upto = (row <= col).astype(jnp.float32)
    kept = jnp.concatenate([kept, jnp.zeros((8 - heads, rows), jnp.float32)], axis=0)
    sums = lax.dot_general(
        kept,
        upto,
        (((1,), (0,)), ((), ())),
        precision=lax.Precision.HIGHEST,
        preferred_element_type=jnp.float32,
    )
    out_ref[...] = jnp.zeros_like(out_ref)
    lines = rows // 128
    for h in range(heads):
        for j in range(lines):
            at = lines * h + j
            out_ref[at : at + 1, :] = sums[h : h + 1, j * 128 : (j + 1) * 128]


def running_sums(gate_wide, gate_narrow):
    return pl.pallas_call(
        running_kernel, out_shape=jax.ShapeDtypeStruct((8, 128), jnp.float32), name="running"
    )(gate_wide.T, gate_narrow.T)


def offset_kernel(place_ref, every_ref, out_ref):
    home = place_ref[0] // 2 * 2
    devices = every_ref.shape[0]
    odd = lax.broadcasted_iota(jnp.int32, (8, 128), 0) % 2 == 1
    offset = jnp.zeros((8, 128), jnp.float32)
    base = offset
    for d in range(devices):
        here = every_ref[d]
        out_ref[d] = here + offset
        base = jnp.where(home == d, offset, base)
        end = jnp.broadcast_to(here[:, 127:128], (8, 128))
        offset = offset + jnp.where(odd, end, jnp.concatenate([end[1:], end[:1]], axis=0))
    for d in range(devices):
        out_ref[d] = (out_ref[d] - base) * LOG2E


def offset_sums(place, every):
    return pl.pallas_call(
        offset_kernel,
        out_shape=jax.ShapeDtypeStruct(every.shape, jnp.float32),
        in_specs=[pl.BlockSpec(memory_space=pltpu.SMEM), pl.BlockSpec(memory_space=pltpu.VMEM)],
        name="offset",
    )(place, every)


def placed_slots(routing, experts, capacity):
    rows = routing.shape[0]
    expert = lax.broadcasted_iota(jnp.int32, (rows, experts), 1)
    hits = [(routing[:, k : k + 1] == expert).astype(jnp.float32) for k in range(2)]
    row = lax.broadcasted_iota(jnp.int32, (rows, rows), 0)
    col = lax.broadcasted_iota(jnp.int32, (rows, rows), 1)
    before = (col < row).astype(jnp.bfloat16)
    earlier = dot_f32(before, (hits[0] + hits[1]).astype(jnp.bfloat16))
    slot = lax.broadcasted_iota(jnp.int32, (rows, 2 * experts * capacity), 1)
    picks = []
    for k in range(2):
        rank = jnp.sum(earlier * hits[k], axis=1, keepdims=True).astype(jnp.int32)
        place = routing[:, k : k + 1] * (2 * capacity) + rank
        picks.append([(place + half * capacity == slot).astype(jnp.bfloat16) for half in range(2)])
    return picks


def project_kernel(
    att_ref, wide_ref, narrow_ref, residual_ref, gain_ref, routing_ref, middle_ref, out_ref, *, experts, capacity
):
    half = att_ref.shape[0] // 2
    wide = jnp.concatenate([att_ref[j] for j in range(half)], axis=1)
    narrow = jnp.concatenate([att_ref[half + j] for j in range(half)], axis=1)
    mixed = dot_f32(wide, wide_ref[...]) + dot_f32(narrow, narrow_ref[...])
    middle = (residual_ref[...].astype(jnp.float32) + mixed).astype(jnp.bfloat16)
    middle_ref[...] = middle
    wider = middle.astype(jnp.float32)
    spread = jnp.mean(wider * wider, axis=1, keepdims=True)
    normed = (wider * lax.rsqrt(spread + EPS) * gain_ref[...]).astype(jnp.bfloat16)
    picks = placed_slots(routing_ref[...], experts, capacity)
    half = normed.shape[1] // 2
    over_rows = (((0,), (0,)), ((), ()))
    low = dot_f32(picks[0][0] + picks[1][0], normed[:, :half], over_rows)
    high = dot_f32(picks[0][1] + picks[1][1], normed[:, half:], over_rows)
    out_ref[...] = (low + high).astype(jnp.bfloat16)


def project(att, wide, narrow, residual, gain, routing, experts, capacity):
    rows, width = residual.shape
    return pl.pallas_call(
        functools.partial(project_kernel, experts=experts, capacity=capacity),
        out_shape=[
            jax.ShapeDtypeStruct((rows, width), jnp.bfloat16),
            jax.ShapeDtypeStruct((2 * experts * capacity, width // 2), jnp.bfloat16),
        ],
        compiler_params=pltpu.CompilerParams(vmem_limit_bytes=40 * 1024 * 1024),
        cost_estimate=pl.CostEstimate(
            flops=2 * rows * 1024 * width, transcendentals=0, bytes_accessed=2 * 1024 * width
        ),
        name="project",
    )(att, wide, narrow, residual, gain, routing)


def expert_kernel(x_ref, *rest, capacity):
    weights, (out_ref, g_ref, u_ref, d_ref, sems) = rest[:13], rest[13:]
    copies = []
    for j in range(4):
        mine = [
            pltpu.make_async_copy(weights[3 * j], g_ref.at[j], sems.at[j, 0]),
            pltpu.make_async_copy(weights[3 * j + 1], u_ref.at[j], sems.at[j, 1]),
        ]
        if j < 3:
            mine.append(pltpu.make_async_copy(weights[3 * j + 2], d_ref.at[j], sems.at[j, 2]))
        else:
            part = weights[11].shape[0]
            mine.append(pltpu.make_async_copy(weights[11], d_ref.at[j, pl.ds(0, part)], sems.at[j, 2]))
            mine.append(pltpu.make_async_copy(weights[12], d_ref.at[j, pl.ds(part, part)], sems.at[j, 3]))
        copies.append(mine)
    for mine in copies:
        for copy in mine:
            copy.start()
    x = x_ref[...]
    slots = x.shape[0]
    slot = lax.broadcasted_iota(jnp.int32, (slots // 2, slots), 0)
    from_slot = lax.broadcasted_iota(jnp.int32, (slots // 2, slots), 1)
    low_place = slot // capacity * (2 * capacity) + slot % capacity
    low = (from_slot == low_place).astype(jnp.bfloat16)
    high = (from_slot == low_place + capacity).astype(jnp.bfloat16)
    x = jnp.concatenate([dot_f32(low, x), dot_f32(high, x)], axis=1).astype(jnp.bfloat16)
    total = None
    for j in range(4):
        for copy in copies[j]:
            copy.wait()
        gate = dot_f32(x, g_ref[j])
        up = dot_f32(x, u_ref[j])
        hidden = (gate * jax.nn.sigmoid(gate) * up).astype(jnp.bfloat16)
        part = dot_f32(hidden, d_ref[j])
        total = part if total is None else total + part
    total = total.astype(jnp.bfloat16)
    half = total.shape[1] // 2
    over_rows = (((0,), (0,)), ((), ()))
    spread = dot_f32(low, total[:, :half], over_rows) + dot_f32(high, total[:, half:], over_rows)
    out_ref[...] = spread.astype(jnp.bfloat16)


def expert(x, weights, capacity):
    rows, width = x.shape[0] // 2, 2 * x.shape[1]
    units = weights[0].shape[1]
    anywhere = pl.BlockSpec(memory_space=pl.ANY)
    vmem = pl.BlockSpec(memory_space=pltpu.VMEM)
    return pl.pallas_call(
        functools.partial(expert_kernel, capacity=capacity),
        out_shape=jax.ShapeDtypeStruct(x.shape, jnp.bfloat16),
        in_specs=[vmem] + [anywhere] * 13,
        out_specs=vmem,
        scratch_shapes=[
            pltpu.VMEM((4, width, units), jnp.bfloat16),
            pltpu.VMEM((4, width, units), jnp.bfloat16),
            pltpu.VMEM((4, units, width), jnp.bfloat16),
            pltpu.SemaphoreType.DMA((4, 4)),
        ],
        compiler_params=pltpu.CompilerParams(vmem_limit_bytes=48 * 1024 * 1024),
        cost_estimate=pl.CostEstimate(
            flops=24 * rows * width * units, transcendentals=0, bytes_accessed=24 * width * units
        ),
        name="expert",
    )(x, *weights)


def combine_kernel(back_ref, middle_ref, routing_ref, weight_ref, out_ref, *, experts, capacity):
    picks = placed_slots(routing_ref[...], experts, capacity)
    back = back_ref[...]
    total = middle_ref[...].astype(jnp.float32)
    for k in range(2):
        answer = jnp.concatenate([dot_f32(picks[k][0], back), dot_f32(picks[k][1], back)], axis=1)
        total = total + weight_ref[:, k : k + 1] * answer
    out_ref[...] = total.astype(jnp.bfloat16)


def combine(back, middle, routing, weight, experts, capacity):
    return pl.pallas_call(
        functools.partial(combine_kernel, experts=experts, capacity=capacity),
        out_shape=jax.ShapeDtypeStruct(middle.shape, jnp.bfloat16),
        compiler_params=pltpu.CompilerParams(vmem_limit_bytes=24 * 1024 * 1024),
        name="combine",
    )(back, middle, routing, weight)


def body(
    residual,
    query_wide,
    key_wide,
    value_wide,
    query_narrow,
    key_narrow,
    value_narrow,
    gate_wide,
    gate_narrow,
    out_wide,
    out_narrow,
    norm_gain,
    routing,
    route_weight,
    gate_weight,
    up_weight,
    down_weight,
):
    dev_rows = query_wide.shape[0]
    own_rows, width = residual.shape
    core = lax.axis_index("core")
    is_wide = core == 0
    n_chip = lax.axis_size("chip")
    n_sp = 2 * n_chip
    n_tp = lax.axis_size("tp")
    place = jnp.full((1,), lax.axis_index(("chip", "core")), jnp.int32)

    def pick(a, b):
        return jnp.where(is_wide, a, b)

    keep = jnp.concatenate([pick(key_wide, key_narrow), pick(value_wide, value_narrow)], axis=1)
    give = jnp.concatenate([pick(key_narrow, key_wide), pick(value_narrow, value_wide)], axis=1)
    swap = [(0, 1), (1, 0)]
    got = lax.ppermute(give, "core", swap)
    q_keep = pick(query_wide, query_narrow)
    q_got = lax.ppermute(pick(query_narrow, query_wide), "core", swap)
    queries = jnp.concatenate([pick(q_keep, q_got), pick(q_got, q_keep)], axis=0)

    g, u, d = gate_weight[0], up_weight[0], down_weight[0]
    ahead = [(i, (i + 1) % n_tp) for i in range(n_tp)]
    behind = [(i, (i - 1) % n_tp) for i in range(n_tp)]
    from_left = [lax.ppermute(w, "tp", ahead) for w in (g, u, d)]
    from_right = [lax.ppermute(w, "tp", behind) for w in (g, u, d)]
    part = d.shape[0] // 2
    far = [
        lax.ppermute(from_left[0], "tp", ahead),
        lax.ppermute(from_right[1], "tp", behind),
        lax.ppermute(from_left[2][:part], "tp", ahead),
        lax.ppermute(from_right[2][part:], "tp", behind),
    ]

    chunk_a = lax.all_gather(keep, "chip", axis=0, tiled=True)
    chunk_b = lax.all_gather(got, "chip", axis=0, tiled=True)

    every = lax.all_gather(running_sums(gate_wide, gate_narrow), ("chip", "core"), axis=0)
    decay = offset_sums(place, every)

    state = attend_chunk(place, queries, decay, chunk_a, None, 0, 0, dev_rows, dev_rows, False)
    att = attend_chunk(place, queries, decay, chunk_b, state, 1, 0, dev_rows, dev_rows, True)

    att = lax.all_to_all(
        att.reshape(2 * n_tp, own_rows, HW), ("core", "tp"), split_axis=0, concat_axis=0, tiled=True
    )
    experts = n_sp
    capacity = own_rows * GROUPS // experts
    middle, outgoing = project(
        att, out_wide, out_narrow, residual, norm_gain.reshape(1, width), routing, experts, capacity
    )

    def exchange(slots):
        shape = slots.shape
        slots = slots.reshape(experts, 2 * capacity, width // 2)
        slots = lax.all_to_all(slots, ("chip", "core"), split_axis=0, concat_axis=0, tiled=True)
        return slots.reshape(shape)

    arrived = exchange(outgoing)
    answers = expert(arrived, [g, u, d, *from_left, *from_right, *far], capacity)
    returned = exchange(answers)
    return combine(returned, middle, routing, route_weight, experts, capacity)


def solution(mesh):
    n_sp, n_tp = mesh.shape["sp"], mesh.shape["tp"]
    fine = Mesh(mesh.devices.reshape(n_sp // 2, 2, n_tp), ("chip", "core", "tp"))
    sp = ("chip", "core")
    rows = P(("chip", "core", "tp"), None)
    heads = P(sp, "tp")
    placed = (
        rows,
        *([heads] * 8),
        P(),
        P(),
        P(),
        rows,
        rows,
        P(sp, None, "tp"),
        P(sp, None, "tp"),
        P(sp, "tp", None),
    )
    return jax.shard_map(body, mesh=fine, in_specs=placed, out_specs=rows, check_vma=False)
```

```python
import functools

import jax
import jax.numpy as jnp
from jax import lax
from jax.experimental import pallas as pl
from jax.experimental.pallas import tpu as pltpu
from jax.sharding import Mesh
from jax.sharding import PartitionSpec as P

HW = 128
HN = 64
GROUPS = 4
EPS = 1e-06
LOG2E = 1.4426950408889634
LOW = -1e30
TQ = 256


def dot_f32(a, b, dims=(((1,), (0,)), ((), ()))):
    return lax.dot_general(a, b, dims, preferred_element_type=jnp.float32)


def decay_line(decay_ref, chips, head, sub, row0, rows, lines):
    return jnp.concatenate(
        [
            decay_ref[2 * chip + sub, pl.ds(lines * head + (row0 + r) // 128, 1), :]
            for chip in chips
            for r in range(0, rows, 128)
        ],
        axis=1,
    )


def visit(place, q_ref, decay_ref, kv, chips, sub, row0, rows, dev_rows, held, forms):
    m_ref, l_ref, acc_ref, qh_ref = held
    chip, core = place // 2, place % 2
    queries = q_ref.shape[0]
    scale = jnp.where(core == 0, jnp.float32(HW**-0.5 * LOG2E), jnp.float32(HN**-0.5 * LOG2E))
    lines = dev_rows // 128
    earliest, latest = chips[0], chips[0]
    for c in chips[1:]:
        earliest, latest = jnp.minimum(earliest, c), jnp.maximum(latest, c)

    def run(h, masked):
        k = kv[:, :HW]
        v = kv[:, HW:]
        starts = range(0, queries, TQ)
        dk = decay_line(decay_ref, chips, h + core, sub, row0, rows, lines)
        if masked:
            own = lax.broadcasted_iota(jnp.int32, (1, rows), 1) + (sub * dev_rows + row0)
            key_place = jnp.concatenate([own + c * (2 * dev_rows) for c in chips], axis=1)

        def scores(r0):
            return dot_f32(qh_ref[h, pl.ds(r0, TQ), :], k, (((1,), (1,)), ((), ())))

        ahead = scores(0)
        for r0 in starts:
            s = ahead * scale - dk
            if r0 + TQ < queries:
                ahead = scores(r0 + TQ)
            span = pl.ds(r0, TQ)
            if masked:
                row = lax.broadcasted_iota(jnp.int32, (TQ, 1), 0) + (chip * (2 * dev_rows) + r0)
                s = jnp.where(key_place <= row, s, LOW)
            m_old = m_ref[h, span, :]
            m_new = jnp.maximum(m_old, jnp.max(s, axis=1, keepdims=True))
            alpha = jnp.exp2(m_old - m_new)
            p = jnp.exp2(s - m_new[:, :1])
            m_ref[h, span, :] = m_new
            l_ref[h, span, :] = l_ref[h, span, :] * alpha + jnp.sum(p, axis=1, keepdims=True)
            acc_ref[h, span, :] = acc_ref[h, span, :] * alpha + dot_f32(p.astype(jnp.bfloat16), v)

    for masked in forms:
        at = (earliest <= chip) & (latest >= chip) if masked else latest < chip

        @pl.when(at)
        def _():
            def head(h, carry):
                run(h, masked)
                return carry

            lax.fori_loop(0, core + 1, head, 0)


def head_queries(place, q_ref, qh_ref):
    core = place % 2
    q = q_ref[...]
    lane = lax.broadcasted_iota(jnp.int32, q.shape, 1)
    qh_ref[0] = jnp.where((core == 0) | (lane < HN), q, jnp.zeros_like(q))
    qh_ref[1] = jnp.where(lane >= HN, q, jnp.zeros_like(q))


def plane_kernel(place_ref, q_ref, decay_ref, *rest, shifts, offs, n_z, n_x, flip, row0, rows, dev_rows, first):
    n = len(shifts)
    kvs, rest = rest[:n], rest[n:]
    if not first:
        ins, rest = rest[:3], rest[3:]
    m_ref, l_ref, acc_ref, qh_ref = rest
    if first:
        m_ref[...] = jnp.full_like(m_ref, LOW)
        l_ref[...] = jnp.zeros_like(l_ref)
        acc_ref[...] = jnp.zeros_like(acc_ref)
    else:
        m_ref[...] = ins[0][...]
        l_ref[...] = ins[1][...]
        acc_ref[...] = ins[2][...]
    place = place_ref[0]
    head_queries(place, q_ref, qh_ref)
    z, x = place // 2 // n_x, place // 2 % n_x
    sub = (place % 2 + flip) % 2
    for kv_ref, shift in zip(kvs, shifts):
        plane = (z - shift + n_z) % n_z * n_x
        chips = [plane + (x + off + n_x) % n_x for off in offs]
        visit(place, q_ref, decay_ref, kv_ref, chips, sub, row0, rows, dev_rows, rest, (shift == 0,))


def attend_planes(place, q, decay, kvs, shifts, offs, sizes, flip, row0, rows, dev_rows, state):
    queries = q.shape[0]
    held = jax.ShapeDtypeStruct((2, queries, HW), jnp.float32)
    smem = pl.BlockSpec(memory_space=pltpu.SMEM)
    vmem = pl.BlockSpec(memory_space=pltpu.VMEM)
    args = [q, decay, *kvs, *(state or ())]
    keys = sum(kv.shape[0] for kv in kvs)
    return pl.pallas_call(
        functools.partial(
            plane_kernel,
            shifts=shifts,
            offs=offs,
            n_z=sizes[0],
            n_x=sizes[1],
            flip=flip,
            row0=row0,
            rows=rows,
            dev_rows=dev_rows,
            first=state is None,
        ),
        out_shape=[held] * 3,
        in_specs=[smem] + [vmem] * len(args),
        out_specs=[vmem] * 3,
        scratch_shapes=[pltpu.VMEM((2, queries, HW), jnp.bfloat16)],
        compiler_params=pltpu.CompilerParams(vmem_limit_bytes=58 * 1024 * 1024),
        cost_estimate=pl.CostEstimate(
            flops=8 * queries * keys * HW, transcendentals=2 * queries * keys, bytes_accessed=4 * keys * HW
        ),
        name="planes",
    )(place, *args)


def rest_kernel(place_ref, q_ref, decay_ref, kv_ref, *rest, flip, row0, rows, dev_rows, tiles):
    ins, (out_ref, m_ref, l_ref, acc_ref, qh_ref) = rest[:3], rest[3:]
    t = pl.program_id(0)
    place = place_ref[0]
    core = place % 2

    @pl.when(t == 0)
    def _():
        m_ref[...] = ins[0][...]
        l_ref[...] = ins[1][...]
        acc_ref[...] = ins[2][...]
        head_queries(place, q_ref, qh_ref)

    count = kv_ref.shape[0] // rows
    chips = [t * count + c for c in range(count)]
    sub = (core + flip) % 2
    held = (m_ref, l_ref, acc_ref, qh_ref)
    visit(place, q_ref, decay_ref, kv_ref, chips, sub, row0, rows, dev_rows, held, (False, True))

    @pl.when(t == tiles - 1)
    def _():
        lane = lax.broadcasted_iota(jnp.int32, q_ref.shape, 1)
        one_head = acc_ref[0] / l_ref[0]
        other = acc_ref[1] / jnp.where(core == 0, 1.0, l_ref[1])
        out_ref[...] = jnp.where((core == 0) | (lane < HN), one_head, other).astype(jnp.bfloat16)


def attend_rest(place, q, decay, kv, state, flip, row0, rows, dev_rows):
    queries = q.shape[0]
    keys = kv.shape[0]
    tile_keys = min(1024, keys)
    tiles = keys // tile_keys
    count = tile_keys // rows
    whole = pl.BlockSpec((2, queries, HW), lambda t, place: (0, 0, 0))
    q_spec = pl.BlockSpec((queries, HW), lambda t, place: (0, 0))
    held = pltpu.VMEM((2, queries, HW), jnp.float32)
    return pl.pallas_call(
        functools.partial(rest_kernel, flip=flip, row0=row0, rows=rows, dev_rows=dev_rows, tiles=tiles),
        out_shape=jax.ShapeDtypeStruct((queries, HW), jnp.bfloat16),
        grid_spec=pltpu.PrefetchScalarGridSpec(
            num_scalar_prefetch=1,
            grid=(tiles,),
            in_specs=[
                q_spec,
                pl.BlockSpec(decay.shape, lambda t, place: (0, 0, 0)),
                pl.BlockSpec((tile_keys, 2 * HW), lambda t, place: (jnp.minimum(t, place[0] // 2 // count), 0)),
                whole,
                whole,
                whole,
            ],
            out_specs=q_spec,
            scratch_shapes=[held, held, held, pltpu.VMEM((2, queries, HW), jnp.bfloat16)],
        ),
        compiler_params=pltpu.CompilerParams(
            dimension_semantics=("arbitrary",), vmem_limit_bytes=60 * 1024 * 1024
        ),
        cost_estimate=pl.CostEstimate(
            flops=8 * queries * keys * HW, transcendentals=2 * queries * keys, bytes_accessed=4 * keys * HW
        ),
        name="rest",
    )(place, q, decay, kv, *state)


def running_kernel(wide_ref, narrow_ref, out_ref):
    gates = jnp.concatenate([wide_ref[...], narrow_ref[...]], axis=0)
    kept = jnp.minimum(gates, 0.0) - jnp.log1p(jnp.exp(-jnp.abs(gates)))
    heads, rows = kept.shape
    row = lax.broadcasted_iota(jnp.int32, (rows, rows), 0)
    col = lax.broadcasted_iota(jnp.int32, (rows, rows), 1)
    upto = (row <= col).astype(jnp.float32)
    kept = jnp.concatenate([kept, jnp.zeros((8 - heads, rows), jnp.float32)], axis=0)
    sums = lax.dot_general(
        kept,
        upto,
        (((1,), (0,)), ((), ())),
        precision=lax.Precision.HIGHEST,
        preferred_element_type=jnp.float32,
    )
    out_ref[...] = jnp.zeros_like(out_ref)
    lines = rows // 128
    for h in range(heads):
        for j in range(lines):
            at = lines * h + j
            out_ref[at : at + 1, :] = sums[h : h + 1, j * 128 : (j + 1) * 128]


def running_sums(gate_wide, gate_narrow):
    return pl.pallas_call(
        running_kernel, out_shape=jax.ShapeDtypeStruct((8, 128), jnp.float32), name="running"
    )(gate_wide.T, gate_narrow.T)


def offset_kernel(place_ref, every_ref, out_ref):
    home = place_ref[0] // 2 * 2
    devices = every_ref.shape[0]
    odd = lax.broadcasted_iota(jnp.int32, (8, 128), 0) % 2 == 1
    offset = jnp.zeros((8, 128), jnp.float32)
    base = offset
    for d in range(devices):
        here = every_ref[d]
        out_ref[d] = here + offset
        base = jnp.where(home == d, offset, base)
        end = jnp.broadcast_to(here[:, 127:128], (8, 128))
        offset = offset + jnp.where(odd, end, jnp.concatenate([end[1:], end[:1]], axis=0))
    for d in range(devices):
        out_ref[d] = (out_ref[d] - base) * LOG2E


def offset_sums(place, every):
    return pl.pallas_call(
        offset_kernel,
        out_shape=jax.ShapeDtypeStruct(every.shape, jnp.float32),
        in_specs=[pl.BlockSpec(memory_space=pltpu.SMEM), pl.BlockSpec(memory_space=pltpu.VMEM)],
        name="offset",
    )(place, every)


def placed_slots(routing, experts, capacity):
    rows = routing.shape[0]
    expert = lax.broadcasted_iota(jnp.int32, (rows, experts), 1)
    hits = [(routing[:, k : k + 1] == expert).astype(jnp.float32) for k in range(2)]
    row = lax.broadcasted_iota(jnp.int32, (rows, rows), 0)
    col = lax.broadcasted_iota(jnp.int32, (rows, rows), 1)
    before = (col < row).astype(jnp.bfloat16)
    earlier = dot_f32(before, (hits[0] + hits[1]).astype(jnp.bfloat16))
    slot = lax.broadcasted_iota(jnp.int32, (rows, 2 * experts * capacity), 1)
    picks = []
    for k in range(2):
        rank = jnp.sum(earlier * hits[k], axis=1, keepdims=True).astype(jnp.int32)
        place = routing[:, k : k + 1] * (2 * capacity) + rank
        picks.append([(place + half * capacity == slot).astype(jnp.bfloat16) for half in range(2)])
    return picks


def project_kernel(
    att_ref, wide_ref, narrow_ref, residual_ref, gain_ref, routing_ref, middle_ref, out_ref, *, experts, capacity
):
    half = att_ref.shape[0] // 2
    wide = jnp.concatenate([att_ref[j] for j in range(half)], axis=1)
    narrow = jnp.concatenate([att_ref[half + j] for j in range(half)], axis=1)
    mixed = dot_f32(wide, wide_ref[...]) + dot_f32(narrow, narrow_ref[...])
    middle = (residual_ref[...].astype(jnp.float32) + mixed).astype(jnp.bfloat16)
    middle_ref[...] = middle
    wider = middle.astype(jnp.float32)
    spread = jnp.mean(wider * wider, axis=1, keepdims=True)
    normed = (wider * lax.rsqrt(spread + EPS) * gain_ref[...]).astype(jnp.bfloat16)
    picks = placed_slots(routing_ref[...], experts, capacity)
    half = normed.shape[1] // 2
    over_rows = (((0,), (0,)), ((), ()))
    low = dot_f32(picks[0][0] + picks[1][0], normed[:, :half], over_rows)
    high = dot_f32(picks[0][1] + picks[1][1], normed[:, half:], over_rows)
    out_ref[...] = (low + high).astype(jnp.bfloat16)


def project(att, wide, narrow, residual, gain, routing, experts, capacity):
    rows, width = residual.shape
    return pl.pallas_call(
        functools.partial(project_kernel, experts=experts, capacity=capacity),
        out_shape=[
            jax.ShapeDtypeStruct((rows, width), jnp.bfloat16),
            jax.ShapeDtypeStruct((2 * experts * capacity, width // 2), jnp.bfloat16),
        ],
        compiler_params=pltpu.CompilerParams(vmem_limit_bytes=40 * 1024 * 1024),
        cost_estimate=pl.CostEstimate(
            flops=2 * rows * 1024 * width, transcendentals=0, bytes_accessed=2 * 1024 * width
        ),
        name="project",
    )(att, wide, narrow, residual, gain, routing)


def expert_kernel(x_ref, *rest, capacity):
    weights, (out_ref, g_ref, u_ref, d_ref, sems) = rest[:13], rest[13:]
    copies = []
    for j in range(4):
        mine = [
            pltpu.make_async_copy(weights[3 * j], g_ref.at[j], sems.at[j, 0]),
            pltpu.make_async_copy(weights[3 * j + 1], u_ref.at[j], sems.at[j, 1]),
        ]
        if j < 3:
            mine.append(pltpu.make_async_copy(weights[3 * j + 2], d_ref.at[j], sems.at[j, 2]))
        else:
            part = weights[11].shape[0]
            mine.append(pltpu.make_async_copy(weights[11], d_ref.at[j, pl.ds(0, part)], sems.at[j, 2]))
            mine.append(pltpu.make_async_copy(weights[12], d_ref.at[j, pl.ds(part, part)], sems.at[j, 3]))
        copies.append(mine)
    for mine in copies:
        for copy in mine:
            copy.start()
    x = x_ref[...]
    slots = x.shape[0]
    slot = lax.broadcasted_iota(jnp.int32, (slots // 2, slots), 0)
    from_slot = lax.broadcasted_iota(jnp.int32, (slots // 2, slots), 1)
    low_place = slot // capacity * (2 * capacity) + slot % capacity
    low = (from_slot == low_place).astype(jnp.bfloat16)
    high = (from_slot == low_place + capacity).astype(jnp.bfloat16)
    x = jnp.concatenate([dot_f32(low, x), dot_f32(high, x)], axis=1).astype(jnp.bfloat16)
    total = None
    for j in range(4):
        for copy in copies[j]:
            copy.wait()
        gate = dot_f32(x, g_ref[j])
        up = dot_f32(x, u_ref[j])
        hidden = (gate * jax.nn.sigmoid(gate) * up).astype(jnp.bfloat16)
        part = dot_f32(hidden, d_ref[j])
        total = part if total is None else total + part
    total = total.astype(jnp.bfloat16)
    half = total.shape[1] // 2
    over_rows = (((0,), (0,)), ((), ()))
    spread = dot_f32(low, total[:, :half], over_rows) + dot_f32(high, total[:, half:], over_rows)
    out_ref[...] = spread.astype(jnp.bfloat16)


def expert(x, weights, capacity):
    rows, width = x.shape[0] // 2, 2 * x.shape[1]
    units = weights[0].shape[1]
    anywhere = pl.BlockSpec(memory_space=pl.ANY)
    vmem = pl.BlockSpec(memory_space=pltpu.VMEM)
    return pl.pallas_call(
        functools.partial(expert_kernel, capacity=capacity),
        out_shape=jax.ShapeDtypeStruct(x.shape, jnp.bfloat16),
        in_specs=[vmem] + [anywhere] * 13,
        out_specs=vmem,
        scratch_shapes=[
            pltpu.VMEM((4, width, units), jnp.bfloat16),
            pltpu.VMEM((4, width, units), jnp.bfloat16),
            pltpu.VMEM((4, units, width), jnp.bfloat16),
            pltpu.SemaphoreType.DMA((4, 4)),
        ],
        compiler_params=pltpu.CompilerParams(vmem_limit_bytes=48 * 1024 * 1024),
        cost_estimate=pl.CostEstimate(
            flops=24 * rows * width * units, transcendentals=0, bytes_accessed=24 * width * units
        ),
        name="expert",
    )(x, *weights)


def combine_kernel(back_ref, middle_ref, routing_ref, weight_ref, out_ref, *, experts, capacity):
    picks = placed_slots(routing_ref[...], experts, capacity)
    back = back_ref[...]
    total = middle_ref[...].astype(jnp.float32)
    for k in range(2):
        answer = jnp.concatenate([dot_f32(picks[k][0], back), dot_f32(picks[k][1], back)], axis=1)
        total = total + weight_ref[:, k : k + 1] * answer
    out_ref[...] = total.astype(jnp.bfloat16)


def combine(back, middle, routing, weight, experts, capacity):
    return pl.pallas_call(
        functools.partial(combine_kernel, experts=experts, capacity=capacity),
        out_shape=jax.ShapeDtypeStruct(middle.shape, jnp.bfloat16),
        compiler_params=pltpu.CompilerParams(vmem_limit_bytes=24 * 1024 * 1024),
        name="combine",
    )(back, middle, routing, weight)


def body(
    residual,
    query_wide,
    key_wide,
    value_wide,
    query_narrow,
    key_narrow,
    value_narrow,
    gate_wide,
    gate_narrow,
    out_wide,
    out_narrow,
    norm_gain,
    routing,
    route_weight,
    gate_weight,
    up_weight,
    down_weight,
):
    dev_rows = query_wide.shape[0]
    own_rows, width = residual.shape
    core = lax.axis_index("core")
    is_wide = core == 0
    n_z, n_x, n_tp = lax.axis_size("z"), lax.axis_size("x"), lax.axis_size("tp")
    n_sp = 2 * n_z * n_x
    sp = ("z", "x", "core")
    place = jnp.full((1,), lax.axis_index(sp), jnp.int32)

    def pick(a, b):
        return jnp.where(is_wide, a, b)

    keep = jnp.concatenate([pick(key_wide, key_narrow), pick(value_wide, value_narrow)], axis=1)
    give = jnp.concatenate([pick(key_narrow, key_wide), pick(value_narrow, value_wide)], axis=1)
    swap = [(0, 1), (1, 0)]
    got = lax.ppermute(give, "core", swap)
    q_keep = pick(query_wide, query_narrow)
    q_got = lax.ppermute(pick(query_narrow, query_wide), "core", swap)
    queries = jnp.concatenate([pick(q_keep, q_got), pick(q_got, q_keep)], axis=0)

    g, u, d = gate_weight[0], up_weight[0], down_weight[0]
    ahead = [(i, (i + 1) % n_tp) for i in range(n_tp)]
    behind = [(i, (i - 1) % n_tp) for i in range(n_tp)]
    from_left = [lax.ppermute(w, "tp", ahead) for w in (g, u, d)]
    from_right = [lax.ppermute(w, "tp", behind) for w in (g, u, d)]
    part = d.shape[0] // 2
    far = [
        lax.ppermute(from_left[0], "tp", ahead),
        lax.ppermute(from_right[1], "tp", behind),
        lax.ppermute(from_left[2][:part], "tp", ahead),
        lax.ppermute(from_right[2][part:], "tp", behind),
    ]

    gathered = lax.all_gather(keep, ("z", "x"), axis=0, tiled=True)
    offs = (0, -1, 1, 2)
    line = [got] + [
        lax.ppermute(got, "x", [((i + off) % n_x, i) for i in range(n_x)]) for off in offs[1:]
    ]
    plane = jnp.concatenate(line, axis=0)
    up = [(i, (i + 1) % n_z) for i in range(n_z)]
    down = [(i, (i - 1) % n_z) for i in range(n_z)]
    planes = [[(plane, 0)]]
    lower = upper = plane
    for step in range(1, n_z // 2 + 1):
        lower = lax.ppermute(lower, "z", up)
        if step < n_z // 2:
            upper = lax.ppermute(upper, "z", down)
            planes.append([(lower, step), (upper, -step)])
        else:
            planes.append([(lower, step)])

    every = running_sums(gate_wide, gate_narrow)
    for axis in ("core", "x", "z"):
        every = lax.all_gather(every, axis, axis=0)
    decay = offset_sums(place, every.reshape(n_sp, 8, 128))

    state = None
    for pieces in planes:
        state = attend_planes(
            place,
            queries,
            decay,
            [piece for piece, _ in pieces],
            [shift for _, shift in pieces],
            offs,
            (n_z, n_x),
            1,
            0,
            dev_rows,
            dev_rows,
            state,
        )
    att = attend_rest(place, queries, decay, gathered, state, 0, 0, dev_rows, dev_rows)

    att = lax.all_to_all(
        att.reshape(2 * n_tp, own_rows, HW), ("core", "tp"), split_axis=0, concat_axis=0, tiled=True
    )
    experts = n_sp
    capacity = own_rows * GROUPS // experts
    middle, outgoing = project(
        att, out_wide, out_narrow, residual, norm_gain.reshape(1, width), routing, experts, capacity
    )

    def exchange(slots):
        shape = slots.shape
        slots = slots.reshape(experts, 2 * capacity, width // 2)
        slots = lax.all_to_all(slots, sp, split_axis=0, concat_axis=0, tiled=True)
        return slots.reshape(shape)

    arrived = exchange(outgoing)
    answers = expert(arrived, [g, u, d, *from_left, *from_right, *far], capacity)
    returned = exchange(answers)
    return combine(returned, middle, routing, route_weight, experts, capacity)


def solution(mesh):
    n_sp, n_tp = mesh.shape["sp"], mesh.shape["tp"]
    n_x = 4
    fine = Mesh(mesh.devices.reshape(n_sp // 2 // n_x, n_x, 2, n_tp), ("z", "x", "core", "tp"))
    sp = ("z", "x", "core")
    rows = P((*sp, "tp"), None)
    heads = P(sp, "tp")
    placed = (
        rows,
        *([heads] * 8),
        P(),
        P(),
        P(),
        rows,
        rows,
        P(sp, None, "tp"),
        P(sp, None, "tp"),
        P(sp, "tp", None),
    )
    return jax.shard_map(body, mesh=fine, in_specs=placed, out_specs=rows, check_vma=False)
```

```python
import functools

import jax
import jax.numpy as jnp
from jax import lax
from jax.experimental import pallas as pl
from jax.experimental.pallas import tpu as pltpu
from jax.sharding import Mesh
from jax.sharding import PartitionSpec as P

HW = 128
HN = 64
GROUPS = 4
EPS = 1e-06
LOG2E = 1.4426950408889634
LOW = -1e30
TQ = 256


def dot_f32(a, b, dims=(((1,), (0,)), ((), ()))):
    return lax.dot_general(a, b, dims, preferred_element_type=jnp.float32)


def decay_line(decay_ref, chips, head, sub, row0, rows, lines):
    return jnp.concatenate(
        [
            decay_ref[2 * chip + sub, pl.ds(lines * head + (row0 + r) // 128, 1), :]
            for chip in chips
            for r in range(0, rows, 128)
        ],
        axis=1,
    )


def visit(place, q_ref, decay_ref, kv, chips, sub, row0, rows, dev_rows, held, forms):
    m_ref, l_ref, acc_ref, qh_ref = held
    chip, core = place // 2, place % 2
    queries = q_ref.shape[0]
    scale = jnp.where(core == 0, jnp.float32(HW**-0.5 * LOG2E), jnp.float32(HN**-0.5 * LOG2E))
    lines = dev_rows // 128
    earliest, latest = chips[0], chips[0]
    for c in chips[1:]:
        earliest, latest = jnp.minimum(earliest, c), jnp.maximum(latest, c)

    def run(h, masked):
        k = kv[:, :HW]
        v = kv[:, HW:]
        starts = range(0, queries, TQ)
        dk = decay_line(decay_ref, chips, h + core, sub, row0, rows, lines)
        if masked:
            own = lax.broadcasted_iota(jnp.int32, (1, rows), 1) + (sub * dev_rows + row0)
            key_place = jnp.concatenate([own + c * (2 * dev_rows) for c in chips], axis=1)

        def scores(r0):
            return dot_f32(qh_ref[h, pl.ds(r0, TQ), :], k, (((1,), (1,)), ((), ())))

        ahead = scores(0)
        for r0 in starts:
            s = ahead * scale - dk
            if r0 + TQ < queries:
                ahead = scores(r0 + TQ)
            span = pl.ds(r0, TQ)
            if masked:
                row = lax.broadcasted_iota(jnp.int32, (TQ, 1), 0) + (chip * (2 * dev_rows) + r0)
                s = jnp.where(key_place <= row, s, LOW)
            m_old = m_ref[h, span, :]
            m_new = jnp.maximum(m_old, jnp.max(s, axis=1, keepdims=True))
            alpha = jnp.exp2(m_old - m_new)
            p = jnp.exp2(s - m_new[:, :1])
            m_ref[h, span, :] = m_new
            l_ref[h, span, :] = l_ref[h, span, :] * alpha + jnp.sum(p, axis=1, keepdims=True)
            acc_ref[h, span, :] = acc_ref[h, span, :] * alpha + dot_f32(p.astype(jnp.bfloat16), v)

    for masked in forms:
        at = (earliest <= chip) & (latest >= chip) if masked else latest < chip

        @pl.when(at)
        def _():
            def head(h, carry):
                run(h, masked)
                return carry

            lax.fori_loop(0, core + 1, head, 0)


def head_queries(place, q_ref, qh_ref):
    core = place % 2
    q = q_ref[...]
    lane = lax.broadcasted_iota(jnp.int32, q.shape, 1)
    qh_ref[0] = jnp.where((core == 0) | (lane < HN), q, jnp.zeros_like(q))
    qh_ref[1] = jnp.where(lane >= HN, q, jnp.zeros_like(q))


def plane_kernel(place_ref, q_ref, decay_ref, *rest, shifts, offs, n_z, n_x, flip, row0, rows, dev_rows, first):
    n = len(shifts)
    kvs, rest = rest[:n], rest[n:]
    if not first:
        ins, rest = rest[:3], rest[3:]
    m_ref, l_ref, acc_ref, qh_ref = rest
    if first:
        m_ref[...] = jnp.full_like(m_ref, LOW)
        l_ref[...] = jnp.zeros_like(l_ref)
        acc_ref[...] = jnp.zeros_like(acc_ref)
    else:
        m_ref[...] = ins[0][...]
        l_ref[...] = ins[1][...]
        acc_ref[...] = ins[2][...]
    place = place_ref[0]
    head_queries(place, q_ref, qh_ref)
    z, x = place // 2 // n_x, place // 2 % n_x
    sub = (place % 2 + flip) % 2
    for kv_ref, shift in zip(kvs, shifts):
        plane = (z - shift + n_z) % n_z * n_x
        chips = [plane + (x + off + n_x) % n_x for off in offs]
        visit(place, q_ref, decay_ref, kv_ref, chips, sub, row0, rows, dev_rows, rest, (shift == 0,))


def attend_planes(place, q, decay, kvs, shifts, offs, sizes, flip, row0, rows, dev_rows, state):
    queries = q.shape[0]
    held = jax.ShapeDtypeStruct((2, queries, HW), jnp.float32)
    smem = pl.BlockSpec(memory_space=pltpu.SMEM)
    vmem = pl.BlockSpec(memory_space=pltpu.VMEM)
    args = [q, decay, *kvs, *(state or ())]
    keys = sum(kv.shape[0] for kv in kvs)
    return pl.pallas_call(
        functools.partial(
            plane_kernel,
            shifts=shifts,
            offs=offs,
            n_z=sizes[0],
            n_x=sizes[1],
            flip=flip,
            row0=row0,
            rows=rows,
            dev_rows=dev_rows,
            first=state is None,
        ),
        out_shape=[held] * 3,
        in_specs=[smem] + [vmem] * len(args),
        out_specs=[vmem] * 3,
        scratch_shapes=[pltpu.VMEM((2, queries, HW), jnp.bfloat16)],
        compiler_params=pltpu.CompilerParams(vmem_limit_bytes=24 * 1024 * 1024),
        cost_estimate=pl.CostEstimate(
            flops=8 * queries * keys * HW, transcendentals=2 * queries * keys, bytes_accessed=4 * keys * HW
        ),
        name="planes",
    )(place, *args)


def rest_kernel(place_ref, q_ref, decay_ref, kv_ref, *rest, flip, row0, rows, dev_rows, tiles):
    ins, (out_ref, m_ref, l_ref, acc_ref, qh_ref) = rest[:3], rest[3:]
    t = pl.program_id(0)
    place = place_ref[0]
    core = place % 2

    @pl.when(t == 0)
    def _():
        m_ref[...] = ins[0][...]
        l_ref[...] = ins[1][...]
        acc_ref[...] = ins[2][...]
        head_queries(place, q_ref, qh_ref)

    count = kv_ref.shape[0] // rows
    chips = [t * count + c for c in range(count)]
    sub = (core + flip) % 2
    held = (m_ref, l_ref, acc_ref, qh_ref)
    visit(place, q_ref, decay_ref, kv_ref, chips, sub, row0, rows, dev_rows, held, (False, True))

    @pl.when(t == tiles - 1)
    def _():
        lane = lax.broadcasted_iota(jnp.int32, q_ref.shape, 1)
        one_head = acc_ref[0] / l_ref[0]
        other = acc_ref[1] / jnp.where(core == 0, 1.0, l_ref[1])
        out_ref[...] = jnp.where((core == 0) | (lane < HN), one_head, other).astype(jnp.bfloat16)


def attend_rest(place, q, decay, kv, state, flip, row0, rows, dev_rows):
    queries = q.shape[0]
    keys = kv.shape[0]
    tile_keys = min(1024, keys)
    tiles = keys // tile_keys
    count = tile_keys // rows
    whole = pl.BlockSpec((2, queries, HW), lambda t, place: (0, 0, 0))
    q_spec = pl.BlockSpec((queries, HW), lambda t, place: (0, 0))
    held = pltpu.VMEM((2, queries, HW), jnp.float32)
    return pl.pallas_call(
        functools.partial(rest_kernel, flip=flip, row0=row0, rows=rows, dev_rows=dev_rows, tiles=tiles),
        out_shape=jax.ShapeDtypeStruct((queries, HW), jnp.bfloat16),
        grid_spec=pltpu.PrefetchScalarGridSpec(
            num_scalar_prefetch=1,
            grid=(tiles,),
            in_specs=[
                q_spec,
                pl.BlockSpec(decay.shape, lambda t, place: (0, 0, 0)),
                pl.BlockSpec((tile_keys, 2 * HW), lambda t, place: (jnp.minimum(t, place[0] // 2 // count), 0)),
                whole,
                whole,
                whole,
            ],
            out_specs=q_spec,
            scratch_shapes=[held, held, held, pltpu.VMEM((2, queries, HW), jnp.bfloat16)],
        ),
        compiler_params=pltpu.CompilerParams(
            dimension_semantics=("arbitrary",), vmem_limit_bytes=60 * 1024 * 1024
        ),
        cost_estimate=pl.CostEstimate(
            flops=8 * queries * keys * HW, transcendentals=2 * queries * keys, bytes_accessed=4 * keys * HW
        ),
        name="rest",
    )(place, q, decay, kv, *state)


def running_kernel(wide_ref, narrow_ref, out_ref):
    gates = jnp.concatenate([wide_ref[...], narrow_ref[...]], axis=0)
    kept = jnp.minimum(gates, 0.0) - jnp.log1p(jnp.exp(-jnp.abs(gates)))
    heads, rows = kept.shape
    row = lax.broadcasted_iota(jnp.int32, (rows, rows), 0)
    col = lax.broadcasted_iota(jnp.int32, (rows, rows), 1)
    upto = (row <= col).astype(jnp.float32)
    kept = jnp.concatenate([kept, jnp.zeros((8 - heads, rows), jnp.float32)], axis=0)
    sums = lax.dot_general(
        kept,
        upto,
        (((1,), (0,)), ((), ())),
        precision=lax.Precision.HIGHEST,
        preferred_element_type=jnp.float32,
    )
    out_ref[...] = jnp.zeros_like(out_ref)
    lines = rows // 128
    for h in range(heads):
        for j in range(lines):
            at = lines * h + j
            out_ref[at : at + 1, :] = sums[h : h + 1, j * 128 : (j + 1) * 128]


def running_sums(gate_wide, gate_narrow):
    return pl.pallas_call(
        running_kernel,
        out_shape=jax.ShapeDtypeStruct((8, 128), jnp.float32),
        compiler_params=pltpu.CompilerParams(vmem_limit_bytes=8 * 1024 * 1024),
        name="running",
    )(gate_wide.T, gate_narrow.T)


def offset_kernel(place_ref, *rest, n_z, n_x, offs):
    pieces, (out_ref, abs_ref) = rest[:n_z], rest[n_z:]
    chip = place_ref[0] // 2
    z, x = chip // n_x, chip % n_x
    for k in range(n_z):
        for i, off in enumerate(offs):
            at = (z - k + n_z) % n_z * n_x + (x + off + n_x) % n_x
            abs_ref[2 * at] = pieces[k][2 * i]
            abs_ref[2 * at + 1] = pieces[k][2 * i + 1]
    devices = abs_ref.shape[0]
    odd = lax.broadcasted_iota(jnp.int32, (8, 128), 0) % 2 == 1
    offset = jnp.zeros((8, 128), jnp.float32)
    base = offset
    for d in range(devices):
        here = abs_ref[d]
        out_ref[d] = here + offset
        base = jnp.where(2 * chip == d, offset, base)
        end = jnp.broadcast_to(here[:, 127:128], (8, 128))
        offset = offset + jnp.where(odd, end, jnp.concatenate([end[1:], end[:1]], axis=0))
    for d in range(devices):
        out_ref[d] = (out_ref[d] - base) * LOG2E


def offset_sums(place, pieces, n_x, offs):
    every = (len(pieces) * pieces[0].shape[0], 8, 128)
    smem = pl.BlockSpec(memory_space=pltpu.SMEM)
    vmem = pl.BlockSpec(memory_space=pltpu.VMEM)
    return pl.pallas_call(
        functools.partial(offset_kernel, n_z=len(pieces), n_x=n_x, offs=offs),
        out_shape=jax.ShapeDtypeStruct(every, jnp.float32),
        in_specs=[smem] + [vmem] * len(pieces),
        scratch_shapes=[pltpu.VMEM(every, jnp.float32)],
        compiler_params=pltpu.CompilerParams(vmem_limit_bytes=8 * 1024 * 1024),
        name="offset",
    )(place, *pieces)


def placed_slots(routing, experts, capacity):
    rows = routing.shape[0]
    expert = lax.broadcasted_iota(jnp.int32, (rows, experts), 1)
    hits = [(routing[:, k : k + 1] == expert).astype(jnp.float32) for k in range(2)]
    row = lax.broadcasted_iota(jnp.int32, (rows, rows), 0)
    col = lax.broadcasted_iota(jnp.int32, (rows, rows), 1)
    before = (col < row).astype(jnp.bfloat16)
    earlier = dot_f32(before, (hits[0] + hits[1]).astype(jnp.bfloat16))
    slot = lax.broadcasted_iota(jnp.int32, (rows, 2 * experts * capacity), 1)
    picks = []
    for k in range(2):
        rank = jnp.sum(earlier * hits[k], axis=1, keepdims=True).astype(jnp.int32)
        place = routing[:, k : k + 1] * (2 * capacity) + rank
        picks.append([(place + half * capacity == slot).astype(jnp.bfloat16) for half in range(2)])
    return picks


def project_kernel(
    att_ref, wide_ref, narrow_ref, residual_ref, gain_ref, routing_ref, middle_ref, out_ref, *, experts, capacity
):
    half = att_ref.shape[0] // 2
    wide = jnp.concatenate([att_ref[j] for j in range(half)], axis=1)
    narrow = jnp.concatenate([att_ref[half + j] for j in range(half)], axis=1)
    mixed = dot_f32(wide, wide_ref[...]) + dot_f32(narrow, narrow_ref[...])
    middle = (residual_ref[...].astype(jnp.float32) + mixed).astype(jnp.bfloat16)
    middle_ref[...] = middle
    wider = middle.astype(jnp.float32)
    spread = jnp.mean(wider * wider, axis=1, keepdims=True)
    normed = (wider * lax.rsqrt(spread + EPS) * gain_ref[...]).astype(jnp.bfloat16)
    picks = placed_slots(routing_ref[...], experts, capacity)
    half = normed.shape[1] // 2
    over_rows = (((0,), (0,)), ((), ()))
    low = dot_f32(picks[0][0] + picks[1][0], normed[:, :half], over_rows)
    high = dot_f32(picks[0][1] + picks[1][1], normed[:, half:], over_rows)
    out_ref[...] = (low + high).astype(jnp.bfloat16)


def project(att, wide, narrow, residual, gain, routing, experts, capacity):
    rows, width = residual.shape
    return pl.pallas_call(
        functools.partial(project_kernel, experts=experts, capacity=capacity),
        out_shape=[
            jax.ShapeDtypeStruct((rows, width), jnp.bfloat16),
            jax.ShapeDtypeStruct((2 * experts * capacity, width // 2), jnp.bfloat16),
        ],
        compiler_params=pltpu.CompilerParams(vmem_limit_bytes=40 * 1024 * 1024),
        cost_estimate=pl.CostEstimate(
            flops=2 * rows * 1024 * width, transcendentals=0, bytes_accessed=2 * 1024 * width
        ),
        name="project",
    )(att, wide, narrow, residual, gain, routing)


def expert_kernel(x_ref, *rest, capacity):
    weights, (out_ref, g_ref, u_ref, d_ref, sems) = rest[:13], rest[13:]
    copies = []
    for j in range(4):
        mine = [
            pltpu.make_async_copy(weights[3 * j], g_ref.at[j], sems.at[j, 0]),
            pltpu.make_async_copy(weights[3 * j + 1], u_ref.at[j], sems.at[j, 1]),
        ]
        if j < 3:
            mine.append(pltpu.make_async_copy(weights[3 * j + 2], d_ref.at[j], sems.at[j, 2]))
        else:
            part = weights[11].shape[0]
            mine.append(pltpu.make_async_copy(weights[11], d_ref.at[j, pl.ds(0, part)], sems.at[j, 2]))
            mine.append(pltpu.make_async_copy(weights[12], d_ref.at[j, pl.ds(part, part)], sems.at[j, 3]))
        copies.append(mine)
    for mine in copies:
        for copy in mine:
            copy.start()
    x = x_ref[...]
    slots = x.shape[0]
    slot = lax.broadcasted_iota(jnp.int32, (slots // 2, slots), 0)
    from_slot = lax.broadcasted_iota(jnp.int32, (slots // 2, slots), 1)
    low_place = slot // capacity * (2 * capacity) + slot % capacity
    low = (from_slot == low_place).astype(jnp.bfloat16)
    high = (from_slot == low_place + capacity).astype(jnp.bfloat16)
    x = jnp.concatenate([dot_f32(low, x), dot_f32(high, x)], axis=1).astype(jnp.bfloat16)
    total = None
    for j in range(4):
        for copy in copies[j]:
            copy.wait()
        gate = dot_f32(x, g_ref[j])
        up = dot_f32(x, u_ref[j])
        hidden = (gate * jax.nn.sigmoid(gate) * up).astype(jnp.bfloat16)
        part = dot_f32(hidden, d_ref[j])
        total = part if total is None else total + part
    total = total.astype(jnp.bfloat16)
    half = total.shape[1] // 2
    over_rows = (((0,), (0,)), ((), ()))
    spread = dot_f32(low, total[:, :half], over_rows) + dot_f32(high, total[:, half:], over_rows)
    out_ref[...] = spread.astype(jnp.bfloat16)


def expert(x, weights, capacity):
    rows, width = x.shape[0] // 2, 2 * x.shape[1]
    units = weights[0].shape[1]
    anywhere = pl.BlockSpec(memory_space=pl.ANY)
    vmem = pl.BlockSpec(memory_space=pltpu.VMEM)
    return pl.pallas_call(
        functools.partial(expert_kernel, capacity=capacity),
        out_shape=jax.ShapeDtypeStruct(x.shape, jnp.bfloat16),
        in_specs=[vmem] + [anywhere] * 13,
        out_specs=vmem,
        scratch_shapes=[
            pltpu.VMEM((4, width, units), jnp.bfloat16),
            pltpu.VMEM((4, width, units), jnp.bfloat16),
            pltpu.VMEM((4, units, width), jnp.bfloat16),
            pltpu.SemaphoreType.DMA((4, 4)),
        ],
        compiler_params=pltpu.CompilerParams(vmem_limit_bytes=48 * 1024 * 1024),
        cost_estimate=pl.CostEstimate(
            flops=24 * rows * width * units, transcendentals=0, bytes_accessed=24 * width * units
        ),
        name="expert",
    )(x, *weights)


def combine_kernel(back_ref, middle_ref, routing_ref, weight_ref, out_ref, *, experts, capacity):
    picks = placed_slots(routing_ref[...], experts, capacity)
    back = back_ref[...]
    total = middle_ref[...].astype(jnp.float32)
    for k in range(2):
        answer = jnp.concatenate([dot_f32(picks[k][0], back), dot_f32(picks[k][1], back)], axis=1)
        total = total + weight_ref[:, k : k + 1] * answer
    out_ref[...] = total.astype(jnp.bfloat16)


def combine(back, middle, routing, weight, experts, capacity):
    return pl.pallas_call(
        functools.partial(combine_kernel, experts=experts, capacity=capacity),
        out_shape=jax.ShapeDtypeStruct(middle.shape, jnp.bfloat16),
        compiler_params=pltpu.CompilerParams(vmem_limit_bytes=24 * 1024 * 1024),
        name="combine",
    )(back, middle, routing, weight)


def body(
    residual,
    query_wide,
    key_wide,
    value_wide,
    query_narrow,
    key_narrow,
    value_narrow,
    gate_wide,
    gate_narrow,
    out_wide,
    out_narrow,
    norm_gain,
    routing,
    route_weight,
    gate_weight,
    up_weight,
    down_weight,
):
    dev_rows = query_wide.shape[0]
    own_rows, width = residual.shape
    core = lax.axis_index("core")
    is_wide = core == 0
    n_z, n_x, n_tp = lax.axis_size("z"), lax.axis_size("x"), lax.axis_size("tp")
    n_sp = 2 * n_z * n_x
    sp = ("z", "x", "core")
    place = jnp.full((1,), lax.axis_index(sp), jnp.int32)

    def pick(a, b):
        return jnp.where(is_wide, a, b)

    keep = jnp.concatenate([pick(key_wide, key_narrow), pick(value_wide, value_narrow)], axis=1)
    give = jnp.concatenate([pick(key_narrow, key_wide), pick(value_narrow, value_wide)], axis=1)
    swap = [(0, 1), (1, 0)]
    got = lax.ppermute(give, "core", swap)
    q_keep = pick(query_wide, query_narrow)
    q_got = lax.ppermute(pick(query_narrow, query_wide), "core", swap)
    queries = jnp.concatenate([pick(q_keep, q_got), pick(q_got, q_keep)], axis=0)

    g, u, d = gate_weight[0], up_weight[0], down_weight[0]
    ahead = [(i, (i + 1) % n_tp) for i in range(n_tp)]
    behind = [(i, (i - 1) % n_tp) for i in range(n_tp)]
    from_left = [lax.ppermute(w, "tp", ahead) for w in (g, u, d)]
    from_right = [lax.ppermute(w, "tp", behind) for w in (g, u, d)]
    part = d.shape[0] // 2
    far = [
        lax.ppermute(from_left[0], "tp", ahead),
        lax.ppermute(from_right[1], "tp", behind),
        lax.ppermute(from_left[2][:part], "tp", ahead),
        lax.ppermute(from_right[2][part:], "tp", behind),
    ]

    gathered = lax.all_gather(keep, ("z", "x"), axis=0, tiled=True)
    offs = (0, -1, 1, 2)
    line = [got] + [
        lax.ppermute(got, "x", [((i + off) % n_x, i) for i in range(n_x)]) for off in offs[1:]
    ]
    plane = jnp.concatenate(line, axis=0)
    up = [(i, (i + 1) % n_z) for i in range(n_z)]
    down = [(i, (i - 1) % n_z) for i in range(n_z)]
    planes = [[(plane, 0)]]
    lower = upper = plane
    for step in range(1, n_z // 2 + 1):
        lower = lax.ppermute(lower, "z", up)
        if step < n_z // 2:
            upper = lax.ppermute(upper, "z", down)
            planes.append([(lower, step), (upper, -step)])
        else:
            planes.append([(lower, step)])

    sums = lax.all_gather(running_sums(gate_wide, gate_narrow), "core", axis=0)
    sums = [sums] + [
        lax.ppermute(sums, "x", [((i + off) % n_x, i) for i in range(n_x)]) for off in offs[1:]
    ]
    sums = jnp.concatenate(sums, axis=0)
    sums = [sums] + [
        lax.ppermute(sums, "z", [((i - k) % n_z, i) for i in range(n_z)]) for k in range(1, n_z)
    ]
    decay = offset_sums(place, sums, n_x, offs)

    state = None
    for pieces in planes:
        state = attend_planes(
            place,
            queries,
            decay,
            [piece for piece, _ in pieces],
            [shift for _, shift in pieces],
            offs,
            (n_z, n_x),
            1,
            0,
            dev_rows,
            dev_rows,
            state,
        )
    att = attend_rest(place, queries, decay, gathered, state, 0, 0, dev_rows, dev_rows)

    att = lax.all_to_all(
        att.reshape(2 * n_tp, own_rows, HW), ("core", "tp"), split_axis=0, concat_axis=0, tiled=True
    )
    experts = n_sp
    capacity = own_rows * GROUPS // experts
    middle, outgoing = project(
        att, out_wide, out_narrow, residual, norm_gain.reshape(1, width), routing, experts, capacity
    )

    def exchange(slots):
        shape = slots.shape
        slots = slots.reshape(experts, 2 * capacity, width // 2)
        slots = lax.all_to_all(slots, sp, split_axis=0, concat_axis=0, tiled=True)
        return slots.reshape(shape)

    arrived = exchange(outgoing)
    answers = expert(arrived, [g, u, d, *from_left, *from_right, *far], capacity)
    returned = exchange(answers)
    return combine(returned, middle, routing, route_weight, experts, capacity)


def solution(mesh):
    n_sp, n_tp = mesh.shape["sp"], mesh.shape["tp"]
    n_x = 4
    fine = Mesh(mesh.devices.reshape(n_sp // 2 // n_x, n_x, 2, n_tp), ("z", "x", "core", "tp"))
    sp = ("z", "x", "core")
    rows = P((*sp, "tp"), None)
    heads = P(sp, "tp")
    placed = (
        rows,
        *([heads] * 8),
        P(),
        P(),
        P(),
        rows,
        rows,
        P(sp, None, "tp"),
        P(sp, None, "tp"),
        P(sp, "tp", None),
    )
    return jax.shard_map(body, mesh=fine, in_specs=placed, out_specs=rows, check_vma=False)
```

```python
import functools

import jax
import jax.numpy as jnp
from jax import lax
from jax.experimental import pallas as pl
from jax.experimental.pallas import tpu as pltpu
from jax.sharding import Mesh
from jax.sharding import PartitionSpec as P

HW = 128
HN = 64
GROUPS = 4
EPS = 1e-06
LOG2E = 1.4426950408889634
LOW = -1e30
TQ = 256
OFFLOADED = 128
REST_MIB = 60


def dot_f32(a, b, dims=(((1,), (0,)), ((), ()))):
    return lax.dot_general(a, b, dims, preferred_element_type=jnp.float32)


def decay_line(decay_ref, blocks, head, lines):
    return jnp.concatenate(
        [
            decay_ref[2 * chip + sub, pl.ds(lines * head + (row0 + r) // 128, 1), :]
            for chip, sub, row0, rows in blocks
            for r in range(0, rows, 128)
        ],
        axis=1,
    )


def visit(place, q_ref, decay_ref, kv, blocks, dev_rows, held, forms):
    m_ref, l_ref, acc_ref, qh_ref = held
    chip, core = place // 2, place % 2
    queries = q_ref.shape[0]
    scale = jnp.where(core == 0, jnp.float32(HW**-0.5 * LOG2E), jnp.float32(HN**-0.5 * LOG2E))
    lines = dev_rows // 128
    earliest = latest = blocks[0][0]
    for block in blocks[1:]:
        earliest, latest = jnp.minimum(earliest, block[0]), jnp.maximum(latest, block[0])

    def run(h, masked):
        k = kv[:, :HW]
        v = kv[:, HW:]
        starts = range(0, queries, TQ)
        dk = decay_line(decay_ref, blocks, h + core, lines)
        if masked:
            key_place = jnp.concatenate(
                [
                    lax.broadcasted_iota(jnp.int32, (1, rows), 1) + ((2 * c + sub) * dev_rows + row0)
                    for c, sub, row0, rows in blocks
                ],
                axis=1,
            )

        def scores(r0):
            return dot_f32(qh_ref[h, pl.ds(r0, TQ), :], k, (((1,), (1,)), ((), ())))

        ahead = scores(0)
        for r0 in starts:
            s = ahead * scale - dk
            if r0 + TQ < queries:
                ahead = scores(r0 + TQ)
            span = pl.ds(r0, TQ)
            if masked:
                row = lax.broadcasted_iota(jnp.int32, (TQ, 1), 0) + (chip * (2 * dev_rows) + r0)
                s = jnp.where(key_place <= row, s, LOW)
            m_old = m_ref[h, span, :]
            m_new = jnp.maximum(m_old, jnp.max(s, axis=1, keepdims=True))
            alpha = jnp.exp2(m_old - m_new)
            p = jnp.exp2(s - m_new[:, :1])
            m_ref[h, span, :] = m_new
            l_ref[h, span, :] = l_ref[h, span, :] * alpha + jnp.sum(p, axis=1, keepdims=True)
            acc_ref[h, span, :] = acc_ref[h, span, :] * alpha + dot_f32(p.astype(jnp.bfloat16), v)

    for masked in forms:
        at = (earliest <= chip) & (latest >= chip) if masked else latest < chip

        @pl.when(at)
        def _():
            def head(h, carry):
                run(h, masked)
                return carry

            lax.fori_loop(0, core + 1, head, 0)


def head_queries(place, q_ref, qh_ref):
    core = place % 2
    q = q_ref[...]
    lane = lax.broadcasted_iota(jnp.int32, q.shape, 1)
    qh_ref[0] = jnp.where((core == 0) | (lane < HN), q, jnp.zeros_like(q))
    qh_ref[1] = jnp.where(lane >= HN, q, jnp.zeros_like(q))


def take_state(ins, held):
    m_ref, l_ref, acc_ref = held
    if ins:
        for source, target in zip(ins, held):
            target[...] = source[...]
    else:
        m_ref[...] = jnp.full_like(m_ref, LOW)
        l_ref[...] = jnp.zeros_like(l_ref)
        acc_ref[...] = jnp.zeros_like(acc_ref)


def plane_kernel(place_ref, q_ref, decay_ref, *rest, pieces, n_z, n_x, dev_rows, first, last):
    n = len(pieces)
    kvs, rest = rest[:n], rest[n:]
    ins = ()
    if not first:
        ins, rest = rest[:3], rest[3:]
    if last:
        out_ref, rest = rest[0], rest[1:]
    held, qh_ref = rest[:3], rest[3]
    take_state(ins, held)
    place = place_ref[0]
    core = place % 2
    head_queries(place, q_ref, qh_ref)
    z, x = place // 2 // n_x, place // 2 % n_x
    for kv_ref, (shift, offs, parts) in zip(kvs, pieces):
        plane = (z - shift + n_z) % n_z * n_x
        blocks = [
            (plane + (x + off + n_x) % n_x, (core + flip) % 2, row0, rows)
            for off in offs
            for flip, row0, rows in parts
        ]
        visit(place, q_ref, decay_ref, kv_ref, blocks, dev_rows, rest, (shift == 0,))
    if last:
        _, l_ref, acc_ref = held
        lane = lax.broadcasted_iota(jnp.int32, q_ref.shape, 1)
        one_head = acc_ref[0] / l_ref[0]
        other = acc_ref[1] / jnp.where(core == 0, 1.0, l_ref[1])
        out_ref[...] = jnp.where((core == 0) | (lane < HN), one_head, other).astype(jnp.bfloat16)


def attend_planes(place, q, decay, kvs, pieces, sizes, dev_rows, state, last):
    queries = q.shape[0]
    shape = (2, queries, HW)
    smem = pl.BlockSpec(memory_space=pltpu.SMEM)
    vmem = pl.BlockSpec(memory_space=pltpu.VMEM)
    args = [q, decay, *kvs, *(state or ())]
    keys = sum(kv.shape[0] for kv in kvs)
    scratch = [pltpu.VMEM(shape, jnp.bfloat16)]
    if last:
        out_shape, out_specs = jax.ShapeDtypeStruct((queries, HW), jnp.bfloat16), vmem
        scratch = [pltpu.VMEM(shape, jnp.float32)] * 3 + scratch
    else:
        out_shape, out_specs = [jax.ShapeDtypeStruct(shape, jnp.float32)] * 3, [vmem] * 3
    return pl.pallas_call(
        functools.partial(
            plane_kernel,
            pieces=pieces,
            n_z=sizes[0],
            n_x=sizes[1],
            dev_rows=dev_rows,
            first=state is None,
            last=last,
        ),
        out_shape=out_shape,
        in_specs=[smem] + [vmem] * len(args),
        out_specs=out_specs,
        scratch_shapes=scratch,
        compiler_params=pltpu.CompilerParams(vmem_limit_bytes=26 * 1024 * 1024),
        cost_estimate=pl.CostEstimate(
            flops=8 * queries * keys * HW, transcendentals=2 * queries * keys, bytes_accessed=4 * keys * HW
        ),
        name="planes",
    )(place, *args)


def rest_kernel(place_ref, q_ref, decay_ref, kv_ref, *rest, row0, rows, dev_rows):
    ins, held, qh_ref = rest[:3], rest[3:6], rest[6]
    t = pl.program_id(0)
    place = place_ref[0]

    @pl.when(t == 0)
    def _():
        take_state(ins, held)
        head_queries(place, q_ref, qh_ref)

    count = kv_ref.shape[0] // rows
    blocks = [(t * count + c, place % 2, row0, rows) for c in range(count)]
    visit(place, q_ref, decay_ref, kv_ref, blocks, dev_rows, rest[3:], (False, True))


def attend_rest(place, q, decay, kv, state, row0, rows, dev_rows):
    queries = q.shape[0]
    keys = kv.shape[0]
    tile_keys = min(1024, keys)
    tiles = keys // tile_keys
    count = tile_keys // rows
    whole = pl.BlockSpec((2, queries, HW), lambda t, place: (0, 0, 0))
    return pl.pallas_call(
        functools.partial(rest_kernel, row0=row0, rows=rows, dev_rows=dev_rows),
        out_shape=[jax.ShapeDtypeStruct((2, queries, HW), jnp.float32)] * 3,
        grid_spec=pltpu.PrefetchScalarGridSpec(
            num_scalar_prefetch=1,
            grid=(tiles,),
            in_specs=[
                pl.BlockSpec((queries, HW), lambda t, place: (0, 0)),
                pl.BlockSpec(decay.shape, lambda t, place: (0, 0, 0)),
                pl.BlockSpec((tile_keys, 2 * HW), lambda t, place: (jnp.minimum(t, place[0] // 2 // count), 0)),
                whole,
                whole,
                whole,
            ],
            out_specs=[whole] * 3,
            scratch_shapes=[pltpu.VMEM((2, queries, HW), jnp.bfloat16)],
        ),
        compiler_params=pltpu.CompilerParams(
            dimension_semantics=("arbitrary",), vmem_limit_bytes=REST_MIB * 1024 * 1024
        ),
        cost_estimate=pl.CostEstimate(
            flops=8 * queries * keys * HW, transcendentals=2 * queries * keys, bytes_accessed=4 * keys * HW
        ),
        name="rest",
    )(place, q, decay, kv, *state)


def running_kernel(wide_ref, narrow_ref, out_ref):
    gates = jnp.concatenate([wide_ref[...], narrow_ref[...]], axis=0)
    kept = jnp.minimum(gates, 0.0) - jnp.log1p(jnp.exp(-jnp.abs(gates)))
    heads, rows = kept.shape
    row = lax.broadcasted_iota(jnp.int32, (rows, rows), 0)
    col = lax.broadcasted_iota(jnp.int32, (rows, rows), 1)
    upto = (row <= col).astype(jnp.float32)
    kept = jnp.concatenate([kept, jnp.zeros((8 - heads, rows), jnp.float32)], axis=0)
    sums = lax.dot_general(
        kept,
        upto,
        (((1,), (0,)), ((), ())),
        precision=lax.Precision.HIGHEST,
        preferred_element_type=jnp.float32,
    )
    out_ref[...] = jnp.zeros_like(out_ref)
    lines = rows // 128
    for h in range(heads):
        for j in range(lines):
            at = lines * h + j
            out_ref[at : at + 1, :] = sums[h : h + 1, j * 128 : (j + 1) * 128]


def running_sums(gate_wide, gate_narrow):
    return pl.pallas_call(
        running_kernel,
        out_shape=jax.ShapeDtypeStruct((8, 128), jnp.float32),
        compiler_params=pltpu.CompilerParams(vmem_limit_bytes=8 * 1024 * 1024),
        name="running",
    )(gate_wide.T, gate_narrow.T)


def offset_kernel(place_ref, *rest, n_z, n_x, offs):
    pieces, (out_ref, abs_ref) = rest[:n_z], rest[n_z:]
    chip = place_ref[0] // 2
    z, x = chip // n_x, chip % n_x
    for k in range(n_z):
        for i, off in enumerate(offs):
            at = (z - k + n_z) % n_z * n_x + (x + off + n_x) % n_x
            abs_ref[2 * at] = pieces[k][2 * i]
            abs_ref[2 * at + 1] = pieces[k][2 * i + 1]
    devices = abs_ref.shape[0]
    odd = lax.broadcasted_iota(jnp.int32, (8, 128), 0) % 2 == 1
    offset = jnp.zeros((8, 128), jnp.float32)
    base = offset
    for d in range(devices):
        here = abs_ref[d]
        out_ref[d] = here + offset
        base = jnp.where(2 * chip == d, offset, base)
        end = jnp.broadcast_to(here[:, 127:128], (8, 128))
        offset = offset + jnp.where(odd, end, jnp.concatenate([end[1:], end[:1]], axis=0))
    for d in range(devices):
        out_ref[d] = (out_ref[d] - base) * LOG2E


def offset_sums(place, pieces, n_x, offs):
    every = (len(pieces) * pieces[0].shape[0], 8, 128)
    smem = pl.BlockSpec(memory_space=pltpu.SMEM)
    vmem = pl.BlockSpec(memory_space=pltpu.VMEM)
    return pl.pallas_call(
        functools.partial(offset_kernel, n_z=len(pieces), n_x=n_x, offs=offs),
        out_shape=jax.ShapeDtypeStruct(every, jnp.float32),
        in_specs=[smem] + [vmem] * len(pieces),
        scratch_shapes=[pltpu.VMEM(every, jnp.float32)],
        compiler_params=pltpu.CompilerParams(vmem_limit_bytes=8 * 1024 * 1024),
        name="offset",
    )(place, *pieces)


def placed_slots(routing, experts, capacity):
    rows = routing.shape[0]
    expert = lax.broadcasted_iota(jnp.int32, (rows, experts), 1)
    hits = [(routing[:, k : k + 1] == expert).astype(jnp.float32) for k in range(2)]
    row = lax.broadcasted_iota(jnp.int32, (rows, rows), 0)
    col = lax.broadcasted_iota(jnp.int32, (rows, rows), 1)
    before = (col < row).astype(jnp.bfloat16)
    earlier = dot_f32(before, (hits[0] + hits[1]).astype(jnp.bfloat16))
    slot = lax.broadcasted_iota(jnp.int32, (rows, 2 * experts * capacity), 1)
    picks = []
    for k in range(2):
        rank = jnp.sum(earlier * hits[k], axis=1, keepdims=True).astype(jnp.int32)
        place = routing[:, k : k + 1] * (2 * capacity) + rank
        picks.append([(place + half * capacity == slot).astype(jnp.bfloat16) for half in range(2)])
    return picks


def project_kernel(
    att_ref,
    wide_hbm,
    narrow_hbm,
    residual_ref,
    gain_ref,
    routing_ref,
    middle_ref,
    out_ref,
    wide_ref,
    narrow_ref,
    sems,
    *,
    experts,
    capacity,
):
    copies = [
        pltpu.make_async_copy(wide_hbm, wide_ref, sems.at[0]),
        pltpu.make_async_copy(narrow_hbm, narrow_ref, sems.at[1]),
    ]
    for copy in copies:
        copy.start()
    picks = placed_slots(routing_ref[...], experts, capacity)
    half = att_ref.shape[0] // 2
    wide = jnp.concatenate([att_ref[j] for j in range(half)], axis=1)
    narrow = jnp.concatenate([att_ref[half + j] for j in range(half)], axis=1)
    copies[0].wait()
    mixed = dot_f32(wide, wide_ref[...])
    copies[1].wait()
    mixed = mixed + dot_f32(narrow, narrow_ref[...])
    middle = (residual_ref[...].astype(jnp.float32) + mixed).astype(jnp.bfloat16)
    middle_ref[...] = middle
    wider = middle.astype(jnp.float32)
    spread = jnp.mean(wider * wider, axis=1, keepdims=True)
    normed = (wider * lax.rsqrt(spread + EPS) * gain_ref[...]).astype(jnp.bfloat16)
    half = normed.shape[1] // 2
    over_rows = (((0,), (0,)), ((), ()))
    low = dot_f32(picks[0][0] + picks[1][0], normed[:, :half], over_rows)
    high = dot_f32(picks[0][1] + picks[1][1], normed[:, half:], over_rows)
    out_ref[...] = (low + high).astype(jnp.bfloat16)


def project(att, wide, narrow, residual, gain, routing, experts, capacity):
    rows, width = residual.shape
    anywhere = pl.BlockSpec(memory_space=pltpu.HBM)
    vmem = pl.BlockSpec(memory_space=pltpu.VMEM)
    return pl.pallas_call(
        functools.partial(project_kernel, experts=experts, capacity=capacity),
        out_shape=[
            jax.ShapeDtypeStruct((rows, width), jnp.bfloat16),
            jax.ShapeDtypeStruct((2 * experts * capacity, width // 2), jnp.bfloat16),
        ],
        in_specs=[vmem, anywhere, anywhere, vmem, vmem, vmem],
        out_specs=[vmem, vmem],
        scratch_shapes=[
            pltpu.VMEM(wide.shape, wide.dtype),
            pltpu.VMEM(narrow.shape, narrow.dtype),
            pltpu.SemaphoreType.DMA((2,)),
        ],
        compiler_params=pltpu.CompilerParams(vmem_limit_bytes=24 * 1024 * 1024),
        cost_estimate=pl.CostEstimate(
            flops=2 * rows * 1024 * width, transcendentals=0, bytes_accessed=2 * 1024 * width
        ),
        name="project",
    )(att, wide, narrow, residual, gain, routing)


def expert_kernel(x_ref, *rest, capacity):
    weights, (out_ref, g_ref, u_ref, d_ref, sems) = rest[:13], rest[13:]
    copies = []
    for j in range(4):
        mine = [
            pltpu.make_async_copy(weights[3 * j], g_ref.at[j], sems.at[j, 0]),
            pltpu.make_async_copy(weights[3 * j + 1], u_ref.at[j], sems.at[j, 1]),
        ]
        if j < 3:
            mine.append(pltpu.make_async_copy(weights[3 * j + 2], d_ref.at[j], sems.at[j, 2]))
        else:
            part = weights[11].shape[0]
            mine.append(pltpu.make_async_copy(weights[11], d_ref.at[j, pl.ds(0, part)], sems.at[j, 2]))
            mine.append(pltpu.make_async_copy(weights[12], d_ref.at[j, pl.ds(part, part)], sems.at[j, 3]))
        copies.append(mine)
    for mine in copies:
        for copy in mine:
            copy.start()
    x = x_ref[...]
    slots = x.shape[0]
    slot = lax.broadcasted_iota(jnp.int32, (slots // 2, slots), 0)
    from_slot = lax.broadcasted_iota(jnp.int32, (slots // 2, slots), 1)
    low_place = slot // capacity * (2 * capacity) + slot % capacity
    low = (from_slot == low_place).astype(jnp.bfloat16)
    high = (from_slot == low_place + capacity).astype(jnp.bfloat16)
    x = jnp.concatenate([dot_f32(low, x), dot_f32(high, x)], axis=1).astype(jnp.bfloat16)
    total = None
    for j in range(4):
        for copy in copies[j]:
            copy.wait()
        gate = dot_f32(x, g_ref[j])
        up = dot_f32(x, u_ref[j])
        hidden = (gate * jax.nn.sigmoid(gate) * up).astype(jnp.bfloat16)
        part = dot_f32(hidden, d_ref[j])
        total = part if total is None else total + part
    total = total.astype(jnp.bfloat16)
    half = total.shape[1] // 2
    over_rows = (((0,), (0,)), ((), ()))
    spread = dot_f32(low, total[:, :half], over_rows) + dot_f32(high, total[:, half:], over_rows)
    out_ref[...] = spread.astype(jnp.bfloat16)


def expert(x, weights, capacity):
    rows, width = x.shape[0] // 2, 2 * x.shape[1]
    units = weights[0].shape[1]
    anywhere = pl.BlockSpec(memory_space=pl.ANY)
    vmem = pl.BlockSpec(memory_space=pltpu.VMEM)
    return pl.pallas_call(
        functools.partial(expert_kernel, capacity=capacity),
        out_shape=jax.ShapeDtypeStruct(x.shape, jnp.bfloat16),
        in_specs=[vmem] + [anywhere] * 13,
        out_specs=vmem,
        scratch_shapes=[
            pltpu.VMEM((4, width, units), jnp.bfloat16),
            pltpu.VMEM((4, width, units), jnp.bfloat16),
            pltpu.VMEM((4, units, width), jnp.bfloat16),
            pltpu.SemaphoreType.DMA((4, 4)),
        ],
        compiler_params=pltpu.CompilerParams(vmem_limit_bytes=48 * 1024 * 1024),
        cost_estimate=pl.CostEstimate(
            flops=24 * rows * width * units, transcendentals=0, bytes_accessed=24 * width * units
        ),
        name="expert",
    )(x, *weights)


def combine_kernel(back_ref, middle_ref, routing_ref, weight_ref, out_ref, *, experts, capacity):
    picks = placed_slots(routing_ref[...], experts, capacity)
    back = back_ref[...]
    total = middle_ref[...].astype(jnp.float32)
    for k in range(2):
        answer = jnp.concatenate([dot_f32(picks[k][0], back), dot_f32(picks[k][1], back)], axis=1)
        total = total + weight_ref[:, k : k + 1] * answer
    out_ref[...] = total.astype(jnp.bfloat16)


def combine(back, middle, routing, weight, experts, capacity):
    return pl.pallas_call(
        functools.partial(combine_kernel, experts=experts, capacity=capacity),
        out_shape=jax.ShapeDtypeStruct(middle.shape, jnp.bfloat16),
        compiler_params=pltpu.CompilerParams(vmem_limit_bytes=24 * 1024 * 1024),
        name="combine",
    )(back, middle, routing, weight)


def body(
    residual,
    query_wide,
    key_wide,
    value_wide,
    query_narrow,
    key_narrow,
    value_narrow,
    gate_wide,
    gate_narrow,
    out_wide,
    out_narrow,
    norm_gain,
    routing,
    route_weight,
    gate_weight,
    up_weight,
    down_weight,
):
    dev_rows = query_wide.shape[0]
    own_rows, width = residual.shape
    core = lax.axis_index("core")
    is_wide = core == 0
    n_z, n_x, n_tp = lax.axis_size("z"), lax.axis_size("x"), lax.axis_size("tp")
    n_sp = 2 * n_z * n_x
    sp = ("z", "x", "core")
    place = jnp.full((1,), lax.axis_index(sp), jnp.int32)

    def pick(a, b):
        return jnp.where(is_wide, a, b)

    keep = [
        jnp.concatenate([pick(key_wide[span], key_narrow[span]), pick(value_wide[span], value_narrow[span])], axis=1)
        for span in (slice(0, OFFLOADED), slice(OFFLOADED, None))
    ]
    keep[0] = lax.optimization_barrier(keep[0])
    give = jnp.concatenate([pick(key_narrow, key_wide), pick(value_narrow, value_wide)], axis=1)
    swap = [(0, 1), (1, 0)]
    got = lax.ppermute(give, "core", swap)
    q_keep = pick(query_wide, query_narrow)
    q_got = lax.ppermute(pick(query_narrow, query_wide), "core", swap)
    queries = jnp.concatenate([pick(q_keep, q_got), pick(q_got, q_keep)], axis=0)

    g, u, d = gate_weight[0], up_weight[0], down_weight[0]
    ahead = [(i, (i + 1) % n_tp) for i in range(n_tp)]
    behind = [(i, (i - 1) % n_tp) for i in range(n_tp)]
    from_left = [lax.ppermute(w, "tp", ahead) for w in (g, u, d)]
    from_right = [lax.ppermute(w, "tp", behind) for w in (g, u, d)]
    part = d.shape[0] // 2
    far = [
        lax.ppermute(from_left[0], "tp", ahead),
        lax.ppermute(from_right[1], "tp", behind),
        lax.ppermute(from_left[2][:part], "tp", ahead),
        lax.ppermute(from_right[2][part:], "tp", behind),
    ]

    gathered = lax.all_gather(keep[0], ("z", "x"), axis=0, tiled=True)
    mine = jnp.concatenate([got, keep[1]], axis=0)
    parts = [(1, 0, dev_rows), (0, OFFLOADED, dev_rows - OFFLOADED)]
    offs = (0, -1, 1, 2)
    line = [mine] + [
        lax.ppermute(mine, "x", [((i + off) % n_x, i) for i in range(n_x)]) for off in offs[1:]
    ]
    plane = jnp.concatenate(line, axis=0)
    half = plane.shape[0] // 2
    up = [(i, (i + 1) % n_z) for i in range(n_z)]
    down = [(i, (i - 1) % n_z) for i in range(n_z)]
    planes = [[(plane, (0, offs, parts))]]
    lower = upper = plane
    last = n_z // 2
    for step in range(1, last + 1):
        if step == last:
            lower, upper = lower[:half], upper[half:]
        lower = lax.ppermute(lower, "z", up)
        upper = lax.ppermute(upper, "z", down)
        if step < last:
            planes.append([(lower, (step, offs, parts)), (upper, (-step, offs, parts))])
        else:
            planes.append([(lower, (step, offs[:2], parts)), (upper, (step, offs[2:], parts))])

    sums = lax.all_gather(running_sums(gate_wide, gate_narrow), "core", axis=0)
    sums = [sums] + [
        lax.ppermute(sums, "x", [((i + off) % n_x, i) for i in range(n_x)]) for off in offs[1:]
    ]
    sums = jnp.concatenate(sums, axis=0)
    sums = [sums] + [
        lax.ppermute(sums, "z", [((i - k) % n_z, i) for i in range(n_z)]) for k in range(1, n_z)
    ]
    decay = offset_sums(place, sums, n_x, offs)

    state = None
    for step, pieces in enumerate(planes):
        if step == last - 1:
            state = attend_rest(place, queries, decay, gathered, state, 0, OFFLOADED, dev_rows)
        state = attend_planes(
            place,
            queries,
            decay,
            [piece for piece, _ in pieces],
            [layout for _, layout in pieces],
            (n_z, n_x),
            dev_rows,
            state,
            step == last,
        )
    att = state

    att = lax.all_to_all(
        att.reshape(2 * n_tp, own_rows, HW), ("core", "tp"), split_axis=0, concat_axis=0, tiled=True
    )
    experts = n_sp
    capacity = own_rows * GROUPS // experts
    middle, outgoing = project(
        att, out_wide, out_narrow, residual, norm_gain.reshape(1, width), routing, experts, capacity
    )

    def exchange(slots):
        shape = slots.shape
        slots = slots.reshape(experts, 2 * capacity, width // 2)
        slots = lax.all_to_all(slots, sp, split_axis=0, concat_axis=0, tiled=True)
        return slots.reshape(shape)

    arrived = exchange(outgoing)
    answers = expert(arrived, [g, u, d, *from_left, *from_right, *far], capacity)
    returned = exchange(answers)
    return combine(returned, middle, routing, route_weight, experts, capacity)


def solution(mesh):
    n_sp, n_tp = mesh.shape["sp"], mesh.shape["tp"]
    n_x = 4
    fine = Mesh(mesh.devices.reshape(n_sp // 2 // n_x, n_x, 2, n_tp), ("z", "x", "core", "tp"))
    sp = ("z", "x", "core")
    rows = P((*sp, "tp"), None)
    heads = P(sp, "tp")
    placed = (
        rows,
        *([heads] * 8),
        P(),
        P(),
        P(),
        rows,
        rows,
        P(sp, None, "tp"),
        P(sp, None, "tp"),
        P(sp, "tp", None),
    )
    return jax.shard_map(body, mesh=fine, in_specs=placed, out_specs=rows, check_vma=False)
```

```python
import functools

import jax
import jax.numpy as jnp
from jax import lax
from jax.experimental import pallas as pl
from jax.experimental.pallas import tpu as pltpu
from jax.sharding import Mesh
from jax.sharding import PartitionSpec as P

HW = 128
HN = 64
GROUPS = 4
EPS = 1e-06
LOG2E = 1.4426950408889634
LOW = -1e30
TQ = 256
OFFLOADED = 128
TILE = 1024


def dot_f32(a, b, dims=(((1,), (0,)), ((), ()))):
    return lax.dot_general(a, b, dims, preferred_element_type=jnp.float32)


def decay_line(decay_ref, blocks, head, lines):
    return jnp.concatenate(
        [
            decay_ref[2 * chip + sub, pl.ds(lines * head + (row0 + r) // 128, 1), :]
            for chip, sub, row0, rows in blocks
            for r in range(0, rows, 128)
        ],
        axis=1,
    )


def visit(place, q_ref, decay_ref, kv, blocks, dev_rows, held, forms):
    m_ref, l_ref, acc_ref, qh_ref = held
    chip, core = place // 2, place % 2
    queries = q_ref.shape[0]
    scale = jnp.where(core == 0, jnp.float32(HW**-0.5 * LOG2E), jnp.float32(HN**-0.5 * LOG2E))
    lines = dev_rows // 128
    earliest = latest = blocks[0][0]
    for block in blocks[1:]:
        earliest, latest = jnp.minimum(earliest, block[0]), jnp.maximum(latest, block[0])

    def run(h, masked):
        k = kv[:, :HW]
        v = kv[:, HW:]
        starts = range(0, queries, TQ)
        dk = decay_line(decay_ref, blocks, h + core, lines)
        if masked:
            key_place = jnp.concatenate(
                [
                    lax.broadcasted_iota(jnp.int32, (1, rows), 1) + ((2 * c + sub) * dev_rows + row0)
                    for c, sub, row0, rows in blocks
                ],
                axis=1,
            )

        def scores(r0):
            return dot_f32(qh_ref[h, pl.ds(r0, TQ), :], k, (((1,), (1,)), ((), ())))

        ahead = scores(0)
        for r0 in starts:
            s = ahead * scale - dk
            if r0 + TQ < queries:
                ahead = scores(r0 + TQ)
            span = pl.ds(r0, TQ)
            if masked:
                row = lax.broadcasted_iota(jnp.int32, (TQ, 1), 0) + (chip * (2 * dev_rows) + r0)
                s = jnp.where(key_place <= row, s, LOW)
            m_old = m_ref[h, span, :]
            m_new = jnp.maximum(m_old, jnp.max(s, axis=1, keepdims=True))
            alpha = jnp.exp2(m_old - m_new)
            p = jnp.exp2(s - m_new[:, :1])
            m_ref[h, span, :] = m_new
            l_ref[h, span, :] = l_ref[h, span, :] * alpha + jnp.sum(p, axis=1, keepdims=True)
            acc_ref[h, span, :] = acc_ref[h, span, :] * alpha + dot_f32(p.astype(jnp.bfloat16), v)

    for masked in forms:
        at = (earliest <= chip) & (latest >= chip) if masked else latest < chip

        @pl.when(at)
        def _():
            def head(h, carry):
                run(h, masked)
                return carry

            lax.fori_loop(0, core + 1, head, 0)


def head_queries(place, q_ref, qh_ref):
    core = place % 2
    q = q_ref[...]
    lane = lax.broadcasted_iota(jnp.int32, q.shape, 1)
    qh_ref[0] = jnp.where((core == 0) | (lane < HN), q, jnp.zeros_like(q))
    qh_ref[1] = jnp.where(lane >= HN, q, jnp.zeros_like(q))


def take_state(ins, held):
    m_ref, l_ref, acc_ref = held
    if ins:
        for source, target in zip(ins, held):
            target[...] = source[...]
    else:
        m_ref[...] = jnp.full_like(m_ref, LOW)
        l_ref[...] = jnp.zeros_like(l_ref)
        acc_ref[...] = jnp.zeros_like(acc_ref)


def plane_kernel(place_ref, q_ref, decay_ref, *rest, pieces, gathered, n_z, n_x, dev_rows, first, last):
    n = len(pieces)
    kvs, rest = rest[:n], rest[n:]
    if gathered:
        every_ref, rest = rest[0], rest[1:]
    ins = ()
    if not first:
        ins, rest = rest[:3], rest[3:]
    if last:
        out_ref, rest = rest[0], rest[1:]
    held, qh_ref = rest[:3], rest[3]
    take_state(ins, held)
    place = place_ref[0]
    core = place % 2
    head_queries(place, q_ref, qh_ref)
    z, x = place // 2 // n_x, place // 2 % n_x
    for kv_ref, (shift, offs, parts) in zip(kvs, pieces):
        plane = (z - shift + n_z) % n_z * n_x
        blocks = [
            (plane + (x + off + n_x) % n_x, (core + flip) % 2, row0, rows)
            for off in offs
            for flip, row0, rows in parts
        ]
        visit(place, q_ref, decay_ref, kv_ref, blocks, dev_rows, rest, (shift == 0,))
    if gathered:
        tile = min(TILE, every_ref.shape[0])
        count = tile // gathered

        def one(t, carry):
            blocks = [(t * count + c, core, 0, gathered) for c in range(count)]
            kv = every_ref.at[pl.ds(pl.multiple_of(t * tile, tile), tile), :]
            visit(place, q_ref, decay_ref, kv, blocks, dev_rows, rest, (False, True))
            return carry

        lax.fori_loop(0, place // 2 // count + 1, one, 0)
    if last:
        _, l_ref, acc_ref = held
        lane = lax.broadcasted_iota(jnp.int32, q_ref.shape, 1)
        one_head = acc_ref[0] / l_ref[0]
        other = acc_ref[1] / jnp.where(core == 0, 1.0, l_ref[1])
        out_ref[...] = jnp.where((core == 0) | (lane < HN), one_head, other).astype(jnp.bfloat16)


def attend_planes(place, q, decay, kvs, pieces, gathered, sizes, dev_rows, state, last):
    queries = q.shape[0]
    shape = (2, queries, HW)
    smem = pl.BlockSpec(memory_space=pltpu.SMEM)
    vmem = pl.BlockSpec(memory_space=pltpu.VMEM)
    args = [q, decay, *kvs, *(state or ())]
    keys = sum(kv.shape[0] for kv in kvs)
    scratch = [pltpu.VMEM(shape, jnp.bfloat16)]
    if last:
        out_shape, out_specs = jax.ShapeDtypeStruct((queries, HW), jnp.bfloat16), vmem
        scratch = [pltpu.VMEM(shape, jnp.float32)] * 3 + scratch
    else:
        out_shape, out_specs = [jax.ShapeDtypeStruct(shape, jnp.float32)] * 3, [vmem] * 3
    return pl.pallas_call(
        functools.partial(
            plane_kernel,
            pieces=pieces,
            gathered=gathered,
            n_z=sizes[0],
            n_x=sizes[1],
            dev_rows=dev_rows,
            first=state is None,
            last=last,
        ),
        out_shape=out_shape,
        in_specs=[smem] + [vmem] * len(args),
        out_specs=out_specs,
        scratch_shapes=scratch,
        compiler_params=pltpu.CompilerParams(vmem_limit_bytes=26 * 1024 * 1024),
        cost_estimate=pl.CostEstimate(
            flops=8 * queries * keys * HW, transcendentals=2 * queries * keys, bytes_accessed=4 * keys * HW
        ),
        name="planes",
    )(place, *args)


def running_kernel(wide_ref, narrow_ref, out_ref):
    gates = jnp.concatenate([wide_ref[...], narrow_ref[...]], axis=0)
    kept = jnp.minimum(gates, 0.0) - jnp.log1p(jnp.exp(-jnp.abs(gates)))
    heads, rows = kept.shape
    row = lax.broadcasted_iota(jnp.int32, (rows, rows), 0)
    col = lax.broadcasted_iota(jnp.int32, (rows, rows), 1)
    upto = (row <= col).astype(jnp.float32)
    kept = jnp.concatenate([kept, jnp.zeros((8 - heads, rows), jnp.float32)], axis=0)
    sums = lax.dot_general(
        kept,
        upto,
        (((1,), (0,)), ((), ())),
        precision=lax.Precision.HIGHEST,
        preferred_element_type=jnp.float32,
    )
    out_ref[...] = jnp.zeros_like(out_ref)
    lines = rows // 128
    for h in range(heads):
        for j in range(lines):
            at = lines * h + j
            out_ref[at : at + 1, :] = sums[h : h + 1, j * 128 : (j + 1) * 128]


def running_sums(gate_wide, gate_narrow):
    return pl.pallas_call(
        running_kernel,
        out_shape=jax.ShapeDtypeStruct((8, 128), jnp.float32),
        compiler_params=pltpu.CompilerParams(vmem_limit_bytes=8 * 1024 * 1024),
        name="running",
    )(gate_wide.T, gate_narrow.T)


def offset_kernel(place_ref, *rest, n_z, n_x, offs):
    pieces, (out_ref, abs_ref) = rest[:n_z], rest[n_z:]
    chip = place_ref[0] // 2
    z, x = chip // n_x, chip % n_x
    for k in range(n_z):
        for i, off in enumerate(offs):
            at = (z - k + n_z) % n_z * n_x + (x + off + n_x) % n_x
            abs_ref[2 * at] = pieces[k][2 * i]
            abs_ref[2 * at + 1] = pieces[k][2 * i + 1]
    devices = abs_ref.shape[0]
    odd = lax.broadcasted_iota(jnp.int32, (8, 128), 0) % 2 == 1
    offset = jnp.zeros((8, 128), jnp.float32)
    base = offset
    for d in range(devices):
        here = abs_ref[d]
        out_ref[d] = here + offset
        base = jnp.where(2 * chip == d, offset, base)
        end = jnp.broadcast_to(here[:, 127:128], (8, 128))
        offset = offset + jnp.where(odd, end, jnp.concatenate([end[1:], end[:1]], axis=0))
    for d in range(devices):
        out_ref[d] = (out_ref[d] - base) * LOG2E


def offset_sums(place, pieces, n_x, offs):
    every = (len(pieces) * pieces[0].shape[0], 8, 128)
    smem = pl.BlockSpec(memory_space=pltpu.SMEM)
    vmem = pl.BlockSpec(memory_space=pltpu.VMEM)
    return pl.pallas_call(
        functools.partial(offset_kernel, n_z=len(pieces), n_x=n_x, offs=offs),
        out_shape=jax.ShapeDtypeStruct(every, jnp.float32),
        in_specs=[smem] + [vmem] * len(pieces),
        scratch_shapes=[pltpu.VMEM(every, jnp.float32)],
        compiler_params=pltpu.CompilerParams(vmem_limit_bytes=8 * 1024 * 1024),
        name="offset",
    )(place, *pieces)


def placed_slots(routing, experts, capacity):
    rows = routing.shape[0]
    expert = lax.broadcasted_iota(jnp.int32, (rows, experts), 1)
    hits = [(routing[:, k : k + 1] == expert).astype(jnp.float32) for k in range(2)]
    row = lax.broadcasted_iota(jnp.int32, (rows, rows), 0)
    col = lax.broadcasted_iota(jnp.int32, (rows, rows), 1)
    before = (col < row).astype(jnp.bfloat16)
    earlier = dot_f32(before, (hits[0] + hits[1]).astype(jnp.bfloat16))
    slot = lax.broadcasted_iota(jnp.int32, (rows, 2 * experts * capacity), 1)
    picks = []
    for k in range(2):
        rank = jnp.sum(earlier * hits[k], axis=1, keepdims=True).astype(jnp.int32)
        place = routing[:, k : k + 1] * (2 * capacity) + rank
        picks.append([(place + half * capacity == slot).astype(jnp.bfloat16) for half in range(2)])
    return picks


def project_kernel(
    att_ref, wide_ref, narrow_ref, residual_ref, gain_ref, routing_ref, middle_ref, out_ref, *, experts, capacity
):
    half = att_ref.shape[0] // 2
    wide = jnp.concatenate([att_ref[j] for j in range(half)], axis=1)
    narrow = jnp.concatenate([att_ref[half + j] for j in range(half)], axis=1)
    mixed = dot_f32(wide, wide_ref[...]) + dot_f32(narrow, narrow_ref[...])
    middle = (residual_ref[...].astype(jnp.float32) + mixed).astype(jnp.bfloat16)
    middle_ref[...] = middle
    wider = middle.astype(jnp.float32)
    spread = jnp.mean(wider * wider, axis=1, keepdims=True)
    normed = (wider * lax.rsqrt(spread + EPS) * gain_ref[...]).astype(jnp.bfloat16)
    picks = placed_slots(routing_ref[...], experts, capacity)
    half = normed.shape[1] // 2
    over_rows = (((0,), (0,)), ((), ()))
    low = dot_f32(picks[0][0] + picks[1][0], normed[:, :half], over_rows)
    high = dot_f32(picks[0][1] + picks[1][1], normed[:, half:], over_rows)
    out_ref[...] = (low + high).astype(jnp.bfloat16)


def project(att, wide, narrow, residual, gain, routing, experts, capacity):
    rows, width = residual.shape
    return pl.pallas_call(
        functools.partial(project_kernel, experts=experts, capacity=capacity),
        out_shape=[
            jax.ShapeDtypeStruct((rows, width), jnp.bfloat16),
            jax.ShapeDtypeStruct((2 * experts * capacity, width // 2), jnp.bfloat16),
        ],
        compiler_params=pltpu.CompilerParams(vmem_limit_bytes=40 * 1024 * 1024),
        cost_estimate=pl.CostEstimate(
            flops=2 * rows * 1024 * width, transcendentals=0, bytes_accessed=2 * 1024 * width
        ),
        name="project",
    )(att, wide, narrow, residual, gain, routing)


def expert_kernel(x_ref, *rest, capacity):
    weights, (out_ref, g_ref, u_ref, d_ref, sems) = rest[:12], rest[12:]
    copies = []
    for j in range(4):
        mine = [
            pltpu.make_async_copy(weights[3 * j + i], ref.at[j], sems.at[j, i])
            for i, ref in enumerate((g_ref, u_ref, d_ref))
        ]
        copies.append(mine)
    for mine in copies:
        for copy in mine:
            copy.start()
    x = x_ref[...]
    slots = x.shape[0]
    slot = lax.broadcasted_iota(jnp.int32, (slots // 2, slots), 0)
    from_slot = lax.broadcasted_iota(jnp.int32, (slots // 2, slots), 1)
    low_place = slot // capacity * (2 * capacity) + slot % capacity
    low = (from_slot == low_place).astype(jnp.bfloat16)
    high = (from_slot == low_place + capacity).astype(jnp.bfloat16)
    x = jnp.concatenate([dot_f32(low, x), dot_f32(high, x)], axis=1).astype(jnp.bfloat16)
    total = None
    for j in range(4):
        for copy in copies[j]:
            copy.wait()
        gate = dot_f32(x, g_ref[j])
        up = dot_f32(x, u_ref[j])
        hidden = (gate * jax.nn.sigmoid(gate) * up).astype(jnp.bfloat16)
        part = dot_f32(hidden, d_ref[j])
        total = part if total is None else total + part
    total = total.astype(jnp.bfloat16)
    half = total.shape[1] // 2
    over_rows = (((0,), (0,)), ((), ()))
    spread = dot_f32(low, total[:, :half], over_rows) + dot_f32(high, total[:, half:], over_rows)
    out_ref[...] = spread.astype(jnp.bfloat16)


def expert(x, weights, capacity):
    rows, width = x.shape[0] // 2, 2 * x.shape[1]
    units = weights[0].shape[1]
    anywhere = pl.BlockSpec(memory_space=pl.ANY)
    vmem = pl.BlockSpec(memory_space=pltpu.VMEM)
    return pl.pallas_call(
        functools.partial(expert_kernel, capacity=capacity),
        out_shape=jax.ShapeDtypeStruct(x.shape, jnp.bfloat16),
        in_specs=[vmem] + [anywhere] * 12,
        out_specs=vmem,
        scratch_shapes=[
            pltpu.VMEM((4, width, units), jnp.bfloat16),
            pltpu.VMEM((4, width, units), jnp.bfloat16),
            pltpu.VMEM((4, units, width), jnp.bfloat16),
            pltpu.SemaphoreType.DMA((4, 3)),
        ],
        compiler_params=pltpu.CompilerParams(vmem_limit_bytes=48 * 1024 * 1024),
        cost_estimate=pl.CostEstimate(
            flops=24 * rows * width * units, transcendentals=0, bytes_accessed=24 * width * units
        ),
        name="expert",
    )(x, *weights)


def combine_kernel(back_ref, middle_ref, routing_ref, weight_ref, out_ref, *, experts, capacity):
    picks = placed_slots(routing_ref[...], experts, capacity)
    back = back_ref[...]
    total = middle_ref[...].astype(jnp.float32)
    for k in range(2):
        answer = jnp.concatenate([dot_f32(picks[k][0], back), dot_f32(picks[k][1], back)], axis=1)
        total = total + weight_ref[:, k : k + 1] * answer
    out_ref[...] = total.astype(jnp.bfloat16)


def combine(back, middle, routing, weight, experts, capacity):
    return pl.pallas_call(
        functools.partial(combine_kernel, experts=experts, capacity=capacity),
        out_shape=jax.ShapeDtypeStruct(middle.shape, jnp.bfloat16),
        compiler_params=pltpu.CompilerParams(vmem_limit_bytes=24 * 1024 * 1024),
        name="combine",
    )(back, middle, routing, weight)


def body(
    residual,
    query_wide,
    key_wide,
    value_wide,
    query_narrow,
    key_narrow,
    value_narrow,
    gate_wide,
    gate_narrow,
    out_wide,
    out_narrow,
    norm_gain,
    routing,
    route_weight,
    gate_weight,
    up_weight,
    down_weight,
):
    dev_rows = query_wide.shape[0]
    own_rows, width = residual.shape
    core = lax.axis_index("core")
    is_wide = core == 0
    n_z, n_x, n_tp = lax.axis_size("z"), lax.axis_size("x"), lax.axis_size("tp")
    n_sp = 2 * n_z * n_x
    sp = ("z", "x", "core")
    place = jnp.full((1,), lax.axis_index(sp), jnp.int32)

    def pick(a, b):
        return jnp.where(is_wide, a, b)

    keep = [
        jnp.concatenate([pick(key_wide[span], key_narrow[span]), pick(value_wide[span], value_narrow[span])], axis=1)
        for span in (slice(0, OFFLOADED), slice(OFFLOADED, None))
    ]
    keep[0] = lax.optimization_barrier(keep[0])
    give = jnp.concatenate([pick(key_narrow, key_wide), pick(value_narrow, value_wide)], axis=1)
    swap = [(0, 1), (1, 0)]
    got = lax.ppermute(give, "core", swap)
    q_keep = pick(query_wide, query_narrow)
    q_got = lax.ppermute(pick(query_narrow, query_wide), "core", swap)
    queries = jnp.concatenate([pick(q_keep, q_got), pick(q_got, q_keep)], axis=0)

    g, u, d = gate_weight[0], up_weight[0], down_weight[0]
    ahead = [(i, (i + 1) % n_tp) for i in range(n_tp)]
    behind = [(i, (i - 1) % n_tp) for i in range(n_tp)]
    from_left = [lax.ppermute(w, "tp", ahead) for w in (g, u, d)]
    from_right = [lax.ppermute(w, "tp", behind) for w in (g, u, d)]
    by_core = [(i, (i + 1) % n_tp) for i in range(n_tp)]
    by_core += [(n_tp + i, n_tp + (i - 1) % n_tp) for i in range(n_tp)]
    far = [
        lax.ppermute(from_left[0], "tp", ahead),
        lax.ppermute(from_right[1], "tp", behind),
        lax.ppermute(pick(from_left[2], from_right[2]), ("core", "tp"), by_core),
    ]

    gathered = lax.all_gather(keep[0], ("z", "x"), axis=0, tiled=True)
    mine = jnp.concatenate([got, keep[1]], axis=0)
    parts = [(1, 0, dev_rows), (0, OFFLOADED, dev_rows - OFFLOADED)]
    offs = (0, -1, 1, 2)
    line = [mine] + [
        lax.ppermute(mine, "x", [((i + off) % n_x, i) for i in range(n_x)]) for off in offs[1:]
    ]
    plane = jnp.concatenate(line, axis=0)
    half = plane.shape[0] // 2
    up = [(i, (i + 1) % n_z) for i in range(n_z)]
    down = [(i, (i - 1) % n_z) for i in range(n_z)]
    planes = [[(plane, (0, offs, parts))]]
    lower = upper = plane
    last = n_z // 2
    for step in range(1, last + 1):
        if step == last:
            lower, upper = lower[:half], upper[half:]
        lower = lax.ppermute(lower, "z", up)
        upper = lax.ppermute(upper, "z", down)
        if step < last:
            planes.append([(lower, (step, offs, parts)), (upper, (-step, offs, parts))])
        else:
            planes.append([(lower, (step, offs[:2], parts)), (upper, (step, offs[2:], parts))])

    sums = lax.all_gather(running_sums(gate_wide, gate_narrow), "core", axis=0)
    sums = [sums] + [
        lax.ppermute(sums, "x", [((i + off) % n_x, i) for i in range(n_x)]) for off in offs[1:]
    ]
    sums = jnp.concatenate(sums, axis=0)
    sums = [sums] + [
        lax.ppermute(sums, "z", [((i - k) % n_z, i) for i in range(n_z)]) for k in range(1, n_z)
    ]
    decay = offset_sums(place, sums, n_x, offs)

    state = None
    for step, pieces in enumerate(planes):
        state = attend_planes(
            place,
            queries,
            decay,
            [piece for piece, _ in pieces] + ([gathered] if step == last - 1 else []),
            [layout for _, layout in pieces],
            OFFLOADED if step == last - 1 else 0,
            (n_z, n_x),
            dev_rows,
            state,
            step == last,
        )
    att = state

    att = lax.all_to_all(
        att.reshape(2 * n_tp, own_rows, HW), ("core", "tp"), split_axis=0, concat_axis=0, tiled=True
    )
    experts = n_sp
    capacity = own_rows * GROUPS // experts
    middle, outgoing = project(
        att, out_wide, out_narrow, residual, norm_gain.reshape(1, width), routing, experts, capacity
    )

    def exchange(slots):
        shape = slots.shape
        slots = slots.reshape(experts, 2 * capacity, width // 2)
        slots = lax.all_to_all(slots, sp, split_axis=0, concat_axis=0, tiled=True)
        return slots.reshape(shape)

    arrived = exchange(outgoing)
    answers = expert(arrived, [g, u, d, *from_left, *from_right, *far], capacity)
    returned = exchange(answers)
    return combine(returned, middle, routing, route_weight, experts, capacity)


def solution(mesh):
    n_sp, n_tp = mesh.shape["sp"], mesh.shape["tp"]
    n_x = 4
    fine = Mesh(mesh.devices.reshape(n_sp // 2 // n_x, n_x, 2, n_tp), ("z", "x", "core", "tp"))
    sp = ("z", "x", "core")
    rows = P((*sp, "tp"), None)
    heads = P(sp, "tp")
    placed = (
        rows,
        *([heads] * 8),
        P(),
        P(),
        P(),
        rows,
        rows,
        P(sp, None, "tp"),
        P(sp, None, "tp"),
        P(sp, "tp", None),
    )
    return jax.shard_map(body, mesh=fine, in_specs=placed, out_specs=rows, check_vma=False)
```

```python
import functools

import jax
import jax.numpy as jnp
from jax import lax
from jax.experimental import pallas as pl
from jax.experimental.pallas import tpu as pltpu
from jax.sharding import Mesh
from jax.sharding import PartitionSpec as P

HW = 128
HN = 64
GROUPS = 4
EPS = 1e-06
LOG2E = 1.4426950408889634
LOW = -1e30
TQ = 256


def dot_f32(a, b, dims=(((1,), (0,)), ((), ()))):
    return lax.dot_general(a, b, dims, preferred_element_type=jnp.float32)


def decay_line(decay_ref, blocks, head, lines):
    return jnp.concatenate(
        [
            decay_ref[2 * chip + sub, pl.ds(lines * head + (row0 + r) // 128, 1), :]
            for chip, sub, row0, rows in blocks
            for r in range(0, rows, 128)
        ],
        axis=1,
    )


def visit(place, q_ref, decay_ref, kv, blocks, dev_rows, held, forms):
    m_ref, l_ref, acc_ref, qh_ref = held
    chip, core = place // 2, place % 2
    queries = q_ref.shape[0]
    scale = jnp.where(core == 0, jnp.float32(HW**-0.5 * LOG2E), jnp.float32(HN**-0.5 * LOG2E))
    lines = dev_rows // 128
    earliest = latest = blocks[0][0]
    for block in blocks[1:]:
        earliest, latest = jnp.minimum(earliest, block[0]), jnp.maximum(latest, block[0])

    def run(h, masked):
        k = kv[:, :HW]
        v = kv[:, HW:]
        starts = range(0, queries, TQ)
        dk = decay_line(decay_ref, blocks, h + core, lines)
        if masked:
            key_place = jnp.concatenate(
                [
                    lax.broadcasted_iota(jnp.int32, (1, rows), 1) + ((2 * c + sub) * dev_rows + row0)
                    for c, sub, row0, rows in blocks
                ],
                axis=1,
            )

        def scores(r0):
            return dot_f32(qh_ref[h, pl.ds(r0, TQ), :], k, (((1,), (1,)), ((), ())))

        ahead = scores(0)
        for r0 in starts:
            s = ahead * scale - dk
            if r0 + TQ < queries:
                ahead = scores(r0 + TQ)
            span = pl.ds(r0, TQ)
            if masked:
                row = lax.broadcasted_iota(jnp.int32, (TQ, 1), 0) + (chip * (2 * dev_rows) + r0)
                s = jnp.where(key_place <= row, s, LOW)
            m_old = m_ref[h, span, :]
            m_new = jnp.maximum(m_old, jnp.max(s, axis=1, keepdims=True))
            alpha = jnp.exp2(m_old - m_new)
            p = jnp.exp2(s - m_new[:, :1])
            m_ref[h, span, :] = m_new
            l_ref[h, span, :] = l_ref[h, span, :] * alpha + jnp.sum(p, axis=1, keepdims=True)
            acc_ref[h, span, :] = acc_ref[h, span, :] * alpha + dot_f32(p.astype(jnp.bfloat16), v)

    for masked in forms:
        at = earliest <= chip if masked else latest < chip

        @pl.when(at)
        def _():
            def head(h, carry):
                run(h, masked)
                return carry

            lax.fori_loop(0, core + 1, head, 0)


def head_queries(place, q_ref, qh_ref):
    core = place % 2
    q = q_ref[...]
    lane = lax.broadcasted_iota(jnp.int32, q.shape, 1)
    qh_ref[0] = jnp.where((core == 0) | (lane < HN), q, jnp.zeros_like(q))
    qh_ref[1] = jnp.where(lane >= HN, q, jnp.zeros_like(q))


def take_state(ins, held):
    m_ref, l_ref, acc_ref = held
    if ins:
        for source, target in zip(ins, held):
            target[...] = source[...]
    else:
        m_ref[...] = jnp.full_like(m_ref, LOW)
        l_ref[...] = jnp.zeros_like(l_ref)
        acc_ref[...] = jnp.zeros_like(acc_ref)


def plane_kernel(place_ref, q_ref, decay_ref, *rest, pieces, n_z, n_x, dev_rows, first, last):
    n = len(pieces)
    kvs, rest = rest[:n], rest[n:]
    ins = ()
    if not first:
        ins, rest = rest[:3], rest[3:]
    if last:
        out_ref, rest = rest[0], rest[1:]
    held, qh_ref = rest[:3], rest[3]
    take_state(ins, held)
    place = place_ref[0]
    core = place % 2
    head_queries(place, q_ref, qh_ref)
    z, x = place // 2 // n_x, place // 2 % n_x
    tile = 4 * dev_rows
    for kv_ref, (shift, off0) in zip(kvs, pieces):
        plane = (z - shift + n_z) % n_z * n_x

        def one(t, carry, kv_ref=kv_ref, plane=plane, off0=off0, shift=shift):
            blocks = [
                (plane + (x + off0 + 2 * t + i) % n_x, (core + flip) % 2, 0, dev_rows)
                for i in range(2)
                for flip in (1, 0)
            ]
            kv = kv_ref.at[pl.ds(pl.multiple_of(t * tile, tile), tile), :]
            visit(place, q_ref, decay_ref, kv, blocks, dev_rows, rest, (shift == 0,))
            return carry

        lax.fori_loop(0, kv_ref.shape[0] // tile, one, 0)
    if last:
        _, l_ref, acc_ref = held
        lane = lax.broadcasted_iota(jnp.int32, q_ref.shape, 1)
        one_head = acc_ref[0] / l_ref[0]
        other = acc_ref[1] / jnp.where(core == 0, 1.0, l_ref[1])
        out_ref[...] = jnp.where((core == 0) | (lane < HN), one_head, other).astype(jnp.bfloat16)


def attend_planes(place, q, decay, kvs, pieces, sizes, dev_rows, state, last):
    queries = q.shape[0]
    shape = (2, queries, HW)
    smem = pl.BlockSpec(memory_space=pltpu.SMEM)
    vmem = pl.BlockSpec(memory_space=pltpu.VMEM)
    args = [q, decay, *kvs, *(state or ())]
    keys = sum(kv.shape[0] for kv in kvs)
    scratch = [pltpu.VMEM(shape, jnp.bfloat16)]
    if last:
        out_shape, out_specs = jax.ShapeDtypeStruct((queries, HW), jnp.bfloat16), vmem
        scratch = [pltpu.VMEM(shape, jnp.float32)] * 3 + scratch
    else:
        out_shape, out_specs = [jax.ShapeDtypeStruct(shape, jnp.float32)] * 3, [vmem] * 3
    return pl.pallas_call(
        functools.partial(
            plane_kernel,
            pieces=pieces,
            n_z=sizes[0],
            n_x=sizes[1],
            dev_rows=dev_rows,
            first=state is None,
            last=last,
        ),
        out_shape=out_shape,
        in_specs=[smem] + [vmem] * len(args),
        out_specs=out_specs,
        scratch_shapes=scratch,
        compiler_params=pltpu.CompilerParams(vmem_limit_bytes=26 * 1024 * 1024),
        cost_estimate=pl.CostEstimate(
            flops=8 * queries * keys * HW, transcendentals=2 * queries * keys, bytes_accessed=4 * keys * HW
        ),
        name="planes",
    )(place, *args)


def half_kernel(in_ref, out_ref):
    out_ref[...] = in_ref[...]


def half_of(piece, which):
    shape = (piece.shape[0] // 2, piece.shape[1])
    return pl.pallas_call(
        half_kernel,
        out_shape=jax.ShapeDtypeStruct(shape, piece.dtype),
        grid=(1,),
        in_specs=[pl.BlockSpec(shape, lambda i: (which, 0))],
        out_specs=pl.BlockSpec(shape, lambda i: (0, 0)),
        compiler_params=pltpu.CompilerParams(vmem_limit_bytes=8 * 1024 * 1024),
        name="half",
    )(piece)


def running_kernel(wide_ref, narrow_ref, out_ref):
    gates = jnp.concatenate([wide_ref[...], narrow_ref[...]], axis=0)
    kept = jnp.minimum(gates, 0.0) - jnp.log1p(jnp.exp(-jnp.abs(gates)))
    heads, rows = kept.shape
    row = lax.broadcasted_iota(jnp.int32, (rows, rows), 0)
    col = lax.broadcasted_iota(jnp.int32, (rows, rows), 1)
    upto = (row <= col).astype(jnp.float32)
    kept = jnp.concatenate([kept, jnp.zeros((8 - heads, rows), jnp.float32)], axis=0)
    sums = lax.dot_general(
        kept,
        upto,
        (((1,), (0,)), ((), ())),
        precision=lax.Precision.HIGHEST,
        preferred_element_type=jnp.float32,
    )
    out_ref[...] = jnp.zeros_like(out_ref)
    lines = rows // 128
    for h in range(heads):
        for j in range(lines):
            at = lines * h + j
            out_ref[at : at + 1, :] = sums[h : h + 1, j * 128 : (j + 1) * 128]


def running_sums(gate_wide, gate_narrow):
    return pl.pallas_call(
        running_kernel,
        out_shape=jax.ShapeDtypeStruct((8, 128), jnp.float32),
        compiler_params=pltpu.CompilerParams(vmem_limit_bytes=8 * 1024 * 1024),
        name="running",
    )(gate_wide.T, gate_narrow.T)


def offset_kernel(place_ref, *rest, n_z, n_x, offs):
    pieces, (out_ref, abs_ref) = rest[:n_z], rest[n_z:]
    chip = place_ref[0] // 2
    z, x = chip // n_x, chip % n_x
    for k in range(n_z):
        for i, off in enumerate(offs):
            at = (z - k + n_z) % n_z * n_x + (x + off + n_x) % n_x
            abs_ref[2 * at] = pieces[k][2 * i]
            abs_ref[2 * at + 1] = pieces[k][2 * i + 1]
    devices = abs_ref.shape[0]
    odd = lax.broadcasted_iota(jnp.int32, (8, 128), 0) % 2 == 1
    offset = jnp.zeros((8, 128), jnp.float32)
    base = offset
    for d in range(devices):
        here = abs_ref[d]
        out_ref[d] = here + offset
        base = jnp.where(2 * chip == d, offset, base)
        end = jnp.broadcast_to(here[:, 127:128], (8, 128))
        offset = offset + jnp.where(odd, end, jnp.concatenate([end[1:], end[:1]], axis=0))
    for d in range(devices):
        out_ref[d] = (out_ref[d] - base) * LOG2E


def offset_sums(place, pieces, n_x, offs):
    every = (len(pieces) * pieces[0].shape[0], 8, 128)
    smem = pl.BlockSpec(memory_space=pltpu.SMEM)
    vmem = pl.BlockSpec(memory_space=pltpu.VMEM)
    return pl.pallas_call(
        functools.partial(offset_kernel, n_z=len(pieces), n_x=n_x, offs=offs),
        out_shape=jax.ShapeDtypeStruct(every, jnp.float32),
        in_specs=[smem] + [vmem] * len(pieces),
        scratch_shapes=[pltpu.VMEM(every, jnp.float32)],
        compiler_params=pltpu.CompilerParams(vmem_limit_bytes=8 * 1024 * 1024),
        name="offset",
    )(place, *pieces)


def as_columns(lines):
    n = lines.shape[1]
    same = lax.broadcasted_iota(jnp.int32, (n, n), 0) == lax.broadcasted_iota(jnp.int32, (n, n), 1)
    return [jnp.sum(jnp.where(same, lines[k : k + 1], 0.0), axis=1, keepdims=True) for k in range(2)]


def placed_slots(routing, experts, capacity):
    rows = routing.shape[1]
    routing = [column.astype(jnp.int32) for column in as_columns(routing.astype(jnp.float32))]
    expert = lax.broadcasted_iota(jnp.int32, (rows, experts), 1)
    hits = [(routing[k] == expert).astype(jnp.float32) for k in range(2)]
    row = lax.broadcasted_iota(jnp.int32, (rows, rows), 0)
    col = lax.broadcasted_iota(jnp.int32, (rows, rows), 1)
    before = (col < row).astype(jnp.bfloat16)
    earlier = dot_f32(before, (hits[0] + hits[1]).astype(jnp.bfloat16))
    slot = lax.broadcasted_iota(jnp.int32, (rows, 2 * experts * capacity), 1)
    picks = []
    for k in range(2):
        rank = jnp.sum(earlier * hits[k], axis=1, keepdims=True).astype(jnp.int32)
        place = routing[k] * (2 * capacity) + rank
        picks.append([(place + half * capacity == slot).astype(jnp.bfloat16) for half in range(2)])
    return picks


def project_kernel(
    att_ref, wide_ref, narrow_ref, residual_ref, gain_ref, routing_ref, middle_ref, out_ref, *, experts, capacity
):
    half = att_ref.shape[0] // 2
    wide = jnp.concatenate([att_ref[j] for j in range(half)], axis=1)
    narrow = jnp.concatenate([att_ref[half + j] for j in range(half)], axis=1)
    mixed = dot_f32(wide, wide_ref[...]) + dot_f32(narrow, narrow_ref[...])
    middle = (residual_ref[...].astype(jnp.float32) + mixed).astype(jnp.bfloat16)
    middle_ref[...] = middle
    wider = middle.astype(jnp.float32)
    spread = jnp.mean(wider * wider, axis=1, keepdims=True)
    normed = (wider * lax.rsqrt(spread + EPS) * gain_ref[...]).astype(jnp.bfloat16)
    picks = placed_slots(routing_ref[...], experts, capacity)
    half = normed.shape[1] // 2
    over_rows = (((0,), (0,)), ((), ()))
    low = dot_f32(picks[0][0] + picks[1][0], normed[:, :half], over_rows)
    high = dot_f32(picks[0][1] + picks[1][1], normed[:, half:], over_rows)
    out_ref[...] = (low + high).astype(jnp.bfloat16)


def project(att, wide, narrow, residual, gain, routing, experts, capacity):
    rows, width = residual.shape
    return pl.pallas_call(
        functools.partial(project_kernel, experts=experts, capacity=capacity),
        out_shape=[
            jax.ShapeDtypeStruct((rows, width), jnp.bfloat16),
            jax.ShapeDtypeStruct((2 * experts * capacity, width // 2), jnp.bfloat16),
        ],
        compiler_params=pltpu.CompilerParams(vmem_limit_bytes=40 * 1024 * 1024),
        cost_estimate=pl.CostEstimate(
            flops=2 * rows * 1024 * width, transcendentals=0, bytes_accessed=2 * 1024 * width
        ),
        name="project",
    )(att, wide, narrow, residual, gain, routing)


def expert_kernel(x_ref, *rest, capacity):
    weights, (out_ref, g_ref, u_ref, d_ref, sems) = rest[:12], rest[12:]
    copies = []
    for j in range(4):
        mine = [
            pltpu.make_async_copy(weights[3 * j + i], ref.at[j], sems.at[j, i])
            for i, ref in enumerate((g_ref, u_ref, d_ref))
        ]
        copies.append(mine)
    for mine in copies:
        for copy in mine:
            copy.start()
    x = x_ref[...]
    slots = x.shape[0]
    slot = lax.broadcasted_iota(jnp.int32, (slots // 2, slots), 0)
    from_slot = lax.broadcasted_iota(jnp.int32, (slots // 2, slots), 1)
    low_place = slot // capacity * (2 * capacity) + slot % capacity
    low = (from_slot == low_place).astype(jnp.bfloat16)
    high = (from_slot == low_place + capacity).astype(jnp.bfloat16)
    x = jnp.concatenate([dot_f32(low, x), dot_f32(high, x)], axis=1).astype(jnp.bfloat16)
    total = None
    for j in range(4):
        for copy in copies[j]:
            copy.wait()
        gate = dot_f32(x, g_ref[j])
        up = dot_f32(x, u_ref[j])
        hidden = (gate * jax.nn.sigmoid(gate) * up).astype(jnp.bfloat16)
        part = dot_f32(hidden, d_ref[j])
        total = part if total is None else total + part
    total = total.astype(jnp.bfloat16)
    half = total.shape[1] // 2
    over_rows = (((0,), (0,)), ((), ()))
    spread = dot_f32(low, total[:, :half], over_rows) + dot_f32(high, total[:, half:], over_rows)
    out_ref[...] = spread.astype(jnp.bfloat16)


def expert(x, weights, capacity):
    rows, width = x.shape[0] // 2, 2 * x.shape[1]
    units = weights[0].shape[1]
    anywhere = pl.BlockSpec(memory_space=pl.ANY)
    vmem = pl.BlockSpec(memory_space=pltpu.VMEM)
    return pl.pallas_call(
        functools.partial(expert_kernel, capacity=capacity),
        out_shape=jax.ShapeDtypeStruct(x.shape, jnp.bfloat16),
        in_specs=[vmem] + [anywhere] * 12,
        out_specs=vmem,
        scratch_shapes=[
            pltpu.VMEM((4, width, units), jnp.bfloat16),
            pltpu.VMEM((4, width, units), jnp.bfloat16),
            pltpu.VMEM((4, units, width), jnp.bfloat16),
            pltpu.SemaphoreType.DMA((4, 3)),
        ],
        compiler_params=pltpu.CompilerParams(vmem_limit_bytes=48 * 1024 * 1024),
        cost_estimate=pl.CostEstimate(
            flops=24 * rows * width * units, transcendentals=0, bytes_accessed=24 * width * units
        ),
        name="expert",
    )(x, *weights)


def combine_kernel(back_ref, middle_ref, routing_ref, weight_ref, out_ref, *, experts, capacity):
    picks = placed_slots(routing_ref[...], experts, capacity)
    back = back_ref[...]
    total = middle_ref[...].astype(jnp.float32)
    weights = as_columns(weight_ref[...])
    for k in range(2):
        answer = jnp.concatenate([dot_f32(picks[k][0], back), dot_f32(picks[k][1], back)], axis=1)
        total = total + weights[k] * answer
    out_ref[...] = total.astype(jnp.bfloat16)


def combine(back, middle, routing, weight, experts, capacity):
    return pl.pallas_call(
        functools.partial(combine_kernel, experts=experts, capacity=capacity),
        out_shape=jax.ShapeDtypeStruct(middle.shape, jnp.bfloat16),
        compiler_params=pltpu.CompilerParams(vmem_limit_bytes=24 * 1024 * 1024),
        name="combine",
    )(back, middle, routing, weight)


def body(
    residual,
    query_wide,
    key_wide,
    value_wide,
    query_narrow,
    key_narrow,
    value_narrow,
    gate_wide,
    gate_narrow,
    out_wide,
    out_narrow,
    norm_gain,
    routing,
    route_weight,
    gate_weight,
    up_weight,
    down_weight,
):
    dev_rows = query_wide.shape[0]
    own_rows, width = residual.shape
    core = lax.axis_index("core")
    is_wide = core == 0
    n_z, n_x, n_tp = lax.axis_size("z"), lax.axis_size("x"), lax.axis_size("tp")
    n_sp = 2 * n_z * n_x
    sp = ("z", "x", "core")
    place = jnp.full((1,), lax.axis_index(sp), jnp.int32)

    def pick(a, b):
        return jnp.where(is_wide, a, b)

    keep = jnp.concatenate([pick(key_wide, key_narrow), pick(value_wide, value_narrow)], axis=1)
    give = jnp.concatenate([pick(key_narrow, key_wide), pick(value_narrow, value_wide)], axis=1)
    swap = [(0, 1), (1, 0)]
    got = lax.ppermute(give, "core", swap)
    q_keep = pick(query_wide, query_narrow)
    q_got = lax.ppermute(pick(query_narrow, query_wide), "core", swap)
    queries = jnp.concatenate([pick(q_keep, q_got), pick(q_got, q_keep)], axis=0)

    g, u, d = gate_weight[0], up_weight[0], down_weight[0]
    ahead = [(i, (i + 1) % n_tp) for i in range(n_tp)]
    behind = [(i, (i - 1) % n_tp) for i in range(n_tp)]
    from_left = [lax.ppermute(w, "tp", ahead) for w in (g, u, d)]
    from_right = [lax.ppermute(w, "tp", behind) for w in (g, u, d)]
    by_core = [(i, (i + 1) % n_tp) for i in range(n_tp)]
    by_core += [(n_tp + i, n_tp + (i - 1) % n_tp) for i in range(n_tp)]
    far = [
        lax.ppermute(from_left[0], "tp", ahead),
        lax.ppermute(from_right[1], "tp", behind),
        lax.ppermute(pick(from_left[2], from_right[2]), ("core", "tp"), by_core),
    ]

    next_x = [((i + 1) % n_x, i) for i in range(n_x)]
    prev_x = [((i - 1) % n_x, i) for i in range(n_x)]
    keep_1, keep_3 = lax.ppermute(keep, "x", next_x), lax.ppermute(keep, "x", prev_x)
    got_1, got_3 = lax.ppermute(got, "x", next_x), lax.ppermute(got, "x", prev_x)
    got_2, keep_2 = lax.ppermute(got_1, "x", next_x), lax.ppermute(keep_3, "x", prev_x)
    plane = jnp.concatenate([got, keep, got_1, keep_1, got_2, keep_2, got_3, keep_3], axis=0)
    up = [(i, (i + 1) % n_z) for i in range(n_z)]
    down = [(i, (i - 1) % n_z) for i in range(n_z)]
    planes = [[(plane, (0, 0))]]
    lower = upper = plane
    last = n_z // 2
    for step in range(1, last + 1):
        if step == last:
            lower, upper = half_of(lower, 0), half_of(upper, 1)
        lower = lax.ppermute(lower, "z", up)
        upper = lax.ppermute(upper, "z", down)
        if step < last:
            planes.append([(lower, (step, 0)), (upper, (-step, 0))])
        else:
            planes.append([(lower, (step, 0)), (upper, (step, 2))])

    offs = (0, -1, 1, 2)
    sums = lax.all_gather(running_sums(gate_wide, gate_narrow), "core", axis=0)
    sums = [sums] + [
        lax.ppermute(sums, "x", [((i + off) % n_x, i) for i in range(n_x)]) for off in offs[1:]
    ]
    sums = jnp.concatenate(sums, axis=0)
    sums = [sums] + [
        lax.ppermute(sums, "z", [((i - k) % n_z, i) for i in range(n_z)]) for k in range(1, n_z)
    ]
    decay = offset_sums(place, sums, n_x, offs)

    state = None
    for step, pieces in enumerate(planes):
        state = attend_planes(
            place,
            queries,
            decay,
            [piece for piece, _ in pieces],
            [layout for _, layout in pieces],
            (n_z, n_x),
            dev_rows,
            state,
            step == last,
        )
    att = state

    att = lax.all_to_all(
        att.reshape(2 * n_tp, own_rows, HW), ("core", "tp"), split_axis=0, concat_axis=0, tiled=True
    )
    experts = n_sp
    capacity = own_rows * GROUPS // experts
    middle, outgoing = project(
        att, out_wide, out_narrow, residual, norm_gain.reshape(1, width), routing.T, experts, capacity
    )

    def exchange(slots):
        shape = slots.shape
        slots = slots.reshape(experts, 2 * capacity, width // 2)
        slots = lax.all_to_all(slots, sp, split_axis=0, concat_axis=0, tiled=True)
        return slots.reshape(shape)

    arrived = exchange(outgoing)
    answers = expert(arrived, [g, u, d, *from_left, *from_right, *far], capacity)
    returned = exchange(answers)
    return combine(returned, middle, routing.T, route_weight.T, experts, capacity)


def solution(mesh):
    n_sp, n_tp = mesh.shape["sp"], mesh.shape["tp"]
    n_x = 4
    fine = Mesh(mesh.devices.reshape(n_sp // 2 // n_x, n_x, 2, n_tp), ("z", "x", "core", "tp"))
    sp = ("z", "x", "core")
    rows = P((*sp, "tp"), None)
    heads = P(sp, "tp")
    placed = (
        rows,
        *([heads] * 8),
        P(),
        P(),
        P(),
        rows,
        rows,
        P(sp, None, "tp"),
        P(sp, None, "tp"),
        P(sp, "tp", None),
    )
    return jax.shard_map(body, mesh=fine, in_specs=placed, out_specs=rows, check_vma=False)
```

```python
import functools

import jax
import jax.numpy as jnp
from jax import lax
from jax.experimental import pallas as pl
from jax.experimental.pallas import tpu as pltpu
from jax.sharding import Mesh
from jax.sharding import PartitionSpec as P

HW = 128
HN = 64
GROUPS = 4
EPS = 1e-06
LOG2E = 1.4426950408889634
LOW = -1e30
TQ = 256


def dot_f32(a, b, dims=(((1,), (0,)), ((), ()))):
    return lax.dot_general(a, b, dims, preferred_element_type=jnp.float32)


def decay_line(decay_ref, blocks, head, lines):
    return jnp.concatenate(
        [
            decay_ref[2 * chip + sub, pl.ds(lines * head + (row0 + r) // 128, 1), :]
            for chip, sub, row0, rows in blocks
            for r in range(0, rows, 128)
        ],
        axis=1,
    )


def visit(place, q_ref, decay_ref, kv, blocks, dev_rows, held, forms):
    m_ref, l_ref, acc_ref, qh_ref = held
    chip, core = place // 2, place % 2
    queries = q_ref.shape[0]
    scale = jnp.where(core == 0, jnp.float32(HW**-0.5 * LOG2E), jnp.float32(HN**-0.5 * LOG2E))
    lines = dev_rows // 128
    earliest = latest = blocks[0][0]
    for block in blocks[1:]:
        earliest, latest = jnp.minimum(earliest, block[0]), jnp.maximum(latest, block[0])

    def run(h, masked):
        k = kv[:, :HW]
        v = kv[:, HW:]
        starts = range(0, queries, TQ)
        dk = decay_line(decay_ref, blocks, h + core, lines)
        if masked:
            key_place = jnp.concatenate(
                [
                    lax.broadcasted_iota(jnp.int32, (1, rows), 1) + ((2 * c + sub) * dev_rows + row0)
                    for c, sub, row0, rows in blocks
                ],
                axis=1,
            )

        def scores(r0):
            return dot_f32(qh_ref[h, pl.ds(r0, TQ), :], k, (((1,), (1,)), ((), ())))

        ahead = scores(0)
        for r0 in starts:
            s = ahead * scale - dk
            if r0 + TQ < queries:
                ahead = scores(r0 + TQ)
            span = pl.ds(r0, TQ)
            if masked:
                row = lax.broadcasted_iota(jnp.int32, (TQ, 1), 0) + (chip * (2 * dev_rows) + r0)
                s = jnp.where(key_place <= row, s, LOW)
            m_old = m_ref[h, span, :]
            m_new = jnp.maximum(m_old, jnp.max(s, axis=1, keepdims=True))
            alpha = jnp.exp2(m_old - m_new)
            p = jnp.exp2(s - m_new[:, :1])
            m_ref[h, span, :] = m_new
            l_ref[h, span, :] = l_ref[h, span, :] * alpha + jnp.sum(p, axis=1, keepdims=True)
            acc_ref[h, span, :] = acc_ref[h, span, :] * alpha + dot_f32(p.astype(jnp.bfloat16), v)

    for masked in forms:
        at = earliest <= chip if masked else latest < chip

        @pl.when(at)
        def _():
            def head(h, carry):
                run(h, masked)
                return carry

            lax.fori_loop(0, core + 1, head, 0)


def head_queries(place, q_ref, qh_ref):
    core = place % 2
    q = q_ref[...]
    lane = lax.broadcasted_iota(jnp.int32, q.shape, 1)
    qh_ref[0] = jnp.where((core == 0) | (lane < HN), q, jnp.zeros_like(q))
    qh_ref[1] = jnp.where(lane >= HN, q, jnp.zeros_like(q))


def take_state(ins, held):
    m_ref, l_ref, acc_ref = held
    if ins:
        for source, target in zip(ins, held):
            target[...] = source[...]
    else:
        m_ref[...] = jnp.full_like(m_ref, LOW)
        l_ref[...] = jnp.zeros_like(l_ref)
        acc_ref[...] = jnp.zeros_like(acc_ref)


def plane_kernel(place_ref, q_ref, decay_ref, *rest, pieces, n_z, n_x, dev_rows, first, last):
    n = len(pieces)
    kvs, rest = rest[:n], rest[n:]
    ins = ()
    if not first:
        ins, rest = rest[:3], rest[3:]
    if last:
        out_ref, rest = rest[0], rest[1:]
    held, qh_ref = rest[:3], rest[3]
    take_state(ins, held)
    place = place_ref[0]
    core = place % 2
    head_queries(place, q_ref, qh_ref)
    z, x = place // 2 // n_x, place // 2 % n_x
    tile = 4 * dev_rows
    for kv_ref, (shift, off0) in zip(kvs, pieces):
        plane = (z - shift + n_z) % n_z * n_x

        def one(t, carry, kv_ref=kv_ref, plane=plane, off0=off0, shift=shift):
            blocks = [
                (plane + (x + off0 + 2 * t + i) % n_x, (core + flip) % 2, 0, dev_rows)
                for i in range(2)
                for flip in (1, 0)
            ]
            kv = kv_ref.at[pl.ds(pl.multiple_of(t * tile, tile), tile), :]
            visit(place, q_ref, decay_ref, kv, blocks, dev_rows, rest, (shift == 0,))
            return carry

        lax.fori_loop(0, kv_ref.shape[0] // tile, one, 0)
    if last:
        _, l_ref, acc_ref = held
        lane = lax.broadcasted_iota(jnp.int32, q_ref.shape, 1)
        one_head = acc_ref[0] / l_ref[0]
        other = acc_ref[1] / jnp.where(core == 0, 1.0, l_ref[1])
        out_ref[...] = jnp.where((core == 0) | (lane < HN), one_head, other).astype(jnp.bfloat16)


def attend_planes(place, q, decay, kvs, pieces, sizes, dev_rows, state, last):
    queries = q.shape[0]
    shape = (2, queries, HW)
    smem = pl.BlockSpec(memory_space=pltpu.SMEM)
    vmem = pl.BlockSpec(memory_space=pltpu.VMEM)
    args = [q, decay, *kvs, *(state or ())]
    keys = sum(kv.shape[0] for kv in kvs)
    scratch = [pltpu.VMEM(shape, jnp.bfloat16)]
    if last:
        out_shape, out_specs = jax.ShapeDtypeStruct((queries, HW), jnp.bfloat16), vmem
        scratch = [pltpu.VMEM(shape, jnp.float32)] * 3 + scratch
    else:
        out_shape, out_specs = [jax.ShapeDtypeStruct(shape, jnp.float32)] * 3, [vmem] * 3
    return pl.pallas_call(
        functools.partial(
            plane_kernel,
            pieces=pieces,
            n_z=sizes[0],
            n_x=sizes[1],
            dev_rows=dev_rows,
            first=state is None,
            last=last,
        ),
        out_shape=out_shape,
        in_specs=[smem] + [vmem] * len(args),
        out_specs=out_specs,
        scratch_shapes=scratch,
        compiler_params=pltpu.CompilerParams(vmem_limit_bytes=26 * 1024 * 1024),
        cost_estimate=pl.CostEstimate(
            flops=8 * queries * keys * HW, transcendentals=2 * queries * keys, bytes_accessed=4 * keys * HW
        ),
        name="planes",
    )(place, *args)


def half_kernel(in_ref, out_ref):
    out_ref[...] = in_ref[...]


def half_of(piece, which):
    shape = (piece.shape[0] // 2, piece.shape[1])
    return pl.pallas_call(
        half_kernel,
        out_shape=jax.ShapeDtypeStruct(shape, piece.dtype),
        grid=(1,),
        in_specs=[pl.BlockSpec(shape, lambda i: (which, 0))],
        out_specs=pl.BlockSpec(shape, lambda i: (0, 0)),
        compiler_params=pltpu.CompilerParams(vmem_limit_bytes=8 * 1024 * 1024),
        name="half",
    )(piece)


def running_kernel(wide_ref, narrow_ref, out_ref):
    gates = jnp.concatenate([wide_ref[...], narrow_ref[...]], axis=0)
    kept = jnp.minimum(gates, 0.0) - jnp.log1p(jnp.exp(-jnp.abs(gates)))
    heads, rows = kept.shape
    row = lax.broadcasted_iota(jnp.int32, (rows, rows), 0)
    col = lax.broadcasted_iota(jnp.int32, (rows, rows), 1)
    upto = (row <= col).astype(jnp.float32)
    kept = jnp.concatenate([kept, jnp.zeros((8 - heads, rows), jnp.float32)], axis=0)
    sums = lax.dot_general(
        kept,
        upto,
        (((1,), (0,)), ((), ())),
        precision=lax.Precision.HIGHEST,
        preferred_element_type=jnp.float32,
    )
    out_ref[...] = jnp.zeros_like(out_ref)
    lines = rows // 128
    for h in range(heads):
        for j in range(lines):
            at = lines * h + j
            out_ref[at : at + 1, :] = sums[h : h + 1, j * 128 : (j + 1) * 128]


def running_sums(gate_wide, gate_narrow):
    return pl.pallas_call(
        running_kernel,
        out_shape=jax.ShapeDtypeStruct((8, 128), jnp.float32),
        compiler_params=pltpu.CompilerParams(vmem_limit_bytes=8 * 1024 * 1024),
        name="running",
    )(gate_wide.T, gate_narrow.T)


def offset_kernel(place_ref, *rest, n_z, n_x, offs):
    pieces, (out_ref, abs_ref) = rest[:n_z], rest[n_z:]
    chip = place_ref[0] // 2
    z, x = chip // n_x, chip % n_x
    for k in range(n_z):
        for i, off in enumerate(offs):
            at = (z - k + n_z) % n_z * n_x + (x + off + n_x) % n_x
            abs_ref[2 * at] = pieces[k][2 * i]
            abs_ref[2 * at + 1] = pieces[k][2 * i + 1]
    devices = abs_ref.shape[0]
    odd = lax.broadcasted_iota(jnp.int32, (8, 128), 0) % 2 == 1
    offset = jnp.zeros((8, 128), jnp.float32)
    base = offset
    for d in range(devices):
        here = abs_ref[d]
        out_ref[d] = here + offset
        base = jnp.where(2 * chip == d, offset, base)
        end = jnp.broadcast_to(here[:, 127:128], (8, 128))
        offset = offset + jnp.where(odd, end, jnp.concatenate([end[1:], end[:1]], axis=0))
    for d in range(devices):
        out_ref[d] = (out_ref[d] - base) * LOG2E


def offset_sums(place, pieces, n_x, offs):
    every = (len(pieces) * pieces[0].shape[0], 8, 128)
    smem = pl.BlockSpec(memory_space=pltpu.SMEM)
    vmem = pl.BlockSpec(memory_space=pltpu.VMEM)
    return pl.pallas_call(
        functools.partial(offset_kernel, n_z=len(pieces), n_x=n_x, offs=offs),
        out_shape=jax.ShapeDtypeStruct(every, jnp.float32),
        in_specs=[smem] + [vmem] * len(pieces),
        scratch_shapes=[pltpu.VMEM(every, jnp.float32)],
        compiler_params=pltpu.CompilerParams(vmem_limit_bytes=8 * 1024 * 1024),
        name="offset",
    )(place, *pieces)


def as_columns(lines):
    n = lines.shape[1]
    same = lax.broadcasted_iota(jnp.int32, (n, n), 0) == lax.broadcasted_iota(jnp.int32, (n, n), 1)
    return [jnp.sum(jnp.where(same, lines[k : k + 1], 0.0), axis=1, keepdims=True) for k in range(2)]


def placed_slots(routing, experts, capacity):
    rows = routing.shape[1]
    routing = [column.astype(jnp.int32) for column in as_columns(routing.astype(jnp.float32))]
    expert = lax.broadcasted_iota(jnp.int32, (rows, experts), 1)
    hits = [(routing[k] == expert).astype(jnp.float32) for k in range(2)]
    row = lax.broadcasted_iota(jnp.int32, (rows, rows), 0)
    col = lax.broadcasted_iota(jnp.int32, (rows, rows), 1)
    before = (col < row).astype(jnp.bfloat16)
    earlier = dot_f32(before, (hits[0] + hits[1]).astype(jnp.bfloat16))
    slot = lax.broadcasted_iota(jnp.int32, (rows, 2 * experts * capacity), 1)
    picks = []
    for k in range(2):
        rank = jnp.sum(earlier * hits[k], axis=1, keepdims=True).astype(jnp.int32)
        place = routing[k] * (2 * capacity) + rank
        picks.append([(place + half * capacity == slot).astype(jnp.bfloat16) for half in range(2)])
    return picks


def project_kernel(
    att_ref, wide_ref, narrow_ref, residual_ref, gain_ref, routing_ref, middle_ref, out_ref, *, experts, capacity
):
    half = att_ref.shape[0] // 2
    wide = jnp.concatenate([att_ref[j] for j in range(half)], axis=1)
    narrow = jnp.concatenate([att_ref[half + j] for j in range(half)], axis=1)
    mixed = dot_f32(wide, wide_ref[...]) + dot_f32(narrow, narrow_ref[...])
    middle = (residual_ref[...].astype(jnp.float32) + mixed).astype(jnp.bfloat16)
    middle_ref[...] = middle
    wider = middle.astype(jnp.float32)
    spread = jnp.mean(wider * wider, axis=1, keepdims=True)
    normed = (wider * lax.rsqrt(spread + EPS) * gain_ref[...]).astype(jnp.bfloat16)
    picks = placed_slots(routing_ref[...], experts, capacity)
    half = normed.shape[1] // 2
    over_rows = (((0,), (0,)), ((), ()))
    low = dot_f32(picks[0][0] + picks[1][0], normed[:, :half], over_rows)
    high = dot_f32(picks[0][1] + picks[1][1], normed[:, half:], over_rows)
    out_ref[...] = (low + high).astype(jnp.bfloat16)


def project(att, wide, narrow, residual, gain, routing, experts, capacity):
    rows, width = residual.shape
    return pl.pallas_call(
        functools.partial(project_kernel, experts=experts, capacity=capacity),
        out_shape=[
            jax.ShapeDtypeStruct((rows, width), jnp.bfloat16),
            jax.ShapeDtypeStruct((2 * experts * capacity, width // 2), jnp.bfloat16),
        ],
        compiler_params=pltpu.CompilerParams(vmem_limit_bytes=24 * 1024 * 1024),
        cost_estimate=pl.CostEstimate(
            flops=2 * rows * 1024 * width, transcendentals=0, bytes_accessed=2 * 1024 * width
        ),
        name="project",
    )(att, wide, narrow, residual, gain, routing)


def expert_kernel(x_ref, *rest, capacity):
    weights, (out_ref, g_ref, u_ref, d_ref, sems) = rest[:12], rest[12:]
    copies = []
    for j in range(4):
        mine = [
            pltpu.make_async_copy(weights[3 * j + i], ref.at[j], sems.at[j, i])
            for i, ref in enumerate((g_ref, u_ref, d_ref))
        ]
        copies.append(mine)
    for mine in copies:
        for copy in mine:
            copy.start()
    x = x_ref[...]
    slots = x.shape[0]
    slot = lax.broadcasted_iota(jnp.int32, (slots // 2, slots), 0)
    from_slot = lax.broadcasted_iota(jnp.int32, (slots // 2, slots), 1)
    low_place = slot // capacity * (2 * capacity) + slot % capacity
    low = (from_slot == low_place).astype(jnp.bfloat16)
    high = (from_slot == low_place + capacity).astype(jnp.bfloat16)
    x = jnp.concatenate([dot_f32(low, x), dot_f32(high, x)], axis=1).astype(jnp.bfloat16)
    total = None
    for j in range(4):
        for copy in copies[j]:
            copy.wait()
        gate = dot_f32(x, g_ref[j])
        up = dot_f32(x, u_ref[j])
        hidden = (gate * jax.nn.sigmoid(gate) * up).astype(jnp.bfloat16)
        part = dot_f32(hidden, d_ref[j])
        total = part if total is None else total + part
    total = total.astype(jnp.bfloat16)
    half = total.shape[1] // 2
    over_rows = (((0,), (0,)), ((), ()))
    spread = dot_f32(low, total[:, :half], over_rows) + dot_f32(high, total[:, half:], over_rows)
    out_ref[...] = spread.astype(jnp.bfloat16)


def expert(x, weights, capacity):
    rows, width = x.shape[0] // 2, 2 * x.shape[1]
    units = weights[0].shape[1]
    anywhere = pl.BlockSpec(memory_space=pl.ANY)
    vmem = pl.BlockSpec(memory_space=pltpu.VMEM)
    return pl.pallas_call(
        functools.partial(expert_kernel, capacity=capacity),
        out_shape=jax.ShapeDtypeStruct(x.shape, jnp.bfloat16),
        in_specs=[vmem] + [anywhere] * 12,
        out_specs=vmem,
        scratch_shapes=[
            pltpu.VMEM((4, width, units), jnp.bfloat16),
            pltpu.VMEM((4, width, units), jnp.bfloat16),
            pltpu.VMEM((4, units, width), jnp.bfloat16),
            pltpu.SemaphoreType.DMA((4, 3)),
        ],
        compiler_params=pltpu.CompilerParams(vmem_limit_bytes=48 * 1024 * 1024),
        cost_estimate=pl.CostEstimate(
            flops=24 * rows * width * units, transcendentals=0, bytes_accessed=24 * width * units
        ),
        name="expert",
    )(x, *weights)


def either_kernel(place_ref, a_ref, b_ref, out_ref, sem):
    core = place_ref[0] % 2
    for own, ref in ((0, a_ref), (1, b_ref)):

        @pl.when(core == own)
        def _():
            copy = pltpu.make_async_copy(ref, out_ref, sem)
            copy.start()
            copy.wait()


def either(place, a, b):
    anywhere = pl.BlockSpec(memory_space=pl.ANY)
    return pl.pallas_call(
        either_kernel,
        out_shape=jax.ShapeDtypeStruct(a.shape, a.dtype),
        in_specs=[pl.BlockSpec(memory_space=pltpu.SMEM), anywhere, anywhere],
        out_specs=anywhere,
        scratch_shapes=[pltpu.SemaphoreType.DMA],
        compiler_params=pltpu.CompilerParams(vmem_limit_bytes=4 * 1024 * 1024),
        name="either",
    )(place, a, b)


def combine_kernel(back_ref, middle_ref, routing_ref, weight_ref, out_ref, *, experts, capacity):
    picks = placed_slots(routing_ref[...], experts, capacity)
    back = back_ref[...]
    total = middle_ref[...].astype(jnp.float32)
    weights = as_columns(weight_ref[...])
    for k in range(2):
        answer = jnp.concatenate([dot_f32(picks[k][0], back), dot_f32(picks[k][1], back)], axis=1)
        total = total + weights[k] * answer
    out_ref[...] = total.astype(jnp.bfloat16)


def combine(back, middle, routing, weight, experts, capacity):
    return pl.pallas_call(
        functools.partial(combine_kernel, experts=experts, capacity=capacity),
        out_shape=jax.ShapeDtypeStruct(middle.shape, jnp.bfloat16),
        compiler_params=pltpu.CompilerParams(vmem_limit_bytes=24 * 1024 * 1024),
        name="combine",
    )(back, middle, routing, weight)


def body(
    residual,
    query_wide,
    key_wide,
    value_wide,
    query_narrow,
    key_narrow,
    value_narrow,
    gate_wide,
    gate_narrow,
    out_wide,
    out_narrow,
    norm_gain,
    routing,
    route_weight,
    gate_weight,
    up_weight,
    down_weight,
):
    dev_rows = query_wide.shape[0]
    own_rows, width = residual.shape
    core = lax.axis_index("core")
    is_wide = core == 0
    n_z, n_x, n_tp = lax.axis_size("z"), lax.axis_size("x"), lax.axis_size("tp")
    n_sp = 2 * n_z * n_x
    sp = ("z", "x", "core")
    place = jnp.full((1,), lax.axis_index(sp), jnp.int32)

    def pick(a, b):
        return jnp.where(is_wide, a, b)

    keep = jnp.concatenate([pick(key_wide, key_narrow), pick(value_wide, value_narrow)], axis=1)
    give = jnp.concatenate([pick(key_narrow, key_wide), pick(value_narrow, value_wide)], axis=1)
    swap = [(0, 1), (1, 0)]
    got = lax.ppermute(give, "core", swap)
    q_keep = pick(query_wide, query_narrow)
    q_got = lax.ppermute(pick(query_narrow, query_wide), "core", swap)
    queries = jnp.concatenate([pick(q_keep, q_got), pick(q_got, q_keep)], axis=0)

    g, u, d = gate_weight[0], up_weight[0], down_weight[0]
    ahead = [(i, (i + 1) % n_tp) for i in range(n_tp)]
    behind = [(i, (i - 1) % n_tp) for i in range(n_tp)]
    from_left = [lax.ppermute(w, "tp", ahead) for w in (g, u, d)]
    from_right = [lax.ppermute(w, "tp", behind) for w in (g, u, d)]
    by_core = [(i, (i + 1) % n_tp) for i in range(n_tp)]
    by_core += [(n_tp + i, n_tp + (i - 1) % n_tp) for i in range(n_tp)]
    far = [
        lax.ppermute(from_left[0], "tp", ahead),
        lax.ppermute(from_right[1], "tp", behind),
        lax.ppermute(either(place, from_left[2], from_right[2]), ("core", "tp"), by_core),
    ]

    next_x = [((i + 1) % n_x, i) for i in range(n_x)]
    prev_x = [((i - 1) % n_x, i) for i in range(n_x)]
    keep_1, keep_3 = lax.ppermute(keep, "x", next_x), lax.ppermute(keep, "x", prev_x)
    got_1, got_3 = lax.ppermute(got, "x", next_x), lax.ppermute(got, "x", prev_x)
    got_2, keep_2 = lax.ppermute(got_1, "x", next_x), lax.ppermute(keep_3, "x", prev_x)
    plane = jnp.concatenate([got, keep, got_1, keep_1, got_2, keep_2, got_3, keep_3], axis=0)
    up = [(i, (i + 1) % n_z) for i in range(n_z)]
    down = [(i, (i - 1) % n_z) for i in range(n_z)]
    planes = [[(plane, (0, 0))]]
    lower = upper = plane
    last = n_z // 2
    for step in range(1, last + 1):
        if step == last:
            lower, upper = half_of(lower, 0), half_of(upper, 1)
        lower = lax.ppermute(lower, "z", up)
        upper = lax.ppermute(upper, "z", down)
        if step < last:
            planes.append([(lower, (step, 0)), (upper, (-step, 0))])
        else:
            planes.append([(lower, (step, 0)), (upper, (step, 2))])

    offs = (0, -1, 1, 2)
    sums = lax.all_gather(running_sums(gate_wide, gate_narrow), "core", axis=0)
    sums = [sums] + [
        lax.ppermute(sums, "x", [((i + off) % n_x, i) for i in range(n_x)]) for off in offs[1:]
    ]
    sums = jnp.concatenate(sums, axis=0)
    sums = [sums] + [
        lax.ppermute(sums, "z", [((i - k) % n_z, i) for i in range(n_z)]) for k in range(1, n_z)
    ]
    decay = offset_sums(place, sums, n_x, offs)

    state = None
    for step, pieces in enumerate(planes):
        state = attend_planes(
            place,
            queries,
            decay,
            [piece for piece, _ in pieces],
            [layout for _, layout in pieces],
            (n_z, n_x),
            dev_rows,
            state,
            step == last,
        )
    att = state

    att = lax.all_to_all(
        att.reshape(2 * n_tp, own_rows, HW), ("core", "tp"), split_axis=0, concat_axis=0, tiled=True
    )
    experts = n_sp
    capacity = own_rows * GROUPS // experts
    middle, outgoing = project(
        att, out_wide, out_narrow, residual, norm_gain.reshape(1, width), routing.T, experts, capacity
    )

    def exchange(slots):
        shape = slots.shape
        slots = slots.reshape(experts, 2 * capacity, width // 2)
        slots = lax.all_to_all(slots, sp, split_axis=0, concat_axis=0, tiled=True)
        return slots.reshape(shape)

    arrived = exchange(outgoing)
    answers = expert(arrived, [g, u, d, *from_left, *from_right, *far], capacity)
    returned = exchange(answers)
    return combine(returned, middle, routing.T, route_weight.T, experts, capacity)


def solution(mesh):
    n_sp, n_tp = mesh.shape["sp"], mesh.shape["tp"]
    n_x = 4
    fine = Mesh(mesh.devices.reshape(n_sp // 2 // n_x, n_x, 2, n_tp), ("z", "x", "core", "tp"))
    sp = ("z", "x", "core")
    rows = P((*sp, "tp"), None)
    heads = P(sp, "tp")
    placed = (
        rows,
        *([heads] * 8),
        P(),
        P(),
        P(),
        rows,
        rows,
        P(sp, None, "tp"),
        P(sp, None, "tp"),
        P(sp, "tp", None),
    )
    return jax.shard_map(body, mesh=fine, in_specs=placed, out_specs=rows, check_vma=False)
```

```python
import functools

import jax
import jax.numpy as jnp
from jax import lax
from jax.experimental import pallas as pl
from jax.experimental.pallas import tpu as pltpu
from jax.sharding import Mesh
from jax.sharding import PartitionSpec as P

HW = 128
HN = 64
GROUPS = 4
EPS = 1e-06
LOG2E = 1.4426950408889634
LOW = -1e30
TQ = 256


def dot_f32(a, b, dims=(((1,), (0,)), ((), ()))):
    return lax.dot_general(a, b, dims, preferred_element_type=jnp.float32)


def decay_line(decay_ref, blocks, head, lines):
    return jnp.concatenate(
        [
            decay_ref[2 * chip + sub, pl.ds(lines * head + (row0 + r) // 128, 1), :]
            for chip, sub, row0, rows in blocks
            for r in range(0, rows, 128)
        ],
        axis=1,
    )


def visit(place, q_ref, decay_ref, kv, blocks, dev_rows, held, forms):
    m_ref, l_ref, acc_ref, qh_ref = held
    chip, core = place // 2, place % 2
    queries = q_ref.shape[0]
    scale = jnp.where(core == 0, jnp.float32(HW**-0.5 * LOG2E), jnp.float32(HN**-0.5 * LOG2E))
    lines = dev_rows // 128
    earliest = latest = blocks[0][0]
    for block in blocks[1:]:
        earliest, latest = jnp.minimum(earliest, block[0]), jnp.maximum(latest, block[0])

    def run(h, masked):
        k = kv[:, :HW]
        v = kv[:, HW:]
        starts = range(0, queries, TQ)
        dk = decay_line(decay_ref, blocks, h + core, lines)
        if masked:
            key_place = jnp.concatenate(
                [
                    lax.broadcasted_iota(jnp.int32, (1, rows), 1) + ((2 * c + sub) * dev_rows + row0)
                    for c, sub, row0, rows in blocks
                ],
                axis=1,
            )

        def scores(r0):
            return dot_f32(qh_ref[h, pl.ds(r0, TQ), :], k, (((1,), (1,)), ((), ())))

        ahead = scores(0)
        for r0 in starts:
            s = ahead * scale - dk
            if r0 + TQ < queries:
                ahead = scores(r0 + TQ)
            span = pl.ds(r0, TQ)
            if masked:
                row = lax.broadcasted_iota(jnp.int32, (TQ, 1), 0) + (chip * (2 * dev_rows) + r0)
                s = jnp.where(key_place <= row, s, LOW)
            m_old = m_ref[h, span, :]
            m_new = jnp.maximum(m_old, jnp.max(s, axis=1, keepdims=True))
            alpha = jnp.exp2(m_old - m_new)
            p = jnp.exp2(s - m_new[:, :1])
            m_ref[h, span, :] = m_new
            l_ref[h, span, :] = l_ref[h, span, :] * alpha + jnp.sum(p, axis=1, keepdims=True)
            acc_ref[h, span, :] = acc_ref[h, span, :] * alpha + dot_f32(p.astype(jnp.bfloat16), v)

    for masked in forms:
        at = earliest <= chip if masked else latest < chip

        @pl.when(at)
        def _():
            def head(h, carry):
                run(h, masked)
                return carry

            lax.fori_loop(0, core + 1, head, 0)


def head_queries(place, q_ref, qh_ref):
    core = place % 2
    q = q_ref[...]
    lane = lax.broadcasted_iota(jnp.int32, q.shape, 1)
    qh_ref[0] = jnp.where((core == 0) | (lane < HN), q, jnp.zeros_like(q))
    qh_ref[1] = jnp.where(lane >= HN, q, jnp.zeros_like(q))


def take_state(ins, held):
    m_ref, l_ref, acc_ref = held
    if ins:
        for source, target in zip(ins, held):
            target[...] = source[...]
    else:
        m_ref[...] = jnp.full_like(m_ref, LOW)
        l_ref[...] = jnp.zeros_like(l_ref)
        acc_ref[...] = jnp.zeros_like(acc_ref)


def plane_kernel(place_ref, q_ref, decay_ref, *rest, pieces, n_z, n_x, dev_rows, first, last):
    n = len(pieces)
    kvs, rest = rest[:n], rest[n:]
    ins = ()
    if not first:
        ins, rest = rest[:3], rest[3:]
    if last:
        out_ref, rest = rest[0], rest[1:]
    held, qh_ref = rest[:3], rest[3]
    take_state(ins, held)
    place = place_ref[0]
    core = place % 2
    head_queries(place, q_ref, qh_ref)
    z, x = place // 2 // n_x, place // 2 % n_x
    tile = 4 * dev_rows
    for kv_ref, (shift, off0) in zip(kvs, pieces):
        plane = (z - shift + n_z) % n_z * n_x

        def one(t, carry, kv_ref=kv_ref, plane=plane, off0=off0, shift=shift):
            blocks = [
                (plane + (x + off0 + 2 * t + i) % n_x, (core + flip) % 2, 0, dev_rows)
                for i in range(2)
                for flip in (1, 0)
            ]
            kv = kv_ref.at[pl.ds(pl.multiple_of(t * tile, tile), tile), :]
            visit(place, q_ref, decay_ref, kv, blocks, dev_rows, rest, (shift == 0,))
            return carry

        lax.fori_loop(0, kv_ref.shape[0] // tile, one, 0)
    if last:
        _, l_ref, acc_ref = held
        lane = lax.broadcasted_iota(jnp.int32, q_ref.shape, 1)
        one_head = acc_ref[0] / l_ref[0]
        other = acc_ref[1] / jnp.where(core == 0, 1.0, l_ref[1])
        out_ref[...] = jnp.where((core == 0) | (lane < HN), one_head, other).astype(jnp.bfloat16)


def attend_planes(place, q, decay, kvs, pieces, sizes, dev_rows, state, last):
    queries = q.shape[0]
    shape = (2, queries, HW)
    smem = pl.BlockSpec(memory_space=pltpu.SMEM)
    vmem = pl.BlockSpec(memory_space=pltpu.VMEM)
    args = [q, decay, *kvs, *(state or ())]
    keys = sum(kv.shape[0] for kv in kvs)
    scratch = [pltpu.VMEM(shape, jnp.bfloat16)]
    if last:
        out_shape, out_specs = jax.ShapeDtypeStruct((queries, HW), jnp.bfloat16), vmem
        scratch = [pltpu.VMEM(shape, jnp.float32)] * 3 + scratch
    else:
        out_shape, out_specs = [jax.ShapeDtypeStruct(shape, jnp.float32)] * 3, [vmem] * 3
    return pl.pallas_call(
        functools.partial(
            plane_kernel,
            pieces=pieces,
            n_z=sizes[0],
            n_x=sizes[1],
            dev_rows=dev_rows,
            first=state is None,
            last=last,
        ),
        out_shape=out_shape,
        in_specs=[smem] + [vmem] * len(args),
        out_specs=out_specs,
        scratch_shapes=scratch,
        compiler_params=pltpu.CompilerParams(vmem_limit_bytes=26 * 1024 * 1024),
        cost_estimate=pl.CostEstimate(
            flops=8 * queries * keys * HW, transcendentals=2 * queries * keys, bytes_accessed=4 * keys * HW
        ),
        name="planes",
    )(place, *args)


def half_kernel(in_ref, out_ref):
    out_ref[...] = in_ref[...]


def half_of(piece, which):
    shape = (piece.shape[0] // 2, piece.shape[1])
    return pl.pallas_call(
        half_kernel,
        out_shape=jax.ShapeDtypeStruct(shape, piece.dtype),
        grid=(1,),
        in_specs=[pl.BlockSpec(shape, lambda i: (which, 0))],
        out_specs=pl.BlockSpec(shape, lambda i: (0, 0)),
        compiler_params=pltpu.CompilerParams(vmem_limit_bytes=8 * 1024 * 1024),
        name="half",
    )(piece)


def running_kernel(wide_ref, narrow_ref, out_ref):
    gates = jnp.concatenate([wide_ref[...], narrow_ref[...]], axis=0)
    kept = jnp.minimum(gates, 0.0) - jnp.log1p(jnp.exp(-jnp.abs(gates)))
    heads, rows = kept.shape
    row = lax.broadcasted_iota(jnp.int32, (rows, rows), 0)
    col = lax.broadcasted_iota(jnp.int32, (rows, rows), 1)
    upto = (row <= col).astype(jnp.float32)
    kept = jnp.concatenate([kept, jnp.zeros((8 - heads, rows), jnp.float32)], axis=0)
    sums = lax.dot_general(
        kept,
        upto,
        (((1,), (0,)), ((), ())),
        precision=lax.Precision.HIGHEST,
        preferred_element_type=jnp.float32,
    )
    out_ref[...] = jnp.zeros_like(out_ref)
    lines = rows // 128
    for h in range(heads):
        for j in range(lines):
            at = lines * h + j
            out_ref[at : at + 1, :] = sums[h : h + 1, j * 128 : (j + 1) * 128]


def running_sums(gate_wide, gate_narrow):
    return pl.pallas_call(
        running_kernel,
        out_shape=jax.ShapeDtypeStruct((8, 128), jnp.float32),
        compiler_params=pltpu.CompilerParams(vmem_limit_bytes=8 * 1024 * 1024),
        name="running",
    )(gate_wide.T, gate_narrow.T)


def offset_kernel(place_ref, *rest, n_z, n_x, offs):
    pieces, (out_ref, abs_ref) = rest[:n_z], rest[n_z:]
    chip = place_ref[0] // 2
    z, x = chip // n_x, chip % n_x
    for k in range(n_z):
        for i, off in enumerate(offs):
            at = (z - k + n_z) % n_z * n_x + (x + off + n_x) % n_x
            abs_ref[2 * at] = pieces[k][2 * i]
            abs_ref[2 * at + 1] = pieces[k][2 * i + 1]
    devices = abs_ref.shape[0]
    odd = lax.broadcasted_iota(jnp.int32, (8, 128), 0) % 2 == 1
    offset = jnp.zeros((8, 128), jnp.float32)
    base = offset
    for d in range(devices):
        here = abs_ref[d]
        out_ref[d] = here + offset
        base = jnp.where(2 * chip == d, offset, base)
        end = jnp.broadcast_to(here[:, 127:128], (8, 128))
        offset = offset + jnp.where(odd, end, jnp.concatenate([end[1:], end[:1]], axis=0))
    for d in range(devices):
        out_ref[d] = (out_ref[d] - base) * LOG2E


def offset_sums(place, pieces, n_x, offs):
    every = (len(pieces) * pieces[0].shape[0], 8, 128)
    smem = pl.BlockSpec(memory_space=pltpu.SMEM)
    vmem = pl.BlockSpec(memory_space=pltpu.VMEM)
    return pl.pallas_call(
        functools.partial(offset_kernel, n_z=len(pieces), n_x=n_x, offs=offs),
        out_shape=jax.ShapeDtypeStruct(every, jnp.float32),
        in_specs=[smem] + [vmem] * len(pieces),
        scratch_shapes=[pltpu.VMEM(every, jnp.float32)],
        compiler_params=pltpu.CompilerParams(vmem_limit_bytes=8 * 1024 * 1024),
        name="offset",
    )(place, *pieces)


def as_columns(lines):
    n = lines.shape[1]
    same = lax.broadcasted_iota(jnp.int32, (n, n), 0) == lax.broadcasted_iota(jnp.int32, (n, n), 1)
    return [jnp.sum(jnp.where(same, lines[k : k + 1], 0.0), axis=1, keepdims=True) for k in range(2)]


def placed_slots(routing, experts, capacity):
    rows = routing.shape[1]
    routing = [column.astype(jnp.int32) for column in as_columns(routing.astype(jnp.float32))]
    expert = lax.broadcasted_iota(jnp.int32, (rows, experts), 1)
    hits = [(routing[k] == expert).astype(jnp.float32) for k in range(2)]
    row = lax.broadcasted_iota(jnp.int32, (rows, rows), 0)
    col = lax.broadcasted_iota(jnp.int32, (rows, rows), 1)
    before = (col < row).astype(jnp.bfloat16)
    earlier = dot_f32(before, (hits[0] + hits[1]).astype(jnp.bfloat16))
    slot = lax.broadcasted_iota(jnp.int32, (rows, 2 * experts * capacity), 1)
    picks = []
    for k in range(2):
        rank = jnp.sum(earlier * hits[k], axis=1, keepdims=True).astype(jnp.int32)
        place = routing[k] * (2 * capacity) + rank
        picks.append([(place + half * capacity == slot).astype(jnp.bfloat16) for half in range(2)])
    return picks


def project_kernel(
    att_ref,
    wide_hbm,
    narrow_hbm,
    residual_ref,
    gain_ref,
    routing_ref,
    middle_ref,
    out_ref,
    wide_ref,
    narrow_ref,
    sems,
    *,
    experts,
    capacity,
):
    copies = [
        pltpu.make_async_copy(wide_hbm, wide_ref, sems.at[0]),
        pltpu.make_async_copy(narrow_hbm, narrow_ref, sems.at[1]),
    ]
    for copy in copies:
        copy.start()
    picks = placed_slots(routing_ref[...], experts, capacity)
    half = att_ref.shape[0] // 2
    wide = jnp.concatenate([att_ref[j] for j in range(half)], axis=1)
    narrow = jnp.concatenate([att_ref[half + j] for j in range(half)], axis=1)
    copies[0].wait()
    mixed = dot_f32(wide, wide_ref[...])
    copies[1].wait()
    mixed = mixed + dot_f32(narrow, narrow_ref[...])
    middle = (residual_ref[...].astype(jnp.float32) + mixed).astype(jnp.bfloat16)
    middle_ref[...] = middle
    wider = middle.astype(jnp.float32)
    spread = jnp.mean(wider * wider, axis=1, keepdims=True)
    normed = (wider * lax.rsqrt(spread + EPS) * gain_ref[...]).astype(jnp.bfloat16)
    half = normed.shape[1] // 2
    over_rows = (((0,), (0,)), ((), ()))
    low = dot_f32(picks[0][0] + picks[1][0], normed[:, :half], over_rows)
    high = dot_f32(picks[0][1] + picks[1][1], normed[:, half:], over_rows)
    out_ref[...] = (low + high).astype(jnp.bfloat16)


def project(att, wide, narrow, residual, gain, routing, experts, capacity):
    rows, width = residual.shape
    anywhere = pl.BlockSpec(memory_space=pltpu.HBM)
    vmem = pl.BlockSpec(memory_space=pltpu.VMEM)
    return pl.pallas_call(
        functools.partial(project_kernel, experts=experts, capacity=capacity),
        out_shape=[
            jax.ShapeDtypeStruct((rows, width), jnp.bfloat16),
            jax.ShapeDtypeStruct((2 * experts * capacity, width // 2), jnp.bfloat16),
        ],
        in_specs=[vmem, anywhere, anywhere, vmem, vmem, vmem],
        out_specs=[vmem, vmem],
        scratch_shapes=[
            pltpu.VMEM(wide.shape, wide.dtype),
            pltpu.VMEM(narrow.shape, narrow.dtype),
            pltpu.SemaphoreType.DMA((2,)),
        ],
        compiler_params=pltpu.CompilerParams(vmem_limit_bytes=60 * 1024 * 1024),
        cost_estimate=pl.CostEstimate(
            flops=2 * rows * 1024 * width, transcendentals=0, bytes_accessed=2 * 1024 * width
        ),
        name="project",
    )(att, wide, narrow, residual, gain, routing)


def expert_kernel(x_ref, *rest, capacity):
    weights, (out_ref, g_ref, u_ref, d_ref, sems) = rest[:12], rest[12:]
    copies = []
    for j in range(4):
        mine = [
            pltpu.make_async_copy(weights[3 * j + i], ref.at[j], sems.at[j, i])
            for i, ref in enumerate((g_ref, u_ref, d_ref))
        ]
        copies.append(mine)
    for mine in copies:
        for copy in mine:
            copy.start()
    x = x_ref[...]
    slots = x.shape[0]
    slot = lax.broadcasted_iota(jnp.int32, (slots // 2, slots), 0)
    from_slot = lax.broadcasted_iota(jnp.int32, (slots // 2, slots), 1)
    low_place = slot // capacity * (2 * capacity) + slot % capacity
    low = (from_slot == low_place).astype(jnp.bfloat16)
    high = (from_slot == low_place + capacity).astype(jnp.bfloat16)
    x = jnp.concatenate([dot_f32(low, x), dot_f32(high, x)], axis=1).astype(jnp.bfloat16)
    total = None
    for j in range(4):
        for copy in copies[j]:
            copy.wait()
        gate = dot_f32(x, g_ref[j])
        up = dot_f32(x, u_ref[j])
        hidden = (gate * jax.nn.sigmoid(gate) * up).astype(jnp.bfloat16)
        part = dot_f32(hidden, d_ref[j])
        total = part if total is None else total + part
    total = total.astype(jnp.bfloat16)
    half = total.shape[1] // 2
    over_rows = (((0,), (0,)), ((), ()))
    spread = dot_f32(low, total[:, :half], over_rows) + dot_f32(high, total[:, half:], over_rows)
    out_ref[...] = spread.astype(jnp.bfloat16)


def expert(x, weights, capacity):
    rows, width = x.shape[0] // 2, 2 * x.shape[1]
    units = weights[0].shape[1]
    anywhere = pl.BlockSpec(memory_space=pl.ANY)
    vmem = pl.BlockSpec(memory_space=pltpu.VMEM)
    return pl.pallas_call(
        functools.partial(expert_kernel, capacity=capacity),
        out_shape=jax.ShapeDtypeStruct(x.shape, jnp.bfloat16),
        in_specs=[vmem] + [anywhere] * 12,
        out_specs=vmem,
        scratch_shapes=[
            pltpu.VMEM((4, width, units), jnp.bfloat16),
            pltpu.VMEM((4, width, units), jnp.bfloat16),
            pltpu.VMEM((4, units, width), jnp.bfloat16),
            pltpu.SemaphoreType.DMA((4, 3)),
        ],
        compiler_params=pltpu.CompilerParams(vmem_limit_bytes=48 * 1024 * 1024),
        cost_estimate=pl.CostEstimate(
            flops=24 * rows * width * units, transcendentals=0, bytes_accessed=24 * width * units
        ),
        name="expert",
    )(x, *weights)


def either_kernel(place_ref, a_ref, b_ref, out_ref, sem):
    core = place_ref[0] % 2
    for own, ref in ((0, a_ref), (1, b_ref)):

        @pl.when(core == own)
        def _():
            copy = pltpu.make_async_copy(ref, out_ref, sem)
            copy.start()
            copy.wait()


def either(place, a, b):
    anywhere = pl.BlockSpec(memory_space=pl.ANY)
    return pl.pallas_call(
        either_kernel,
        out_shape=jax.ShapeDtypeStruct(a.shape, a.dtype),
        in_specs=[pl.BlockSpec(memory_space=pltpu.SMEM), anywhere, anywhere],
        out_specs=anywhere,
        scratch_shapes=[pltpu.SemaphoreType.DMA],
        compiler_params=pltpu.CompilerParams(vmem_limit_bytes=4 * 1024 * 1024),
        name="either",
    )(place, a, b)


def combine_kernel(back_ref, middle_ref, routing_ref, weight_ref, out_ref, *, experts, capacity):
    picks = placed_slots(routing_ref[...], experts, capacity)
    back = back_ref[...]
    total = middle_ref[...].astype(jnp.float32)
    weights = as_columns(weight_ref[...])
    for k in range(2):
        answer = jnp.concatenate([dot_f32(picks[k][0], back), dot_f32(picks[k][1], back)], axis=1)
        total = total + weights[k] * answer
    out_ref[...] = total.astype(jnp.bfloat16)


def combine(back, middle, routing, weight, experts, capacity):
    return pl.pallas_call(
        functools.partial(combine_kernel, experts=experts, capacity=capacity),
        out_shape=jax.ShapeDtypeStruct(middle.shape, jnp.bfloat16),
        compiler_params=pltpu.CompilerParams(vmem_limit_bytes=24 * 1024 * 1024),
        name="combine",
    )(back, middle, routing, weight)


def body(
    residual,
    query_wide,
    key_wide,
    value_wide,
    query_narrow,
    key_narrow,
    value_narrow,
    gate_wide,
    gate_narrow,
    out_wide,
    out_narrow,
    norm_gain,
    routing,
    route_weight,
    gate_weight,
    up_weight,
    down_weight,
):
    dev_rows = query_wide.shape[0]
    own_rows, width = residual.shape
    core = lax.axis_index("core")
    is_wide = core == 0
    n_z, n_x, n_tp = lax.axis_size("z"), lax.axis_size("x"), lax.axis_size("tp")
    n_sp = 2 * n_z * n_x
    sp = ("z", "x", "core")
    place = jnp.full((1,), lax.axis_index(sp), jnp.int32)

    def pick(a, b):
        return jnp.where(is_wide, a, b)

    keep = jnp.concatenate([pick(key_wide, key_narrow), pick(value_wide, value_narrow)], axis=1)
    give = jnp.concatenate([pick(key_narrow, key_wide), pick(value_narrow, value_wide)], axis=1)
    swap = [(0, 1), (1, 0)]
    got = lax.ppermute(give, "core", swap)
    q_keep = pick(query_wide, query_narrow)
    q_got = lax.ppermute(pick(query_narrow, query_wide), "core", swap)
    queries = jnp.concatenate([pick(q_keep, q_got), pick(q_got, q_keep)], axis=0)

    g, u, d = gate_weight[0], up_weight[0], down_weight[0]
    ahead = [(i, (i + 1) % n_tp) for i in range(n_tp)]
    behind = [(i, (i - 1) % n_tp) for i in range(n_tp)]
    from_left = [lax.ppermute(w, "tp", ahead) for w in (g, u, d)]
    from_right = [lax.ppermute(w, "tp", behind) for w in (g, u, d)]
    by_core = [(i, (i + 1) % n_tp) for i in range(n_tp)]
    by_core += [(n_tp + i, n_tp + (i - 1) % n_tp) for i in range(n_tp)]
    far = [
        lax.ppermute(from_left[0], "tp", ahead),
        lax.ppermute(from_right[1], "tp", behind),
        lax.ppermute(either(place, from_left[2], from_right[2]), ("core", "tp"), by_core),
    ]

    next_x = [((i + 1) % n_x, i) for i in range(n_x)]
    prev_x = [((i - 1) % n_x, i) for i in range(n_x)]
    keep_1, keep_3 = lax.ppermute(keep, "x", next_x), lax.ppermute(keep, "x", prev_x)
    got_1, got_3 = lax.ppermute(got, "x", next_x), lax.ppermute(got, "x", prev_x)
    got_2, keep_2 = lax.ppermute(got_1, "x", next_x), lax.ppermute(keep_3, "x", prev_x)
    plane = jnp.concatenate([got, keep, got_1, keep_1, got_2, keep_2, got_3, keep_3], axis=0)
    up = [(i, (i + 1) % n_z) for i in range(n_z)]
    down = [(i, (i - 1) % n_z) for i in range(n_z)]
    planes = [[(plane, (0, 0))]]
    lower = upper = plane
    last = n_z // 2
    for step in range(1, last + 1):
        if step == last:
            lower, upper = half_of(lower, 0), half_of(upper, 1)
        lower = lax.ppermute(lower, "z", up)
        upper = lax.ppermute(upper, "z", down)
        if step < last:
            planes.append([(lower, (step, 0)), (upper, (-step, 0))])
        else:
            planes.append([(lower, (step, 0)), (upper, (step, 2))])

    offs = (0, -1, 1, 2)
    sums = lax.all_gather(running_sums(gate_wide, gate_narrow), "core", axis=0)
    sums = [sums] + [
        lax.ppermute(sums, "x", [((i + off) % n_x, i) for i in range(n_x)]) for off in offs[1:]
    ]
    sums = jnp.concatenate(sums, axis=0)
    sums = [sums] + [
        lax.ppermute(sums, "z", [((i - k) % n_z, i) for i in range(n_z)]) for k in range(1, n_z)
    ]
    decay = offset_sums(place, sums, n_x, offs)

    state = None
    for step, pieces in enumerate(planes):
        state = attend_planes(
            place,
            queries,
            decay,
            [piece for piece, _ in pieces],
            [layout for _, layout in pieces],
            (n_z, n_x),
            dev_rows,
            state,
            step == last,
        )
    att = state

    att = lax.all_to_all(
        att.reshape(2 * n_tp, own_rows, HW), ("core", "tp"), split_axis=0, concat_axis=0, tiled=True
    )
    experts = n_sp
    capacity = own_rows * GROUPS // experts
    middle, outgoing = project(
        att, out_wide, out_narrow, residual, norm_gain.reshape(1, width), routing.T, experts, capacity
    )

    def exchange(slots):
        shape = slots.shape
        slots = slots.reshape(experts, 2 * capacity, width // 2)
        slots = lax.all_to_all(slots, sp, split_axis=0, concat_axis=0, tiled=True)
        return slots.reshape(shape)

    arrived = exchange(outgoing)
    answers = expert(arrived, [g, u, d, *from_left, *from_right, *far], capacity)
    returned = exchange(answers)
    return combine(returned, middle, routing.T, route_weight.T, experts, capacity)


def solution(mesh):
    n_sp, n_tp = mesh.shape["sp"], mesh.shape["tp"]
    n_x = 4
    fine = Mesh(mesh.devices.reshape(n_sp // 2 // n_x, n_x, 2, n_tp), ("z", "x", "core", "tp"))
    sp = ("z", "x", "core")
    rows = P((*sp, "tp"), None)
    heads = P(sp, "tp")
    placed = (
        rows,
        *([heads] * 8),
        P(),
        P(),
        P(),
        rows,
        rows,
        P(sp, None, "tp"),
        P(sp, None, "tp"),
        P(sp, "tp", None),
    )
    return jax.shard_map(body, mesh=fine, in_specs=placed, out_specs=rows, check_vma=False)
```
